32 devices in a mesh: fs: 16 (over z, y, x), tp: 2 (over core).
Axes of the slice: x: 2, y: 2, z: 4, core: 2. Of those that a mesh axis runs over, the one named last changes fastest.
Arguments:
- tokens: bfloat16 [12288, 2048], P('fs'), may hold values from -6 to 6
- norm_gain: float32 [2048], replicated, may hold values from 0.1 to 1.9
- gate_weight: float32 [2048, 5120], P('fs', 'tp'), may hold values from -0.125 to 0.125
- value_weight: float32 [2048, 5120], P('fs', 'tp'), may hold values from -0.125 to 0.125
- gate_scale: float32 [5120], P('tp'), may hold values from 0.3 to 3
- value_scale: float32 [5120], P('tp'), may hold values from 0.3 to 3
- gate_kernel: float32 [3, 5120], P(None, 'tp'), may hold values from -3.5 to 3.5
- value_kernel: float32 [3, 5120], P(None, 'tp'), may hold values from -3.5 to 3.5
- gate_bias: float32 [5120], P('tp'), may hold values from -3 to 3
- value_bias: float32 [5120], P('tp'), may hold values from -3 to 3
- down_weight: float32 [5120, 2048], P('tp', 'fs'), may hold values from -0.078125 to 0.078125
- down_scale: float32 [2048], P('tp'), may hold values from 0.3 to 3
Outputs:
- mixed: bfloat16 [12288, 2048], P('fs', 'tp')
The draws below stay inside these ranges and needn't reach their ends.
All inputs are finite; a program needn't handle non-finite values.
Results may differ from the reference program's by a relative error of at most 0.014.
Values may be sent and summed in bfloat16 or wider, within the bound.
A program may use at most 128 MiB of HBM per device.

```python
import math
import jax
import jax.numpy as jnp
from jax import lax

D = 2048
FF = 5120
KERNEL = 3
TOK = 768
TOKENS = 12288
N_FS = 16
N_TP = 2


def block_scale(own_key, extent, shards, least, high):
    loudness, own = 1.0, jax.random.fold_in(own_key, 6)
    for dim, shards_of in shards:
        draws = jnp.exp(jax.random.uniform(jax.random.fold_in(own, dim), (shards_of,), jnp.float32, least / len(shards), high / len(shards)))
        loudness = loudness * jnp.repeat(draws, extent[dim] // shards_of).reshape([-1 if axis == dim else 1 for axis in range(len(extent))])
    return loudness


def gaussian(rng, extent, scale, most, cuts=(), held_as=jnp.bfloat16):
    level = block_scale(rng, extent, cuts, -0.22, 0.18) if cuts else 1.0
    entries = jax.random.normal(rng, extent, jnp.float32) * scale * level
    return jnp.minimum(jnp.maximum(entries, -most), most).astype(held_as)


def setup_inputs(seed: int = 0) -> dict:
    keys = jax.random.split(jax.random.key(seed), 13)
    return {
        "tokens": gaussian(keys[0], (TOKENS, D), 1.0, 6.0, ((0, 16),)),
        "norm_gain": jnp.clip(1.0 + 0.18 * jax.random.normal(keys[1], (D,), jnp.float32), 0.1, 1.9),
        "gate_weight": gaussian(keys[2], (D, FF), D ** -0.5, 0.125, ((0, 16), (1, 2)), jnp.float32),
        "value_weight": gaussian(keys[3], (D, FF), D ** -0.5, 0.125, ((0, 16), (1, 2)), jnp.float32),
        "gate_scale": jnp.clip(jnp.exp(math.log(3.0) - 2.3025851 * jax.random.uniform(keys[4], (FF,), jnp.float32) ** block_scale(keys[4], (FF,), ((0, 2),), -0.2, 0.2)), 0.3, 3.0),
        "value_scale": jnp.clip(jnp.exp(math.log(3.0) - 2.3025851 * jax.random.uniform(keys[5], (FF,), jnp.float32) ** block_scale(keys[5], (FF,), ((0, 2),), -0.2, 0.2)), 0.3, 3.0),
        "gate_kernel": gaussian(keys[6], (KERNEL, FF), KERNEL ** -0.5, 3.5, ((1, 2),), jnp.float32),
        "value_kernel": gaussian(keys[7], (KERNEL, FF), KERNEL ** -0.5, 3.5, ((1, 2),), jnp.float32),
        "gate_bias": gaussian(keys[8], (FF,), 0.5, 3.0, ((0, 2),), jnp.float32),
        "value_bias": gaussian(keys[9], (FF,), 0.5, 3.0, ((0, 2),), jnp.float32),
        "down_weight": gaussian(keys[10], (FF, D), FF ** -0.5, 0.078125, ((0, 2), (1, 16)), jnp.float32),
        "down_scale": jnp.clip(jnp.exp(math.log(3.0) - 2.3025851 * jax.random.uniform(keys[11], (D,), jnp.float32) ** block_scale(keys[11], (D,), ((0, 2),), -0.2, 0.2)), 0.3, 3.0),
    }


epsilon = 1e-06

def normalize(tokens, norm_gain):
    values = tokens.astype(jnp.float32)
    scaled = values * lax.rsqrt(lax.optimization_barrier(jnp.mean(values * values, axis=1, keepdims=True)) + epsilon)
    return (scaled * norm_gain[None, :]).astype(jnp.bfloat16)

def causal_mix(current, previous, kernel, tap_bias):
    row_count = current.shape[0]
    joined = jnp.concatenate([previous, current], axis=0).astype(jnp.float32)
    summed_taps = tap_bias[None, :] + kernel[2][None, :] * joined[2:]
    for back_by in (1, 2):
        summed_taps = summed_taps + kernel[2 - back_by][None, :] * joined[2 - back_by:2 - back_by + row_count]
    return summed_taps

def reference(tokens, norm_gain, gate_weight, value_weight, gate_scale, value_scale, gate_kernel, value_kernel, gate_bias, value_bias, down_weight, down_scale):
    gate_low = gate_weight.astype(jnp.bfloat16)
    value_low = value_weight.astype(jnp.bfloat16)
    down_low = down_weight.astype(jnp.bfloat16)
    block_width = FF // N_TP

    def one_block(carry, block_rows):
        previous_gate, previous_value = carry
        normed = normalize(block_rows, norm_gain)
        gate_pre = (jnp.dot(normed, gate_low, preferred_element_type=jnp.float32) * gate_scale[None, :]).astype(jnp.bfloat16)
        value_pre = (jnp.dot(normed, value_low, preferred_element_type=jnp.float32) * value_scale[None, :]).astype(jnp.bfloat16)
        gate_conv = causal_mix(gate_pre, previous_gate, gate_kernel, gate_bias)
        value_conv = causal_mix(value_pre, previous_value, value_kernel, value_bias)
        hidden = (jax.nn.gelu(gate_conv, approximate=True) * value_conv).astype(jnp.bfloat16)
        summed = jnp.zeros((block_rows.shape[0], D), jnp.float32)
        for block_index in range(N_TP):
            first_col = block_index * block_width
            partial_term = jnp.dot(hidden[:, first_col:first_col + block_width], down_low[first_col:first_col + block_width], preferred_element_type=jnp.float32).astype(jnp.bfloat16)
            partial_term = lax.optimization_barrier(partial_term)
            summed = summed + partial_term.astype(jnp.float32)
        result = (summed * down_scale[None, :]).astype(jnp.bfloat16)
        return ((gate_pre[-2:], value_pre[-2:]), result)
    start = (jnp.zeros((2, FF), jnp.bfloat16), jnp.zeros((2, FF), jnp.bfloat16))
    final_carry, mixed = lax.scan(one_block, start, tokens.reshape(N_FS, TOK, D))
    return mixed.reshape(TOKENS, D)
```

```python
import functools
import math

import jax
import jax.numpy as jnp
from jax import lax
from jax.experimental import pallas as pl
from jax.experimental.pallas import tpu as pltpu
from jax.sharding import PartitionSpec as P

epsilon = 1e-06


def from_behind(value, axis, steps):
    count = lax.axis_size(axis)
    leading, last = (max(0, -steps), min(count, count - steps))
    return lax.ppermute(value, axis, [(source, source + steps) for source in range(leading, last)])


def normalize(tokens, norm_gain):
    values = tokens.astype(jnp.float32)
    scaled = values * lax.rsqrt(jnp.mean(values * values, axis=1, keepdims=True) + epsilon)
    return (scaled * norm_gain[None, :]).astype(jnp.bfloat16)


def causal_mix(current, previous, kernel, tap_bias):
    row_count = current.shape[0]
    joined = jnp.concatenate([previous, current], axis=0).astype(jnp.float32)
    summed_taps = tap_bias[None, :] + kernel[2][None, :] * joined[2:]
    for back_by in (1, 2):
        summed_taps = (
            summed_taps
            + kernel[2 - back_by][None, :] * joined[2 - back_by : 2 - back_by + row_count]
        )
    return summed_taps


def body(
    tokens,
    norm_gain,
    gate_weight,
    value_weight,
    gate_scale,
    value_scale,
    gate_kernel,
    value_kernel,
    gate_bias,
    value_bias,
    down_weight,
    down_scale,
):
    normed = normalize(tokens, norm_gain)
    gate_low = gate_weight.astype(jnp.bfloat16)
    value_low = value_weight.astype(jnp.bfloat16)
    down_low = down_weight.astype(jnp.bfloat16)
    row_count = normed.shape[0]
    gate_full, value_full, down_full = (
        lax.all_gather(gate_low, "fs", axis=0, tiled=True),
        lax.all_gather(value_low, "fs", axis=0, tiled=True),
        lax.all_gather(down_low, "fs", axis=1, tiled=True),
    )
    gate_raw = jnp.dot(normed, gate_full, preferred_element_type=jnp.float32)
    value_raw = jnp.dot(normed, value_full, preferred_element_type=jnp.float32)
    gate_pre = (gate_raw * gate_scale[None, :]).astype(jnp.bfloat16)
    value_pre = (value_raw * value_scale[None, :]).astype(jnp.bfloat16)
    previous_gate, previous_value = from_behind(
        (gate_pre[row_count - 2 :], value_pre[row_count - 2 :]), "fs", 1
    )
    gate_conv = causal_mix(gate_pre, previous_gate, gate_kernel, gate_bias)
    value_conv = causal_mix(value_pre, previous_value, value_kernel, value_bias)
    hidden = (jax.nn.gelu(gate_conv, approximate=True) * value_conv).astype(jnp.bfloat16)
    partial_terms = jnp.dot(hidden, down_full, preferred_element_type=jnp.float32)
    summed = lax.psum_scatter(
        partial_terms.astype(jnp.bfloat16), "tp", scatter_dimension=1, tiled=True
    ).astype(jnp.float32)
    return (summed * down_scale[None, :]).astype(jnp.bfloat16)


MESH = pl.DeviceIdType.MESH
GROUP = 4
EDGE = 16


def fused_kernel(
    depth_planes,
    tok_hbm,
    gate_hbm,
    value_hbm,
    down_hbm,
    gain,
    gate_scale,
    value_scale,
    gate_kernel,
    value_kernel,
    gate_bias,
    value_bias,
    osc,
    out,
    tok,
    up_all,
    down_all,
    hidden,
    stage,
    pair_in,
    peer_in,
    relay_in,
    taps,
    edge,
    edge_pre,
    par,
    wu,
    wd,
    raw_tok,
    raw_gate,
    raw_value,
    raw_down,
    sem_fetch,
    sem_own,
    sem_plane_send,
    sem_recv,
    sem_line_send,
    sem_edge,
    sem_tok_send,
    sem_tok_recv,
    sem_diag_send,
    sem_diag_recv,
    sem_tok_pair_send,
    sem_tok_pair_recv,
    sem_pair_send,
    sem_pair_recv,
    sem_peer_send,
    sem_peer_recv,
    sem_relay_send,
    sem_relay_recv,
):
    planes = depth_planes
    half = planes // 2
    me = lax.axis_index("fs")
    core = lax.axis_index("tp")
    z, p = me // GROUP, me % GROUP
    rows_own = raw_tok.shape[0]
    part_rows = rows_own // 2
    blocks, piece = wu.shape[1], wu.shape[2]
    units = hidden.shape[1]
    out_piece = wd.shape[2]
    chunk = GROUP * out_piece
    has_up, has_down = z < planes - 1, z > 0
    inner_plane = has_up & has_down
    down_kind = blocks

    def flip(mask):
        px, py = p % 2, p // 2
        return (py + mask // 2) % 2 * 2 + (px + mask % 2) % 2

    def chip(target):
        return (z * GROUP + target, core)

    others = (1, 2, 3)

    fetches = [
        pltpu.make_async_copy(src, dst, sem_fetch.at[i])
        for i, (src, dst) in enumerate(
            ((gate_hbm, raw_gate), (value_hbm, raw_value), (tok_hbm, raw_tok), (down_hbm, raw_down))
        )
    ]
    for fetch in fetches:
        fetch.start()

    barrier = pltpu.get_barrier_semaphore()
    for mask in others:
        pl.semaphore_signal(barrier, inc=1, device_id=chip(flip(mask)), device_id_type=MESH)
    pl.semaphore_signal(barrier, inc=1, device_id=(me, 1 - core), device_id_type=MESH)

    @pl.when(has_up)
    def _():
        pl.semaphore_signal(barrier, inc=1, device_id=(me + GROUP, core), device_id_type=MESH)

    @pl.when(has_down)
    def _():
        pl.semaphore_signal(barrier, inc=1, device_id=(me - GROUP, core), device_id_type=MESH)

    def remote(src, dst, send, recv, device):
        return pltpu.make_async_remote_copy(
            src_ref=src, dst_ref=dst, send_sem=send, recv_sem=recv, device_id=device, device_id_type=MESH
        )

    def up_block(j, f):
        return up_all.at[j, pl.ds(pl.multiple_of(f * piece, piece), piece), :]

    def down_block(f):
        return down_all.at[f // GROUP, :, pl.ds(pl.multiple_of(f % GROUP * out_piece, out_piece), out_piece)]

    def plane_up(j, mask):
        target = flip(mask)
        return remote(
            wu.at[target, j], up_block(j, me), sem_plane_send.at[j, mask], sem_recv.at[j, me], chip(target)
        )

    def plane_down(mask):
        target = flip(mask)
        return remote(
            wd.at[target],
            down_block(me),
            sem_plane_send.at[down_kind, mask],
            sem_recv.at[down_kind, me],
            chip(target),
        )

    def line_up(j, direction, f, src=None):
        here = up_block(j, f)
        return remote(
            here if src is None else src,
            here,
            sem_line_send.at[j, direction, f],
            sem_recv.at[j, f],
            (me + (GROUP if direction == 0 else -GROUP), core),
        )

    def line_down(direction, f, src=None):
        here = down_block(f)
        return remote(
            here if src is None else src,
            here,
            sem_line_send.at[down_kind, direction, f],
            sem_recv.at[down_kind, f],
            (me + (GROUP if direction == 0 else -GROUP), core),
        )

    def both_ways(copy_of):
        @pl.when(has_up)
        def _():
            copy_of(0).start()

        @pl.when(has_down)
        def _():
            copy_of(1).start()

    def wait_up(j, f):
        here = up_block(j, f)
        remote(here, here, sem_line_send.at[j, 0, f], sem_recv.at[j, f], (me, 1 - core)).wait_recv()

    def wait_down(f):
        here = down_block(f)
        remote(here, here, sem_line_send.at[down_kind, 0, f], sem_recv.at[down_kind, f], (me, 1 - core)).wait_recv()

    def own_up(j):
        return pltpu.make_async_copy(wu.at[p, j], up_block(j, me), sem_own.at[j])

    own_down = pltpu.make_async_copy(wd.at[p], down_block(me), sem_own.at[down_kind])

    def cast_block(j):
        for m in range(GROUP):
            first = m * units + j * 128
            wu[m, j, :, 0:128] = raw_gate[:, first : first + 128].astype(jnp.bfloat16)
            wu[m, j, :, 128:256] = raw_value[:, first : first + 128].astype(jnp.bfloat16)

    def normed(first, count):
        values = raw_tok[pl.ds(first, count), :].astype(jnp.float32)
        scaled = values * lax.rsqrt(jnp.mean(values * values, axis=1, keepdims=True) + epsilon)
        return (scaled * gain[...]).astype(jnp.bfloat16)

    fetches[0].wait()
    fetches[1].wait()
    for j in range(blocks):
        cast_block(j)
    pl.semaphore_wait(barrier, 4 + has_up.astype(jnp.int32) + has_down.astype(jnp.int32))
    for j in range(blocks):
        for mask in others:
            plane_up(j, mask).start()
        both_ways(lambda direction: line_up(j, direction, me, wu.at[p, j]))
    for j in range(blocks):
        own_up(j).start()

    def edge_slot(slot):
        return edge.at[pl.ds(pl.multiple_of(slot * EDGE, EDGE), EDGE), :]

    def edge_copy(mask):
        here = edge_slot(p + 1)
        return remote(here, here, sem_edge.at[0, mask], sem_edge.at[1, mask], chip(flip(mask)))

    edge_next = remote(
        edge_slot(GROUP), edge_slot(0), sem_edge.at[0, 0], sem_edge.at[1, 0], (me + GROUP, core)
    )

    @pl.when(jnp.logical_not(has_down))
    def _():
        edge[0:EDGE, :] = jnp.zeros_like(edge[0:EDGE, :])

    fetches[2].wait()
    edge[pl.ds(pl.multiple_of((p + 1) * EDGE, EDGE), EDGE), :] = normed(rows_own - EDGE, EDGE)
    for mask in others:
        edge_copy(mask).start()
    norm_tile = 64

    def norm_step(i, carry):
        first = pl.multiple_of(i * norm_tile, norm_tile)
        tok[pl.ds(pl.multiple_of(p * rows_own + i * norm_tile, norm_tile), norm_tile), :] = normed(first, norm_tile)
        return carry

    lax.fori_loop(0, rows_own // norm_tile, norm_step, 0)

    parts = 2
    sub_rows = part_rows // parts
    diag_rows = sub_rows // 2

    def token_rows(owner, side, part):
        start = owner * rows_own + side * part_rows + part * sub_rows
        return tok.at[pl.ds(pl.multiple_of(start, sub_rows), sub_rows), :]

    def diag_part(owner, part, which):
        start = owner * rows_own + core * part_rows + part * sub_rows + which * diag_rows
        return tok.at[pl.ds(pl.multiple_of(start, diag_rows), diag_rows), :]

    def token_copy(mask, part):
        here = token_rows(p, core, part)
        return remote(here, here, sem_tok_send.at[mask, part], sem_tok_recv.at[mask, part], chip(flip(mask)))

    def token_relay(mask, part):
        here = diag_part(flip(mask), part, mask - 1)
        return remote(
            here,
            here,
            sem_diag_send.at[mask, part],
            sem_diag_recv.at[mask, part],
            chip(flip(3 - mask)),
        )

    def token_pair(mask, part):
        here = token_rows(flip(mask), core, part)
        return remote(
            here, here, sem_tok_pair_send.at[mask, part], sem_tok_pair_recv.at[mask, part], (me, 1 - core)
        )

    for part in range(parts):
        for mask in (1, 2):
            token_copy(mask, part).start()

    fetches[3].wait()
    for m in range(GROUP):
        wd[m] = raw_down[m * units : (m + 1) * units, :].astype(jnp.bfloat16)
    own_down.start()
    for mask in others:
        plane_down(mask).start()
    for j in range(blocks):
        src = pl.ds(p * blocks + j, 1)
        cols = pl.ds(pl.multiple_of(p * units + j * 128, 128), 128)
        for side, (scale, kernel, tap_bias) in enumerate(
            ((gate_scale, gate_kernel, gate_bias), (value_scale, value_kernel, value_bias))
        ):
            dst = slice(j * 256 + side * 128, j * 256 + side * 128 + 128)
            par[0:1, dst] = scale[src, :]
            par[1:4, dst] = kernel[0:3, cols]
            par[4:5, dst] = tap_bias[src, :]

    def own_plane(j, carry):
        for mask in others:
            f = z * GROUP + flip(mask)
            wait_up(j, f)
            both_ways(lambda direction: line_up(j, direction, f))
        return carry

    lax.fori_loop(0, blocks, own_plane, 0)

    for mask in others:
        here = edge_slot(flip(mask) + 1)
        remote(here, here, sem_edge.at[0, mask], sem_edge.at[1, mask], (me, 1 - core)).wait_recv()

    @pl.when(has_up)
    def _():
        edge_next.start()

    low_half = (z < half).astype(jnp.int32)

    def plane_of(step):
        distance = (step + 1) // 2
        below = (step + low_half) % 2
        return z + distance * (1 - 2 * below), below

    def relay_one(copy_of, wait_of, below, f):
        wait_of(f)

        @pl.when((below == 1) & has_up)
        def _():
            copy_of(0, f).start()

        @pl.when((below == 0) & has_down)
        def _():
            copy_of(1, f).start()

    def relay(copy_of, wait_of, step):
        q, below = plane_of(step)

        @pl.when((q >= 0) & (q < planes))
        def _():
            def one(i, carry):
                relay_one(copy_of, wait_of, below, q * GROUP + i)
                return carry

            lax.fori_loop(0, GROUP, one, 0)

    def relay_up(j, first, last):
        def one(step, carry):
            relay(lambda direction, f: line_up(j, direction, f), lambda f: wait_up(j, f), step)
            return carry

        lax.fori_loop(first, last, one, 0)

    def wide(j):
        return pl.ds(pl.multiple_of(j * 256, 256), 256)

    def unit(owner, j):
        rows = pl.ds(pl.multiple_of(owner * rows_own, rows_own), rows_own)
        raw = jnp.dot(tok[rows, :], up_all[j], preferred_element_type=jnp.float32)
        taps[8:, :] = (raw * par[0:1, wide(j)]).astype(jnp.bfloat16).astype(jnp.float32)
        taps[0:8, :] = edge_pre[j, pl.ds(pl.multiple_of(owner * EDGE + EDGE - 8, 8), 8), :]
        conv = par[4:5, wide(j)] + par[3:4, wide(j)] * taps[8 : 8 + rows_own, :]
        conv = conv + par[2:3, wide(j)] * taps[7 : 7 + rows_own, :]
        conv = conv + par[1:2, wide(j)] * taps[6 : 6 + rows_own, :]
        g, v = conv[:, :128], conv[:, 128:]
        act = 0.5 * g * (1.0 + jnp.tanh(math.sqrt(2.0 / math.pi) * (g + 0.044715 * (g * g * g))))
        hidden[rows, pl.ds(pl.multiple_of(j * 128, 128), 128)] = (act * v).astype(jnp.bfloat16)

    def landed(mask, part):
        here = token_rows(flip(mask), core, part)
        remote(here, here, sem_tok_send.at[mask, part], sem_tok_recv.at[mask, part], (me, 1 - core)).wait_recv()

    def pair_landed(mask, part):
        there = token_rows(flip(mask), 1 - core, part)
        remote(
            there, there, sem_tok_pair_send.at[mask, part], sem_tok_pair_recv.at[mask, part], (me, 1 - core)
        ).wait_recv()

    def pass_tokens(part):
        for mask in (1, 2):
            landed(mask, part)
            token_relay(mask, part).start()
            token_pair(mask, part).start()

    def near_round(j, carry):
        relay_up(j, 1, 3)
        return carry

    lax.fori_loop(0, blocks, near_round, 0)

    part_rounds = (0, max(0, blocks - 2))

    def far_round(j, carry):
        relay_up(j, 3, 5)
        for part in range(parts):

            @pl.when(j == part_rounds[part])
            def _():
                pass_tokens(part)

        return carry

    lax.fori_loop(0, blocks, far_round, 0)

    own_down.wait()
    both_ways(lambda direction: line_down(direction, me, wd.at[p]))
    for mask in others:
        f = z * GROUP + flip(mask)
        wait_down(f)
        both_ways(lambda direction: line_down(direction, f))

    @pl.when(has_down)
    def _():
        here = edge_slot(0)
        remote(here, here, sem_edge.at[0, 0], sem_edge.at[1, 0], (me, 1 - core)).wait_recv()

    diag_round = jnp.where(inner_plane, blocks - 1, min(2, blocks - 1))

    def up_round(j, carry):
        relay_up(j, 5, 2 * planes - 1)
        own_up(j).wait()
        ahead = jnp.dot(edge[0 : GROUP * EDGE, :], up_all[j], preferred_element_type=jnp.float32)
        edge_pre[j] = (ahead * par[0:1, wide(j)]).astype(jnp.bfloat16).astype(jnp.float32)

        def group(mask, inner):
            ready = jnp.where(mask == 3, diag_round, 0)

            @pl.when((mask == 3) & (j == ready))
            def _():
                for part in range(parts):
                    for which in (0, 1):
                        here = diag_part(flip(3), part, which)
                        remote(
                            here,
                            here,
                            sem_diag_send.at[which + 1, part],
                            sem_diag_recv.at[which + 1, part],
                            (me, 1 - core),
                        ).wait_recv()
                    token_pair(3, part).start()

            @pl.when((mask > 0) & (j == ready))
            def _():
                for part in range(parts):
                    pair_landed(mask, part)

            first = jnp.where(j == ready, 0, j)
            last = jnp.where(j >= ready, j + 1, 0)

            def one(k, deeper):
                unit(flip(mask), k)
                return deeper

            return lax.fori_loop(first, last, one, inner)

        return lax.fori_loop(0, GROUP, group, carry)

    lax.fori_loop(0, blocks, up_round, 0)

    def block_rows(owner):
        return pl.ds(pl.multiple_of(owner * rows_own, rows_own), rows_own)

    strip = 2 * out_piece
    strips = chunk // strip
    per_core = half * strips

    def pair_copy(c, owner):
        return remote(
            stage.at[c, owner],
            pair_in.at[c % per_core, owner],
            sem_pair_send.at[c % per_core, owner],
            sem_pair_recv.at[c % per_core, owner],
            (me, 1 - core),
        )

    half_rows = rows_own // 2

    def half_of(which):
        return pl.ds(which * half_rows, half_rows)

    def peer_copy(c, mask, which):
        slot = (mask - 1) * 2 + which
        return remote(
            stage.at[c, flip(mask), half_of(which)],
            peer_in.at[c % per_core, mask - 1, half_of(which)],
            sem_peer_send.at[c % per_core, slot],
            sem_peer_recv.at[c % per_core, slot],
            chip(flip(mask)),
        )

    def relay_copy(c, mask):
        return remote(
            stage.at[c, flip(3), half_of(mask - 1)],
            relay_in.at[c % per_core, mask - 1],
            sem_relay_send.at[c % per_core, mask - 1],
            sem_relay_recv.at[c % per_core, mask - 1],
            chip(flip(mask)),
        )

    def combine(c, owner):
        pair_copy(c, owner).wait_recv()
        both = stage[c, owner].astype(jnp.float32) + pair_in[c % per_core, owner].astype(jnp.float32)
        stage[c, owner] = both.astype(jnp.bfloat16)

    def send_out(c):
        combine(c, flip(3))
        for mask in (1, 2):
            relay_copy(c, mask).start()
        for mask in (1, 2):
            combine(c, flip(mask))
            peer_copy(c, mask, mask - 1).start()
        combine(c, p)

    def pass_on(c):
        for mask in (1, 2):
            relay_copy(c, mask).wait_recv()
            owner = flip(3 - mask)
            rows = half_of(mask - 1)
            total = stage[c, owner, rows, :].astype(jnp.float32) + relay_in[c % per_core, mask - 1].astype(jnp.float32)
            stage[c, owner, rows, :] = total.astype(jnp.bfloat16)
            peer_copy(c, 3 - mask, mask - 1).start()

    def mine(c):
        return c // per_core == core

    def down_relay(step, carry):
        relay(line_down, wait_down, step)
        return carry

    def down_step(n, before):
        step = n // strips
        q, below = plane_of(step)
        valid = (q >= 0) & (q < planes)
        c = q * strips + n % strips
        patient = inner_plane | (step == 0)
        owed = before >= 0

        @pl.when((n == strips) & inner_plane)
        def _():
            lax.fori_loop(1, 2 * planes - 1, down_relay, 0)

        @pl.when(valid & owed & jnp.logical_not(patient))
        def _():
            pass_on(before)

        @pl.when(valid & (step > 0) & jnp.logical_not(inner_plane))
        def _():
            for i in range(GROUP // strips):
                relay_one(line_down, wait_down, below, q * GROUP + n % strips * (GROUP // strips) + i)

        @pl.when(valid)
        def _():
            cols = pl.ds(pl.multiple_of(n % strips * strip, strip), strip)

            def product(i, inner):
                owner = flip(3 - i)
                value = jnp.dot(
                    hidden[block_rows(owner), :], down_all[q, :, cols], preferred_element_type=jnp.float32
                )
                stage[c, owner] = value.astype(jnp.bfloat16)

                @pl.when(jnp.logical_not(mine(c)))
                def _():
                    pair_copy(c, owner).start()

                return inner

            lax.fori_loop(0, GROUP, product, 0)

            @pl.when(mine(c))
            def _():
                send_out(c)

        @pl.when(valid & owed & patient)
        def _():
            pass_on(before)

        return jnp.where(valid, jnp.where(mine(c), c, -1), before)

    last = lax.fori_loop(0, (2 * planes - 1) * strips, down_step, -1)

    @pl.when(last >= 0)
    def _():
        pass_on(last)

    def finish(i, carry):
        c = core * per_core + i
        total = stage[c, p].astype(jnp.float32)
        for mask in (1, 2):
            for which in (0, 1):
                peer_copy(c, mask, which).wait_recv()
            total = total + peer_in[i, mask - 1].astype(jnp.float32)
        cols = pl.ds(pl.multiple_of(i * strip, strip), strip)
        out[:, cols] = (total * osc[0:1, cols]).astype(jnp.bfloat16)
        return carry

    lax.fori_loop(0, per_core, finish, 0)

    def drain_out(i, carry):
        for mask in (1, 2):
            relay_copy(core * per_core + i, mask).wait_send()
            for which in (0, 1):
                peer_copy(core * per_core + i, mask, which).wait_send()

        def one(owner, inner):
            pair_copy((1 - core) * per_core + i, owner).wait_send()
            return inner

        return lax.fori_loop(0, GROUP, one, carry)

    lax.fori_loop(0, per_core, drain_out, 0)
    for part in range(parts):
        for mask in (1, 2):
            token_copy(mask, part).wait_send()
            token_relay(mask, part).wait_send()
        for mask in others:
            token_pair(mask, part).wait_send()
    for mask in others:
        edge_copy(mask).wait_send()
        plane_down(mask).wait_send()

    @pl.when(has_up)
    def _():
        edge_next.wait_send()

    def drain_plane(j, carry):
        for mask in others:
            plane_up(j, mask).wait_send()
        return carry

    lax.fori_loop(0, blocks, drain_plane, 0)

    def drain_line(f, carry):
        def drain_way(direction, sent):
            @pl.when(sent)
            def _():
                def one(j, inner):
                    line_up(j, direction, f).wait_send()
                    return inner

                lax.fori_loop(0, blocks, one, 0)
                line_down(direction, f).wait_send()

        drain_way(0, has_up & (f // GROUP <= z))
        drain_way(1, has_down & (f // GROUP >= z))
        return carry

    lax.fori_loop(0, planes * GROUP, drain_line, 0)


def grouped_body(count, tokens, norm_gain, gate_weight, value_weight, gate_scale, value_scale, gate_kernel, value_kernel, gate_bias, value_bias, down_weight, down_scale):
    planes = count // GROUP
    half = planes // 2
    rows, width = tokens.shape
    piece, local = gate_weight.shape
    out_piece = down_weight.shape[1]
    units = local // GROUP
    blocks = units // 128
    chunk = GROUP * out_piece
    strip = 2 * out_piece
    strips = chunk // strip
    per_core = half * strips
    dma = pltpu.SemaphoreType.DMA
    bf16, f32 = jnp.bfloat16, jnp.float32
    vmem = pl.BlockSpec(memory_space=pltpu.VMEM)
    hbm = pl.BlockSpec(memory_space=pl.ANY)
    return pl.pallas_call(
        functools.partial(fused_kernel, planes),
        out_shape=jax.ShapeDtypeStruct((rows, half * chunk), bf16),
        in_specs=[hbm] * 4 + [vmem] * 8,
        out_specs=vmem,
        scratch_shapes=[
            pltpu.VMEM((GROUP * rows, width), bf16),
            pltpu.VMEM((blocks, width, 256), bf16),
            pltpu.VMEM((planes, units, chunk), bf16),
            pltpu.VMEM((GROUP * rows, units), bf16),
            pltpu.VMEM((2 * per_core, GROUP, rows, strip), bf16),
            pltpu.VMEM((per_core, GROUP, rows, strip), bf16),
            pltpu.VMEM((per_core, 2, rows, strip), bf16),
            pltpu.VMEM((per_core, 2, rows // 2, strip), bf16),
            pltpu.VMEM((rows + 8, 256), f32),
            pltpu.VMEM(((GROUP + 1) * EDGE, width), bf16),
            pltpu.VMEM((blocks, GROUP * EDGE, 256), f32),
            pltpu.VMEM((8, 2 * units), f32),
            pltpu.VMEM((GROUP, blocks, piece, 256), bf16),
            pltpu.VMEM((GROUP, units, out_piece), bf16),
            pltpu.VMEM((rows, width), bf16),
            pltpu.VMEM((piece, local), f32),
            pltpu.VMEM((piece, local), f32),
            pltpu.VMEM((local, out_piece), f32),
            dma((4,)),
            dma((blocks + 1,)),
            dma((blocks + 1, GROUP)),
            dma((blocks + 1, count)),
            dma((blocks + 1, 2, count)),
            dma((2, GROUP)),
            dma((GROUP, 2)),
            dma((GROUP, 2)),
            dma((GROUP, 2)),
            dma((GROUP, 2)),
            dma((GROUP, 2)),
            dma((GROUP, 2)),
            dma((per_core, GROUP)),
            dma((per_core, GROUP)),
            dma((per_core, 4)),
            dma((per_core, 4)),
            dma((per_core, 2)),
            dma((per_core, 2)),
        ],
        compiler_params=pltpu.CompilerParams(
            collective_id=0, has_side_effects=True, vmem_limit_bytes=67043328
        ),
    )(
        tokens,
        gate_weight,
        value_weight,
        down_weight,
        norm_gain[None, :],
        gate_scale.reshape(-1, 128),
        value_scale.reshape(-1, 128),
        gate_kernel,
        value_kernel,
        gate_bias.reshape(-1, 128),
        value_bias.reshape(-1, 128),
        down_scale[None, :],
    )


def solution(mesh):
    count, tp = mesh.shape["fs"], mesh.shape["tp"]

    def whole(*arrays):
        local = arrays[2].shape[1]
        fits = tp == 2 and count % (2 * GROUP) == 0 and local % (GROUP * 128) == 0
        if fits:
            return grouped_body(count, *arrays)
        return body(*arrays)

    return jax.shard_map(
        whole,
        mesh=mesh,
        in_specs=(
            P("fs", None),
            P(),
            P("fs", "tp"),
            P("fs", "tp"),
            P("tp"),
            P("tp"),
            P(None, "tp"),
            P(None, "tp"),
            P("tp"),
            P("tp"),
            P("tp", "fs"),
            P("tp"),
        ),
        out_specs=P("fs", "tp"),
        check_vma=False,
    )
```

```python
import functools
import math

import jax
import jax.numpy as jnp
from jax import lax
from jax.experimental import pallas as pl
from jax.experimental.pallas import tpu as pltpu
from jax.sharding import PartitionSpec as P

epsilon = 1e-06


def from_behind(value, axis, steps):
    count = lax.axis_size(axis)
    leading, last = (max(0, -steps), min(count, count - steps))
    return lax.ppermute(value, axis, [(source, source + steps) for source in range(leading, last)])


def normalize(tokens, norm_gain):
    values = tokens.astype(jnp.float32)
    scaled = values * lax.rsqrt(jnp.mean(values * values, axis=1, keepdims=True) + epsilon)
    return (scaled * norm_gain[None, :]).astype(jnp.bfloat16)


def causal_mix(current, previous, kernel, tap_bias):
    row_count = current.shape[0]
    joined = jnp.concatenate([previous, current], axis=0).astype(jnp.float32)
    summed_taps = tap_bias[None, :] + kernel[2][None, :] * joined[2:]
    for back_by in (1, 2):
        summed_taps = (
            summed_taps
            + kernel[2 - back_by][None, :] * joined[2 - back_by : 2 - back_by + row_count]
        )
    return summed_taps


def body(
    tokens,
    norm_gain,
    gate_weight,
    value_weight,
    gate_scale,
    value_scale,
    gate_kernel,
    value_kernel,
    gate_bias,
    value_bias,
    down_weight,
    down_scale,
):
    normed = normalize(tokens, norm_gain)
    gate_low = gate_weight.astype(jnp.bfloat16)
    value_low = value_weight.astype(jnp.bfloat16)
    down_low = down_weight.astype(jnp.bfloat16)
    row_count = normed.shape[0]
    gate_full, value_full, down_full = (
        lax.all_gather(gate_low, "fs", axis=0, tiled=True),
        lax.all_gather(value_low, "fs", axis=0, tiled=True),
        lax.all_gather(down_low, "fs", axis=1, tiled=True),
    )
    gate_raw = jnp.dot(normed, gate_full, preferred_element_type=jnp.float32)
    value_raw = jnp.dot(normed, value_full, preferred_element_type=jnp.float32)
    gate_pre = (gate_raw * gate_scale[None, :]).astype(jnp.bfloat16)
    value_pre = (value_raw * value_scale[None, :]).astype(jnp.bfloat16)
    previous_gate, previous_value = from_behind(
        (gate_pre[row_count - 2 :], value_pre[row_count - 2 :]), "fs", 1
    )
    gate_conv = causal_mix(gate_pre, previous_gate, gate_kernel, gate_bias)
    value_conv = causal_mix(value_pre, previous_value, value_kernel, value_bias)
    hidden = (jax.nn.gelu(gate_conv, approximate=True) * value_conv).astype(jnp.bfloat16)
    partial_terms = jnp.dot(hidden, down_full, preferred_element_type=jnp.float32)
    summed = lax.psum_scatter(
        partial_terms.astype(jnp.bfloat16), "tp", scatter_dimension=1, tiled=True
    ).astype(jnp.float32)
    return (summed * down_scale[None, :]).astype(jnp.bfloat16)


MESH = pl.DeviceIdType.MESH
GROUP = 4
EDGE = 16


def fused_kernel(
    depth_planes,
    tok_hbm,
    gate_hbm,
    value_hbm,
    down_hbm,
    gain,
    gate_scale,
    value_scale,
    gate_kernel,
    value_kernel,
    gate_bias,
    value_bias,
    osc,
    out,
    tok,
    up_all,
    down_all,
    hidden,
    stage,
    pair_in,
    peer_in,
    relay_in,
    taps,
    edge,
    edge_pre,
    par,
    wu,
    wd,
    raw_tok,
    raw_gate,
    raw_value,
    raw_down,
    sem_fetch,
    sem_own,
    sem_plane_send,
    sem_plane_recv,
    sem_first_send,
    sem_first_recv,
    sem_piece_send,
    sem_piece_recv,
    sem_far_send,
    sem_far_recv,
    sem_down_send,
    sem_down_recv,
    sem_edge,
    sem_tok_send,
    sem_tok_recv,
    sem_diag_send,
    sem_diag_recv,
    sem_tok_pair_send,
    sem_tok_pair_recv,
    sem_pair_send,
    sem_pair_recv,
    sem_peer_send,
    sem_peer_recv,
    sem_relay_send,
    sem_relay_recv,
):
    planes = depth_planes
    half = planes // 2
    me = lax.axis_index("fs")
    core = lax.axis_index("tp")
    z, p = me // GROUP, me % GROUP
    rows_own = raw_tok.shape[0]
    part_rows = rows_own // 2
    blocks, piece = wu.shape[1], wu.shape[2]
    units = hidden.shape[1]
    out_piece = wd.shape[2]
    chunk = GROUP * out_piece
    has_up, has_down = z < planes - 1, z > 0
    inner_plane = has_up & has_down
    end_plane = jnp.logical_not(inner_plane)
    cut = min(2, blocks - 1)
    groups = ((0, cut), (cut, blocks))

    def flip(mask):
        px, py = p % 2, p // 2
        return (py + mask // 2) % 2 * 2 + (px + mask % 2) % 2

    def chip(target):
        return (z * GROUP + target, core)

    others = (1, 2, 3)

    fetches = [
        pltpu.make_async_copy(src, dst, sem_fetch.at[i])
        for i, (src, dst) in enumerate(
            ((gate_hbm, raw_gate), (value_hbm, raw_value), (tok_hbm, raw_tok), (down_hbm, raw_down))
        )
    ]
    for fetch in fetches:
        fetch.start()

    barrier = pltpu.get_barrier_semaphore()
    for mask in others:
        pl.semaphore_signal(barrier, inc=1, device_id=chip(flip(mask)), device_id_type=MESH)
    pl.semaphore_signal(barrier, inc=1, device_id=(me, 1 - core), device_id_type=MESH)

    @pl.when(has_up)
    def _():
        pl.semaphore_signal(barrier, inc=1, device_id=(me + GROUP, core), device_id_type=MESH)

    @pl.when(has_down)
    def _():
        pl.semaphore_signal(barrier, inc=1, device_id=(me - GROUP, core), device_id_type=MESH)

    def remote(src, dst, send, recv, device):
        return pltpu.make_async_remote_copy(
            src_ref=src, dst_ref=dst, send_sem=send, recv_sem=recv, device_id=device, device_id_type=MESH
        )

    def rows_of(f, count=1):
        return pl.ds(pl.multiple_of(f * piece, piece), count * piece)

    def down_block(f):
        return down_all.at[f // GROUP, :, pl.ds(pl.multiple_of(f % GROUP * out_piece, out_piece), out_piece)]

    def line(side):
        return (me + (GROUP if side == 0 else -GROUP), core)

    def plane_up(g, mask):
        first, last = groups[g]
        return remote(
            wu.at[flip(mask), first:last],
            up_all.at[first:last, rows_of(me), :],
            sem_plane_send.at[g, mask],
            sem_plane_recv.at[g, mask],
            chip(flip(mask)),
        )

    def plane_up_landed(g, mask):
        first, last = groups[g]
        here = up_all.at[first:last, rows_of(z * GROUP + flip(mask)), :]
        remote(here, here, sem_plane_send.at[g, mask], sem_plane_recv.at[g, mask], chip(flip(mask))).wait_recv()

    def first_hop(side, g, mask):
        first, last = groups[g]
        there = up_all.at[first:last, rows_of(z * GROUP + flip(mask)), :]
        here = there if mask else wu.at[p, first:last]
        return remote(here, there, sem_first_send.at[side, g, mask], sem_first_recv.at[side, g, mask], line(side))

    def first_landed(side, g, mask):
        first, last = groups[g]
        q = z + (2 * side - 1)
        here = up_all.at[first:last, rows_of(q * GROUP + flip(mask)), :]
        remote(
            here, here, sem_first_send.at[side, g, mask], sem_first_recv.at[side, g, mask], (me, 1 - core)
        ).wait_recv()

    def piece_hop(side, mask):
        here = up_all.at[:, rows_of((z + (2 * side - 1)) * GROUP + flip(mask)), :]
        return remote(here, here, sem_piece_send.at[mask], sem_piece_recv.at[mask], line(side))

    def piece_landed(side, mask):
        here = up_all.at[:, rows_of((z + 2 * (2 * side - 1)) * GROUP + flip(mask)), :]
        remote(here, here, sem_piece_send.at[mask], sem_piece_recv.at[mask], (me, 1 - core)).wait_recv()

    def far_hop(side, distance, j):
        q = z + distance * (2 * side - 1)
        here = up_all.at[j, rows_of(q * GROUP, GROUP), :]
        return remote(
            here, here, sem_far_send.at[side, distance - 1, j], sem_far_recv.at[side, distance - 1, j], line(side)
        )

    def far_landed(side, distance, j):
        q = z + distance * (2 * side - 1)
        here = up_all.at[j, rows_of(q * GROUP, GROUP), :]
        remote(
            here, here, sem_far_send.at[side, distance - 2, j], sem_far_recv.at[side, distance - 2, j], (me, 1 - core)
        ).wait_recv()

    def plane_down(mask):
        return remote(
            wd.at[flip(mask)],
            down_block(me),
            sem_plane_send.at[2, mask],
            sem_down_recv.at[me],
            chip(flip(mask)),
        )

    def line_down(side, f, slot, src=None):
        here = down_block(f)
        return remote(
            here if src is None else src, here, sem_down_send.at[slot], sem_down_recv.at[f], line(side)
        )

    def wait_down(f):
        here = down_block(f)
        remote(here, here, sem_down_send.at[f], sem_down_recv.at[f], (me, 1 - core)).wait_recv()

    def both_ways(copy_of):
        @pl.when(has_up)
        def _():
            copy_of(0).start()

        @pl.when(has_down)
        def _():
            copy_of(1).start()

    own_up = pltpu.make_async_copy(wu.at[p], up_all.at[:, rows_of(me), :], sem_own.at[0])
    own_down = pltpu.make_async_copy(wd.at[p], down_block(me), sem_own.at[1])

    def cast_block(j):
        for m in range(GROUP):
            first = m * units + j * 128
            wu[m, j, :, 0:128] = raw_gate[:, first : first + 128].astype(jnp.bfloat16)
            wu[m, j, :, 128:256] = raw_value[:, first : first + 128].astype(jnp.bfloat16)

    def normed(first, count):
        values = raw_tok[pl.ds(first, count), :].astype(jnp.float32)
        scaled = values * lax.rsqrt(jnp.mean(values * values, axis=1, keepdims=True) + epsilon)
        return (scaled * gain[...]).astype(jnp.bfloat16)

    fetches[0].wait()
    fetches[1].wait()
    for j in range(blocks):
        cast_block(j)
    pl.semaphore_wait(barrier, 4 + has_up.astype(jnp.int32) + has_down.astype(jnp.int32))
    for g in range(2):
        for mask in others:
            plane_up(g, mask).start()
        both_ways(lambda side: first_hop(side, g, 0))
    own_up.start()

    def edge_slot(slot):
        return edge.at[pl.ds(pl.multiple_of(slot * EDGE, EDGE), EDGE), :]

    def edge_copy(mask):
        here = edge_slot(p + 1)
        return remote(here, here, sem_edge.at[0, mask], sem_edge.at[1, mask], chip(flip(mask)))

    edge_next = remote(
        edge_slot(GROUP), edge_slot(0), sem_edge.at[0, 0], sem_edge.at[1, 0], (me + GROUP, core)
    )

    @pl.when(jnp.logical_not(has_down))
    def _():
        edge[0:EDGE, :] = jnp.zeros_like(edge[0:EDGE, :])

    fetches[2].wait()
    edge[pl.ds(pl.multiple_of((p + 1) * EDGE, EDGE), EDGE), :] = normed(rows_own - EDGE, EDGE)
    for mask in others:
        edge_copy(mask).start()
    norm_tile = 64

    def norm_step(i, carry):
        first = pl.multiple_of(i * norm_tile, norm_tile)
        tok[pl.ds(pl.multiple_of(p * rows_own + i * norm_tile, norm_tile), norm_tile), :] = normed(first, norm_tile)
        return carry

    lax.fori_loop(0, rows_own // norm_tile, norm_step, 0)

    parts = 2
    sub_rows = part_rows // parts
    diag_rows = sub_rows // 2

    def token_rows(owner, side, part):
        start = owner * rows_own + side * part_rows + part * sub_rows
        return tok.at[pl.ds(pl.multiple_of(start, sub_rows), sub_rows), :]

    def diag_part(owner, part, which):
        start = owner * rows_own + core * part_rows + part * sub_rows + which * diag_rows
        return tok.at[pl.ds(pl.multiple_of(start, diag_rows), diag_rows), :]

    def token_copy(mask, part):
        here = token_rows(p, core, part)
        return remote(here, here, sem_tok_send.at[mask - 1, part], sem_tok_recv.at[mask - 1, part], chip(flip(mask)))

    def token_relay(mask, part):
        here = diag_part(flip(mask), part, mask - 1)
        return remote(
            here,
            here,
            sem_diag_send.at[mask - 1, part],
            sem_diag_recv.at[mask - 1, part],
            chip(flip(3 - mask)),
        )

    def token_pair(mask, part):
        here = token_rows(flip(mask), core, part)
        return remote(
            here, here, sem_tok_pair_send.at[mask - 1, part], sem_tok_pair_recv.at[mask - 1, part], (me, 1 - core)
        )

    for part in range(parts):
        for mask in (1, 2):
            token_copy(mask, part).start()

    fetches[3].wait()
    for m in range(GROUP):
        wd[m] = raw_down[m * units : (m + 1) * units, :].astype(jnp.bfloat16)
    own_down.start()
    for j in range(blocks):
        src = pl.ds(p * blocks + j, 1)
        cols = pl.ds(pl.multiple_of(p * units + j * 128, 128), 128)
        for side, (scale, kernel, tap_bias) in enumerate(
            ((gate_scale, gate_kernel, gate_bias), (value_scale, value_kernel, value_bias))
        ):
            dst = slice(j * 256 + side * 128, j * 256 + side * 128 + 128)
            par[1:4, dst] = kernel[0:3, cols] * scale[src, :]
            par[4:5, dst] = tap_bias[src, :]

    for g in range(2):
        for mask in others:
            plane_up_landed(g, mask)
            both_ways(lambda side: first_hop(side, g, mask))

    for mask in others:
        here = edge_slot(flip(mask) + 1)
        remote(here, here, sem_edge.at[0, mask], sem_edge.at[1, mask], (me, 1 - core)).wait_recv()

    @pl.when(has_up)
    def _():
        edge_next.start()

    low_half = (z < half).astype(jnp.int32)

    def plane_of(step):
        distance = (step + 1) // 2
        below = (step + low_half) % 2
        return z + distance * (1 - 2 * below), below

    def wide(j):
        return pl.ds(pl.multiple_of(j * 256, 256), 256)

    def unit(owner, j):
        rows = pl.ds(pl.multiple_of(owner * rows_own, rows_own), rows_own)
        taps[8:, :] = jnp.dot(tok[rows, :], up_all[j], preferred_element_type=jnp.float32)
        taps[0:8, :] = edge_pre[j, pl.ds(pl.multiple_of(owner * EDGE + EDGE - 8, 8), 8), :]
        conv = par[4:5, wide(j)] + par[3:4, wide(j)] * taps[8 : 8 + rows_own, :]
        conv = conv + par[2:3, wide(j)] * taps[7 : 7 + rows_own, :]
        conv = conv + par[1:2, wide(j)] * taps[6 : 6 + rows_own, :]
        g, v = conv[:, :128], conv[:, 128:]
        root = math.sqrt(2.0 / math.pi)
        bend = jnp.tanh(g * (root + (root * 0.044715) * (g * g)))
        hidden[rows, pl.ds(pl.multiple_of(j * 128, 128), 128)] = ((0.5 * (g * v)) * (1.0 + bend)).astype(jnp.bfloat16)

    def landed(mask, part):
        here = token_rows(flip(mask), core, part)
        remote(here, here, sem_tok_send.at[mask - 1, part], sem_tok_recv.at[mask - 1, part], (me, 1 - core)).wait_recv()

    def pair_landed(mask, part):
        there = token_rows(flip(mask), 1 - core, part)
        remote(
            there, there, sem_tok_pair_send.at[mask - 1, part], sem_tok_pair_recv.at[mask - 1, part], (me, 1 - core)
        ).wait_recv()

    def pass_tokens(part):
        for mask in (1, 2):
            landed(mask, part)
            token_relay(mask, part).start()
            token_pair(mask, part).start()

    def near(side):
        def pieces():
            for mask in range(GROUP):
                for g in range(2):
                    first_landed(side, g, mask)
                piece_hop(side, mask).start()

        def whole():
            for mask in range(GROUP):
                for g in range(2):
                    first_landed(side, g, mask)

        onward = z + (1 - 2 * side)
        into_end = onward == (planes - 1 if side == 0 else 0)

        @pl.when(inner_plane & into_end)
        def _():
            pieces()

        @pl.when(inner_plane & jnp.logical_not(into_end))
        def _():
            whole()

            def one(j, carry):
                far_hop(side, 1, j).start()
                return carry

            lax.fori_loop(0, blocks, one, 0)

        @pl.when(end_plane & (has_down if side == 0 else has_up))
        def _():
            whole()

    @pl.when(low_half == 1)
    def _():
        near(1)
        near(0)

    @pl.when(low_half == 0)
    def _():
        near(0)
        near(1)

    pass_tokens(0)

    def send_down():
        for mask in others:
            plane_down(mask).start()

    def pass_rest():
        pass_tokens(parts - 1)
        send_down()

    @pl.when(end_plane)
    def _():
        for mask in range(GROUP):
            for side in (0, 1):

                @pl.when((z >= 2) if side == 0 else (z < planes - 2))
                def _():
                    piece_landed(side, mask)

            if mask == GROUP - 2:
                pass_rest()

    @pl.when(has_down)
    def _():
        here = edge_slot(0)
        remote(here, here, sem_edge.at[0, 0], sem_edge.at[1, 0], (me, 1 - core)).wait_recv()

    own_up.wait()
    own_down.wait()

    def edge_block(j):
        ahead = jnp.dot(edge[0 : GROUP * EDGE, :], up_all[j], preferred_element_type=jnp.float32)
        edge_pre[j] = ahead

    def far_round(j, carry):
        @pl.when(inner_plane)
        def _():
            for distance in range(2, planes - 1):
                for side in (0, 1):

                    @pl.when((z >= distance) if side == 0 else (z < planes - distance))
                    def _():
                        far_landed(side, distance, j)
                        far_hop(side, distance, j).start()

            @pl.when(j == max(0, blocks - 2))
            def _():
                pass_rest()

        return carry

    lax.fori_loop(0, blocks, far_round, 0)

    def block_rows(owner):
        return pl.ds(pl.multiple_of(owner * rows_own, rows_own), rows_own)

    strip = 2 * out_piece
    strips = chunk // strip
    per_core = half * strips

    def pair_copy(c, owner):
        return remote(
            stage.at[c, owner],
            pair_in.at[c % per_core, owner],
            sem_pair_send.at[c % per_core, owner],
            sem_pair_recv.at[c % per_core, owner],
            (me, 1 - core),
        )

    half_rows = rows_own // 2

    def half_of(which):
        return pl.ds(pl.multiple_of(which * half_rows, half_rows), half_rows)

    def peer_copy(c, mask, which):
        slot = (mask - 1) * 2 + which
        return remote(
            stage.at[c, flip(mask), half_of(which)],
            peer_in.at[c % per_core, mask - 1, half_of(which)],
            sem_peer_send.at[c % per_core, slot],
            sem_peer_recv.at[c % per_core, slot],
            chip(flip(mask)),
        )

    def relay_copy(c, mask):
        return remote(
            stage.at[c, flip(3), half_of(mask - 1)],
            relay_in.at[c % per_core, mask - 1],
            sem_relay_send.at[c % per_core, mask - 1],
            sem_relay_recv.at[c % per_core, mask - 1],
            chip(flip(mask)),
        )

    def combine(c, owner):
        pair_copy(c, owner).wait_recv()
        both = stage[c, owner].astype(jnp.float32) + pair_in[c % per_core, owner].astype(jnp.float32)
        stage[c, owner] = both.astype(jnp.bfloat16)

    def product(c, owner):
        first = pl.multiple_of(c % strips * strip, strip)
        value = jnp.dot(
            hidden[block_rows(owner), :], down_all[c // strips, :, pl.ds(first, strip)], preferred_element_type=jnp.float32
        )
        stage[c, owner] = value.astype(jnp.bfloat16)

        @pl.when(jnp.logical_not(mine(c)))
        def _():
            pair_copy(c, owner).start()

    def send_out(c, mask):
        combine(c, flip(mask))

        @pl.when(mask == 3)
        def _():
            for way in (1, 2):
                relay_copy(c, way).start()

        @pl.when((mask == 1) | (mask == 2))
        def _():
            peer_copy(c, mask, mask - 1).start()

    def pass_on(c):
        for mask in (1, 2):
            relay_copy(c, mask).wait_recv()
            owner = flip(3 - mask)
            rows = half_of(mask - 1)
            total = stage[c, owner, rows, :].astype(jnp.float32) + relay_in[c % per_core, mask - 1].astype(jnp.float32)
            stage[c, owner, rows, :] = total.astype(jnp.bfloat16)
            peer_copy(c, 3 - mask, mask - 1).start()

    def mine(c):
        return c // per_core == core

    def own_down_out():
        both_ways(lambda side: line_down(side, me, me if side == 0 else planes * GROUP + p, wd.at[p]))
        for mask in others:
            f = z * GROUP + flip(mask)
            wait_down(f)
            both_ways(lambda side: line_down(side, f, f if side == 0 else planes * GROUP + flip(mask)))

    diag_round = jnp.where(inner_plane, blocks - 1, min(2, blocks - 1))

    def up_round(j, carry):
        @pl.when(end_plane)
        def _():
            for distance in range(3, planes):
                for side in (0, 1):

                    @pl.when((z >= distance) if side == 0 else (z < planes - distance))
                    def _():
                        far_landed(side, distance, j)

        edge_block(j)

        @pl.when(j == diag_round)
        def _():
            for part in range(parts):
                for which in (0, 1):
                    here = diag_part(flip(3), part, which)
                    remote(
                        here,
                        here,
                        sem_diag_send.at[which, part],
                        sem_diag_recv.at[which, part],
                        (me, 1 - core),
                    ).wait_recv()
                token_pair(3, part).start()

        final = j == blocks - 1

        def group(i, inner):
            mask = jnp.where(final, 3 - i, i)
            ready = jnp.where(mask == 3, diag_round, 0)

            @pl.when((mask == 3) & (j == diag_round))
            def _():
                own_down_out()

            @pl.when((mask > 0) & (j == ready))
            def _():
                for part in range(parts):
                    pair_landed(mask, part)

            first = jnp.where(j == ready, 0, j)
            last = jnp.where(j >= ready, j + 1, 0)

            def one(k, deeper):
                unit(flip(mask), k)
                return deeper

            lax.fori_loop(first, last, one, inner)

            @pl.when(final)
            def _():
                for n in range(strips):
                    product(z * strips + n, flip(mask))

                @pl.when(mine(z * strips) & (i > 0))
                def _():
                    for n in range(strips):
                        send_out(z * strips + n, mask + 1)

            return inner

        return lax.fori_loop(0, GROUP, group, carry)

    lax.fori_loop(0, blocks, up_round, 0)

    @pl.when(mine(z * strips))
    def _():
        for n in range(strips):
            send_out(z * strips + n, 0)
        for n in range(strips - 1):
            pass_on(z * strips + n)

    def pass_plane(step):
        q, below = plane_of(step)

        @pl.when((q >= 0) & (q < planes))
        def _():
            def one(i, carry):
                f = q * GROUP + i
                wait_down(f)

                @pl.when((below == 1) & has_up)
                def _():
                    line_down(0, f, f).start()

                @pl.when((below == 0) & has_down)
                def _():
                    line_down(1, f, f).start()

                return carry

            lax.fori_loop(0, GROUP, one, 0)

    def drain_early():
        for part in range(parts):
            for mask in (1, 2):
                token_copy(mask, part).wait_send()
                token_relay(mask, part).wait_send()
            for mask in others:
                token_pair(mask, part).wait_send()
        for mask in others:
            edge_copy(mask).wait_send()
            plane_down(mask).wait_send()
            for g in range(2):
                plane_up(g, mask).wait_send()

        @pl.when(has_up)
        def _():
            edge_next.wait_send()

        for side in (0, 1):

            @pl.when(has_up if side == 0 else has_down)
            def _():
                for g in range(2):
                    for mask in range(GROUP):
                        first_hop(side, g, mask).wait_send()

            onward = z + (1 - 2 * side)
            into_end = onward == (planes - 1 if side == 0 else 0)

            @pl.when(inner_plane & into_end)
            def _():
                for mask in range(GROUP):
                    piece_hop(side, mask).wait_send()

            @pl.when(inner_plane)
            def _():
                for distance in range(1, planes - 1):
                    valid = (z >= distance) if side == 0 else (z < planes - distance)

                    @pl.when(valid & (jnp.logical_not(into_end) if distance == 1 else True))
                    def _():
                        def one(j, carry):
                            far_hop(side, distance, j).wait_send()
                            return carry

                        lax.fori_loop(0, blocks, one, 0)

    def down_step(n, before):
        step = n // strips
        q, below = plane_of(step)
        valid = (q >= 0) & (q < planes)
        c = q * strips + n % strips
        owed = before >= 0

        @pl.when((n == strips) & inner_plane)
        def _():
            pass_plane(1)
            pass_plane(2)

        @pl.when(n == 2 * strips)
        def _():
            drain_early()

        @pl.when((n == 2 * strips + 1) & inner_plane)
        def _():
            for later in range(3, 2 * planes - 1):
                pass_plane(later)

        @pl.when(valid & end_plane)
        def _():
            for i in range(GROUP // strips):
                wait_down(q * GROUP + n % strips * (GROUP // strips) + i)

        @pl.when(valid)
        def _():
            def one(i, inner):
                product(c, flip(3 - i))
                return inner

            lax.fori_loop(0, GROUP, one, 0)

            @pl.when(mine(c))
            def _():
                def one(i, inner):
                    send_out(c, 3 - i)
                    return inner

                lax.fori_loop(0, GROUP, one, 0)

        due = valid & owed & (mine(c) | (n % strips == strips - 1))

        @pl.when(due)
        def _():
            pass_on(before)

        return jnp.where(valid & mine(c), c, jnp.where(due, -1, before))

    first_owed = jnp.where(mine(z * strips), z * strips + strips - 1, -1)
    last = lax.fori_loop(strips, (2 * planes - 1) * strips, down_step, first_owed)

    def finish(c):
        i = c % per_core
        total = stage[c, p].astype(jnp.float32)
        for mask in (1, 2):
            for which in (0, 1):
                peer_copy(c, mask, which).wait_recv()
            total = total + peer_in[i, mask - 1].astype(jnp.float32)
        cols = pl.ds(pl.multiple_of(i * strip, strip), strip)
        out[:, cols] = (total * osc[0:1, cols]).astype(jnp.bfloat16)

    @pl.when(last >= 0)
    def _():
        pass_on(last)

    def finish_one(i, carry):
        finish(core * per_core + i)
        return carry

    lax.fori_loop(0, per_core, finish_one, 0)

    def drain_out(i, carry):
        for mask in (1, 2):
            relay_copy(core * per_core + i, mask).wait_send()
            for which in (0, 1):
                peer_copy(core * per_core + i, mask, which).wait_send()

        def one(owner, inner):
            pair_copy((1 - core) * per_core + i, owner).wait_send()
            return inner

        return lax.fori_loop(0, GROUP, one, carry)

    lax.fori_loop(0, per_core, drain_out, 0)

    for side in (0, 1):

        @pl.when(has_up if side == 0 else has_down)
        def _():
            for mask in range(GROUP):
                f = z * GROUP + flip(mask)
                line_down(side, f, f if side == 0 else planes * GROUP + flip(mask)).wait_send()

    @pl.when(inner_plane)
    def _():
        def drain_down(f, carry):
            @pl.when(f // GROUP < z)
            def _():
                line_down(0, f, f).wait_send()

            @pl.when(f // GROUP > z)
            def _():
                line_down(1, f, f).wait_send()

            return carry

        lax.fori_loop(0, planes * GROUP, drain_down, 0)


def grouped_body(count, tokens, norm_gain, gate_weight, value_weight, gate_scale, value_scale, gate_kernel, value_kernel, gate_bias, value_bias, down_weight, down_scale):
    planes = count // GROUP
    half = planes // 2
    rows, width = tokens.shape
    piece, local = gate_weight.shape
    out_piece = down_weight.shape[1]
    units = local // GROUP
    blocks = units // 128
    chunk = GROUP * out_piece
    strip = 2 * out_piece
    strips = chunk // strip
    per_core = half * strips
    dma = pltpu.SemaphoreType.DMA
    bf16, f32 = jnp.bfloat16, jnp.float32
    vmem = pl.BlockSpec(memory_space=pltpu.VMEM)
    hbm = pl.BlockSpec(memory_space=pl.ANY)
    return pl.pallas_call(
        functools.partial(fused_kernel, planes),
        out_shape=jax.ShapeDtypeStruct((rows, half * chunk), bf16),
        in_specs=[hbm] * 4 + [vmem] * 8,
        out_specs=vmem,
        scratch_shapes=[
            pltpu.VMEM((GROUP * rows, width), bf16),
            pltpu.VMEM((blocks, width, 256), bf16),
            pltpu.VMEM((planes, units, chunk), bf16),
            pltpu.VMEM((GROUP * rows, units), bf16),
            pltpu.VMEM((2 * per_core, GROUP, rows, strip), bf16),
            pltpu.VMEM((per_core, GROUP, rows, strip), bf16),
            pltpu.VMEM((per_core, 2, rows, strip), bf16),
            pltpu.VMEM((per_core, 2, rows // 2, strip), bf16),
            pltpu.VMEM((rows + 8, 256), f32),
            pltpu.VMEM(((GROUP + 1) * EDGE, width), bf16),
            pltpu.VMEM((blocks, GROUP * EDGE, 256), f32),
            pltpu.VMEM((8, 2 * units), f32),
            pltpu.VMEM((GROUP, blocks, piece, 256), bf16),
            pltpu.VMEM((GROUP, units, out_piece), bf16),
            pltpu.VMEM((rows, width), bf16),
            pltpu.VMEM((piece, local), f32),
            pltpu.VMEM((piece, local), f32),
            pltpu.VMEM((local, out_piece), f32),
            dma((4,)),
            dma((2,)),
            dma((3, GROUP)),
            dma((2, GROUP)),
            dma((2, 2, GROUP)),
            dma((2, 2, GROUP)),
            dma((GROUP,)),
            dma((GROUP,)),
            dma((2, max(1, planes - 2), blocks)),
            dma((2, max(1, planes - 2), blocks)),
            dma((count + GROUP,)),
            dma((count,)),
            dma((2, GROUP)),
            dma((2, 2)),
            dma((2, 2)),
            dma((2, 2)),
            dma((2, 2)),
            dma((3, 2)),
            dma((3, 2)),
            dma((per_core, GROUP)),
            dma((per_core, GROUP)),
            dma((per_core, 4)),
            dma((per_core, 4)),
            dma((per_core, 2)),
            dma((per_core, 2)),
        ],
        compiler_params=pltpu.CompilerParams(
            collective_id=0, has_side_effects=True, vmem_limit_bytes=67043328
        ),
    )(
        tokens,
        gate_weight,
        value_weight,
        down_weight,
        norm_gain[None, :],
        gate_scale.reshape(-1, 128),
        value_scale.reshape(-1, 128),
        gate_kernel,
        value_kernel,
        gate_bias.reshape(-1, 128),
        value_bias.reshape(-1, 128),
        down_scale[None, :],
    )


def solution(mesh):
    count, tp = mesh.shape["fs"], mesh.shape["tp"]

    def whole(*arrays):
        local = arrays[2].shape[1]
        fits = tp == 2 and count % (2 * GROUP) == 0 and local % (GROUP * 128) == 0
        if fits:
            return grouped_body(count, *arrays)
        return body(*arrays)

    return jax.shard_map(
        whole,
        mesh=mesh,
        in_specs=(
            P("fs", None),
            P(),
            P("fs", "tp"),
            P("fs", "tp"),
            P("tp"),
            P("tp"),
            P(None, "tp"),
            P(None, "tp"),
            P("tp"),
            P("tp"),
            P("tp", "fs"),
            P("tp"),
        ),
        out_specs=P("fs", "tp"),
        check_vma=False,
    )
```

```python
import functools
import math

import jax
import jax.numpy as jnp
from jax import lax
from jax.experimental import pallas as pl
from jax.experimental.pallas import tpu as pltpu
from jax.sharding import PartitionSpec as P

epsilon = 1e-06


def from_behind(value, axis, steps):
    count = lax.axis_size(axis)
    leading, last = (max(0, -steps), min(count, count - steps))
    return lax.ppermute(value, axis, [(source, source + steps) for source in range(leading, last)])


def normalize(tokens, norm_gain):
    values = tokens.astype(jnp.float32)
    scaled = values * lax.rsqrt(jnp.mean(values * values, axis=1, keepdims=True) + epsilon)
    return (scaled * norm_gain[None, :]).astype(jnp.bfloat16)


def causal_mix(current, previous, kernel, tap_bias):
    row_count = current.shape[0]
    joined = jnp.concatenate([previous, current], axis=0).astype(jnp.float32)
    summed_taps = tap_bias[None, :] + kernel[2][None, :] * joined[2:]
    for back_by in (1, 2):
        summed_taps = (
            summed_taps
            + kernel[2 - back_by][None, :] * joined[2 - back_by : 2 - back_by + row_count]
        )
    return summed_taps


def body(
    tokens,
    norm_gain,
    gate_weight,
    value_weight,
    gate_scale,
    value_scale,
    gate_kernel,
    value_kernel,
    gate_bias,
    value_bias,
    down_weight,
    down_scale,
):
    normed = normalize(tokens, norm_gain)
    gate_low = gate_weight.astype(jnp.bfloat16)
    value_low = value_weight.astype(jnp.bfloat16)
    down_low = down_weight.astype(jnp.bfloat16)
    row_count = normed.shape[0]
    gate_full, value_full, down_full = (
        lax.all_gather(gate_low, "fs", axis=0, tiled=True),
        lax.all_gather(value_low, "fs", axis=0, tiled=True),
        lax.all_gather(down_low, "fs", axis=1, tiled=True),
    )
    gate_raw = jnp.dot(normed, gate_full, preferred_element_type=jnp.float32)
    value_raw = jnp.dot(normed, value_full, preferred_element_type=jnp.float32)
    gate_pre = (gate_raw * gate_scale[None, :]).astype(jnp.bfloat16)
    value_pre = (value_raw * value_scale[None, :]).astype(jnp.bfloat16)
    previous_gate, previous_value = from_behind(
        (gate_pre[row_count - 2 :], value_pre[row_count - 2 :]), "fs", 1
    )
    gate_conv = causal_mix(gate_pre, previous_gate, gate_kernel, gate_bias)
    value_conv = causal_mix(value_pre, previous_value, value_kernel, value_bias)
    hidden = (jax.nn.gelu(gate_conv, approximate=True) * value_conv).astype(jnp.bfloat16)
    partial_terms = jnp.dot(hidden, down_full, preferred_element_type=jnp.float32)
    summed = lax.psum_scatter(
        partial_terms.astype(jnp.bfloat16), "tp", scatter_dimension=1, tiled=True
    ).astype(jnp.float32)
    return (summed * down_scale[None, :]).astype(jnp.bfloat16)


MESH = pl.DeviceIdType.MESH
GROUP = 4
EDGE = 16


def fused_kernel(
    depth_planes,
    tok_hbm,
    gate_hbm,
    value_hbm,
    down_hbm,
    gain_hbm,
    gate_scale_hbm,
    value_scale_hbm,
    gate_kernel_hbm,
    value_kernel_hbm,
    gate_bias_hbm,
    value_bias_hbm,
    osc_hbm,
    out,
    tok,
    up_all,
    down_all,
    hidden,
    stage,
    pair_in,
    peer_in,
    relay_in,
    taps,
    edge,
    edge_pre,
    par,
    wu,
    wd,
    raw_tok,
    raw_gate,
    raw_value,
    raw_down,
    gain,
    gate_scale,
    value_scale,
    gate_kernel,
    value_kernel,
    gate_bias,
    value_bias,
    osc,
    sem_fetch,
    sem_own,
    sem_plane_send,
    sem_plane_recv,
    sem_first_send,
    sem_first_recv,
    sem_piece_send,
    sem_piece_recv,
    sem_far_send,
    sem_far_recv,
    sem_down_send,
    sem_down_recv,
    sem_edge_send,
    sem_edge_recv,
    sem_tok_send,
    sem_tok_recv,
    sem_diag_send,
    sem_diag_recv,
    sem_tok_pair_send,
    sem_tok_pair_recv,
    sem_pair_send,
    sem_pair_recv,
    sem_peer_send,
    sem_peer_recv,
    sem_relay_send,
    sem_relay_recv,
):
    planes = depth_planes
    half = planes // 2
    me = lax.axis_index("fs")
    core = lax.axis_index("tp")
    z, p = me // GROUP, me % GROUP
    rows_own = raw_tok.shape[0]
    part_rows = rows_own // 2
    blocks, piece = wu.shape[1], wu.shape[2]
    units = hidden.shape[1]
    out_piece = wd.shape[2]
    chunk = GROUP * out_piece
    has_up, has_down = z < planes - 1, z > 0
    inner_plane = has_up & has_down
    end_plane = jnp.logical_not(inner_plane)
    cut = min(2, blocks - 1)
    groups = ((0, cut), (cut, blocks))

    def flip(mask):
        px, py = p % 2, p // 2
        return (py + mask // 2) % 2 * 2 + (px + mask % 2) % 2

    def chip(target):
        return (z * GROUP + target, core)

    others = (1, 2, 3)

    fetches = [
        pltpu.make_async_copy(src, dst, sem_fetch.at[i])
        for i, (src, dst) in enumerate(
            (
                (gate_hbm, raw_gate),
                (value_hbm, raw_value),
                (tok_hbm, raw_tok),
                (down_hbm, raw_down),
                (gain_hbm, gain),
                (gate_scale_hbm, gate_scale),
                (value_scale_hbm, value_scale),
                (gate_kernel_hbm, gate_kernel),
                (value_kernel_hbm, value_kernel),
                (gate_bias_hbm, gate_bias),
                (value_bias_hbm, value_bias),
                (osc_hbm, osc),
            )
        )
    ]
    for fetch in fetches:
        fetch.start()

    barrier = pltpu.get_barrier_semaphore()
    for mask in others:
        pl.semaphore_signal(barrier, inc=1, device_id=chip(flip(mask)), device_id_type=MESH)
    pl.semaphore_signal(barrier, inc=1, device_id=(me, 1 - core), device_id_type=MESH)

    @pl.when(has_up)
    def _():
        pl.semaphore_signal(barrier, inc=1, device_id=(me + GROUP, core), device_id_type=MESH)

    @pl.when(has_down)
    def _():
        pl.semaphore_signal(barrier, inc=1, device_id=(me - GROUP, core), device_id_type=MESH)

    def remote(src, dst, send, recv, device):
        return pltpu.make_async_remote_copy(
            src_ref=src, dst_ref=dst, send_sem=send, recv_sem=recv, device_id=device, device_id_type=MESH
        )

    def rows_of(f, count=1):
        return pl.ds(pl.multiple_of(f * piece, piece), count * piece)

    def down_block(f):
        return down_all.at[f // GROUP, :, pl.ds(pl.multiple_of(f % GROUP * out_piece, out_piece), out_piece)]

    def line(side):
        return (me + (GROUP if side == 0 else -GROUP), core)

    def plane_up(g, mask):
        first, last = groups[g]
        return remote(
            wu.at[flip(mask), first:last],
            up_all.at[first:last, rows_of(me), :],
            sem_plane_send.at[0],
            sem_plane_recv.at[g, mask],
            chip(flip(mask)),
        )

    def plane_up_landed(g, mask):
        first, last = groups[g]
        here = up_all.at[first:last, rows_of(z * GROUP + flip(mask)), :]
        remote(here, here, sem_plane_send.at[0], sem_plane_recv.at[g, mask], chip(flip(mask))).wait_recv()

    def first_hop(side, g, mask):
        first, last = groups[g]
        there = up_all.at[first:last, rows_of(z * GROUP + flip(mask)), :]
        here = there if mask else wu.at[p, first:last]
        return remote(here, there, sem_first_send.at[side], sem_first_recv.at[side, mask], line(side))

    def first_landed(side, mask):
        here = up_all.at[:, rows_of((z + (2 * side - 1)) * GROUP + flip(mask)), :]
        remote(here, here, sem_first_send.at[side], sem_first_recv.at[side, mask], (me, 1 - core)).wait_recv()

    def piece_hop(side, mask):
        here = up_all.at[:, rows_of((z + (2 * side - 1)) * GROUP + flip(mask)), :]
        return remote(here, here, sem_piece_send.at[0], sem_piece_recv.at[mask], line(side))

    def piece_landed(side, mask):
        here = up_all.at[:, rows_of((z + 2 * (2 * side - 1)) * GROUP + flip(mask)), :]
        remote(here, here, sem_piece_send.at[0], sem_piece_recv.at[mask], (me, 1 - core)).wait_recv()

    def far_hop(side, distance, j):
        q = z + distance * (2 * side - 1)
        here = up_all.at[j, rows_of(q * GROUP, GROUP), :]
        return remote(
            here, here, sem_far_send.at[side, distance - 1], sem_far_recv.at[side, distance - 1, j], line(side)
        )

    def far_landed(side, distance, j):
        q = z + distance * (2 * side - 1)
        here = up_all.at[j, rows_of(q * GROUP, GROUP), :]
        remote(
            here, here, sem_far_send.at[side, distance - 2], sem_far_recv.at[side, distance - 2, j], (me, 1 - core)
        ).wait_recv()

    def plane_down(mask):
        return remote(
            wd.at[flip(mask)],
            down_block(me),
            sem_plane_send.at[1],
            sem_down_recv.at[me],
            chip(flip(mask)),
        )

    def line_down(side, f, slot, src=None):
        here = down_block(f)
        return remote(
            here if src is None else src, here, sem_down_send.at[slot], sem_down_recv.at[f], line(side)
        )

    def wait_down(f):
        here = down_block(f)
        remote(here, here, sem_down_send.at[0], sem_down_recv.at[f], (me, 1 - core)).wait_recv()

    def both_ways(copy_of):
        @pl.when(has_up)
        def _():
            copy_of(0).start()

        @pl.when(has_down)
        def _():
            copy_of(1).start()

    own_up = pltpu.make_async_copy(wu.at[p], up_all.at[:, rows_of(me), :], sem_own.at[0])
    own_down = pltpu.make_async_copy(wd.at[p], down_block(me), sem_own.at[1])

    def cast_block(j):
        for m in range(GROUP):
            first = m * units + j * 128
            wu[m, j, :, 0:128] = raw_gate[:, first : first + 128].astype(jnp.bfloat16)
            wu[m, j, :, 128:256] = raw_value[:, first : first + 128].astype(jnp.bfloat16)

    def normed(first, count):
        values = raw_tok[pl.ds(first, count), :].astype(jnp.float32)
        scaled = values * lax.rsqrt(jnp.mean(values * values, axis=1, keepdims=True) + epsilon)
        return (scaled * gain[...]).astype(jnp.bfloat16)

    fetches[0].wait()
    fetches[1].wait()
    for j in range(blocks):
        cast_block(j)
    pl.semaphore_wait(barrier, 4 + has_up.astype(jnp.int32) + has_down.astype(jnp.int32))
    for g in range(2):
        for mask in others:
            plane_up(g, mask).start()
        both_ways(lambda side: first_hop(side, g, 0))
    own_up.start()

    def edge_slot(slot):
        return edge.at[pl.ds(pl.multiple_of(slot * EDGE, EDGE), EDGE), :]

    def edge_copy(mask):
        here = edge_slot(p + 1)
        return remote(here, here, sem_edge_send.at[0], sem_edge_recv.at[mask], chip(flip(mask)))

    edge_next = remote(
        edge_slot(GROUP), edge_slot(0), sem_edge_send.at[1], sem_edge_recv.at[0], (me + GROUP, core)
    )

    @pl.when(jnp.logical_not(has_down))
    def _():
        edge[0:EDGE, :] = jnp.zeros_like(edge[0:EDGE, :])

    fetches[2].wait()
    fetches[4].wait()
    edge[pl.ds(pl.multiple_of((p + 1) * EDGE, EDGE), EDGE), :] = normed(rows_own - EDGE, EDGE)
    for mask in others:
        edge_copy(mask).start()
    norm_tile = 64

    def norm_step(i, carry):
        first = pl.multiple_of(i * norm_tile, norm_tile)
        tok[pl.ds(pl.multiple_of(p * rows_own + i * norm_tile, norm_tile), norm_tile), :] = normed(first, norm_tile)
        return carry

    lax.fori_loop(0, rows_own // norm_tile, norm_step, 0)

    parts = 2
    sub_rows = part_rows // parts
    diag_rows = sub_rows // 2

    def token_rows(owner, side, part):
        start = owner * rows_own + side * part_rows + part * sub_rows
        return tok.at[pl.ds(pl.multiple_of(start, sub_rows), sub_rows), :]

    def diag_part(owner, part, which):
        start = owner * rows_own + core * part_rows + part * sub_rows + which * diag_rows
        return tok.at[pl.ds(pl.multiple_of(start, diag_rows), diag_rows), :]

    def token_copy(mask, part):
        here = token_rows(p, core, part)
        return remote(here, here, sem_tok_send.at[0], sem_tok_recv.at[mask - 1, part], chip(flip(mask)))

    def token_relay(mask, part):
        here = diag_part(flip(mask), part, mask - 1)
        return remote(
            here,
            here,
            sem_diag_send.at[0],
            sem_diag_recv.at[0],
            chip(flip(3 - mask)),
        )

    def token_pair(mask, part):
        here = token_rows(flip(mask), core, part)
        return remote(
            here, here, sem_tok_pair_send.at[0], sem_tok_pair_recv.at[mask - 1], (me, 1 - core)
        )

    for part in range(parts):
        for mask in (1, 2):
            token_copy(mask, part).start()

    for i in (3, 5, 6, 7, 8, 9, 10, 11):
        fetches[i].wait()
    for m in range(GROUP):
        wd[m] = raw_down[m * units : (m + 1) * units, :].astype(jnp.bfloat16)
    own_down.start()
    for j in range(blocks):
        src = pl.ds(p * blocks + j, 1)
        cols = pl.ds(pl.multiple_of(p * units + j * 128, 128), 128)
        for side, (scale, kernel, tap_bias) in enumerate(
            ((gate_scale, gate_kernel, gate_bias), (value_scale, value_kernel, value_bias))
        ):
            dst = slice(j * 256 + side * 128, j * 256 + side * 128 + 128)
            par[1:4, dst] = kernel[0:3, cols] * scale[src, :]
            par[4:5, dst] = tap_bias[src, :]

    for g in range(2):
        for mask in others:
            plane_up_landed(g, mask)
            both_ways(lambda side: first_hop(side, g, mask))

    for mask in others:
        here = edge_slot(flip(mask) + 1)
        remote(here, here, sem_edge_send.at[0], sem_edge_recv.at[mask], (me, 1 - core)).wait_recv()

    @pl.when(has_up)
    def _():
        edge_next.start()

    low_half = (z < half).astype(jnp.int32)

    def plane_of(step):
        distance = (step + 1) // 2
        below = (step + low_half) % 2
        return z + distance * (1 - 2 * below), below

    def wide(j):
        return pl.ds(pl.multiple_of(j * 256, 256), 256)

    def unit(owner, j):
        rows = pl.ds(pl.multiple_of(owner * rows_own, rows_own), rows_own)
        taps[8:, :] = jnp.dot(tok[rows, :], up_all[j], preferred_element_type=jnp.float32)
        taps[0:8, :] = edge_pre[j, pl.ds(pl.multiple_of(owner * EDGE + EDGE - 8, 8), 8), :]
        conv = par[4:5, wide(j)] + par[3:4, wide(j)] * taps[8 : 8 + rows_own, :]
        conv = conv + par[2:3, wide(j)] * taps[7 : 7 + rows_own, :]
        conv = conv + par[1:2, wide(j)] * taps[6 : 6 + rows_own, :]
        g, v = conv[:, :128], conv[:, 128:]
        root = math.sqrt(2.0 / math.pi)
        bend = jnp.tanh(g * (root + (root * 0.044715) * (g * g)))
        hidden[rows, pl.ds(pl.multiple_of(j * 128, 128), 128)] = ((0.5 * (g * v)) * (1.0 + bend)).astype(jnp.bfloat16)

    def landed(mask, part):
        here = token_rows(flip(mask), core, part)
        remote(here, here, sem_tok_send.at[0], sem_tok_recv.at[mask - 1, part], (me, 1 - core)).wait_recv()

    def half_group(owner, side):
        return tok.at[pl.ds(pl.multiple_of(owner * rows_own + side * part_rows, part_rows), part_rows), :]

    def pair_landed(mask):
        there = half_group(flip(mask), 1 - core)
        remote(there, there, sem_tok_pair_send.at[0], sem_tok_pair_recv.at[mask - 1], (me, 1 - core)).wait_recv()

    def pass_tokens(part):
        for mask in (1, 2):
            landed(mask, part)
            token_relay(mask, part).start()
            token_pair(mask, part).start()

    def near(side):
        def pieces():
            for mask in range(GROUP):
                first_landed(side, mask)
                piece_hop(side, mask).start()

        def whole():
            for mask in range(GROUP):
                first_landed(side, mask)

        onward = z + (1 - 2 * side)
        into_end = onward == (planes - 1 if side == 0 else 0)

        @pl.when(inner_plane & into_end)
        def _():
            pieces()

        @pl.when(inner_plane & jnp.logical_not(into_end))
        def _():
            whole()

            def one(j, carry):
                far_hop(side, 1, j).start()
                return carry

            lax.fori_loop(0, blocks, one, 0)

        @pl.when(end_plane & (has_down if side == 0 else has_up))
        def _():
            whole()

    @pl.when(low_half == 1)
    def _():
        near(1)
        near(0)

    @pl.when(low_half == 0)
    def _():
        near(0)
        near(1)

    pass_tokens(0)

    def send_down():
        for mask in others:
            plane_down(mask).start()

    def pass_rest():
        pass_tokens(parts - 1)
        send_down()

    @pl.when(end_plane)
    def _():
        for mask in range(GROUP):
            for side in (0, 1):

                @pl.when((z >= 2) if side == 0 else (z < planes - 2))
                def _():
                    piece_landed(side, mask)

            if mask == GROUP - 2:
                pass_rest()

    @pl.when(has_down)
    def _():
        here = edge_slot(0)
        remote(here, here, sem_edge_send.at[1], sem_edge_recv.at[0], (me, 1 - core)).wait_recv()

    own_up.wait()
    own_down.wait()

    def edge_block(j):
        ahead = jnp.dot(edge[0 : GROUP * EDGE, :], up_all[j], preferred_element_type=jnp.float32)
        edge_pre[j] = ahead

    def far_round(j, carry):
        @pl.when(inner_plane)
        def _():
            for distance in range(2, planes - 1):
                for side in (0, 1):

                    @pl.when((z >= distance) if side == 0 else (z < planes - distance))
                    def _():
                        far_landed(side, distance, j)
                        far_hop(side, distance, j).start()

            @pl.when(j == max(0, blocks - 2))
            def _():
                pass_rest()

        return carry

    lax.fori_loop(0, blocks, far_round, 0)

    def block_rows(owner):
        return pl.ds(pl.multiple_of(owner * rows_own, rows_own), rows_own)

    strip = 2 * out_piece
    strips = chunk // strip
    per_core = half * strips

    def pair_copy(c, owner):
        return remote(
            stage.at[c, owner],
            pair_in.at[c % per_core, owner],
            sem_pair_send.at[0],
            sem_pair_recv.at[c % per_core, owner],
            (me, 1 - core),
        )

    half_rows = rows_own // 2

    def half_of(which):
        return pl.ds(pl.multiple_of(which * half_rows, half_rows), half_rows)

    def peer_copy(c, mask, which):
        return remote(
            stage.at[c, flip(mask), half_of(which)],
            peer_in.at[c % per_core, mask - 1, half_of(which)],
            sem_peer_send.at[0],
            sem_peer_recv.at[c % per_core],
            chip(flip(mask)),
        )

    def relay_copy(c, mask):
        return remote(
            stage.at[c, flip(3), half_of(mask - 1)],
            relay_in.at[c % per_core, mask - 1],
            sem_relay_send.at[0],
            sem_relay_recv.at[c % per_core, mask - 1],
            chip(flip(mask)),
        )

    def combine(c, owner):
        pair_copy(c, owner).wait_recv()
        both = stage[c, owner].astype(jnp.float32) + pair_in[c % per_core, owner].astype(jnp.float32)
        stage[c, owner] = both.astype(jnp.bfloat16)

    def product(c, owner):
        first = pl.multiple_of(c % strips * strip, strip)
        value = jnp.dot(
            hidden[block_rows(owner), :], down_all[c // strips, :, pl.ds(first, strip)], preferred_element_type=jnp.float32
        )
        stage[c, owner] = value.astype(jnp.bfloat16)

        @pl.when(jnp.logical_not(mine(c)))
        def _():
            pair_copy(c, owner).start()

    def send_out(c, mask):
        combine(c, flip(mask))

        @pl.when(mask == 3)
        def _():
            for way in (1, 2):
                relay_copy(c, way).start()

        @pl.when((mask == 1) | (mask == 2))
        def _():
            peer_copy(c, mask, mask - 1).start()

    def pass_on(c):
        for mask in (1, 2):
            relay_copy(c, mask).wait_recv()
            owner = flip(3 - mask)
            rows = half_of(mask - 1)
            total = stage[c, owner, rows, :].astype(jnp.float32) + relay_in[c % per_core, mask - 1].astype(jnp.float32)
            stage[c, owner, rows, :] = total.astype(jnp.bfloat16)
            peer_copy(c, 3 - mask, mask - 1).start()

    def mine(c):
        return c // per_core == core

    def own_down_out():
        both_ways(lambda side: line_down(side, me, side, wd.at[p]))
        for mask in others:
            f = z * GROUP + flip(mask)
            wait_down(f)
            both_ways(lambda side: line_down(side, f, side))

    diag_round = jnp.where(inner_plane, blocks - 1, min(2, blocks - 1))

    def up_round(j, carry):
        @pl.when(end_plane)
        def _():
            for distance in range(3, planes):
                for side in (0, 1):

                    @pl.when((z >= distance) if side == 0 else (z < planes - distance))
                    def _():
                        far_landed(side, distance, j)

        edge_block(j)

        @pl.when(j == diag_round)
        def _():
            here = half_group(flip(3), core)
            remote(here, here, sem_diag_send.at[0], sem_diag_recv.at[0], (me, 1 - core)).wait_recv()
            for part in range(parts):
                token_pair(3, part).start()

        final = j == blocks - 1

        def group(i, inner):
            mask = jnp.where(final, 3 - i, i)
            ready = jnp.where(mask == 3, diag_round, 0)

            @pl.when((mask == 3) & (j == diag_round))
            def _():
                own_down_out()

            @pl.when((mask > 0) & (j == ready))
            def _():
                pair_landed(mask)

            first = jnp.where(j == ready, 0, j)
            last = jnp.where(j >= ready, j + 1, 0)

            def one(k, deeper):
                unit(flip(mask), k)
                return deeper

            lax.fori_loop(first, last, one, inner)

            @pl.when(final)
            def _():
                @pl.when(mine(z * strips) & (i > 0))
                def _():
                    for n in range(strips):
                        send_out(z * strips + n, mask + 1)

                for n in range(strips):
                    product(z * strips + n, flip(mask))

            return inner

        return lax.fori_loop(0, GROUP, group, carry)

    lax.fori_loop(0, blocks, up_round, 0)

    @pl.when(mine(z * strips))
    def _():
        for n in range(strips):
            send_out(z * strips + n, 0)
        for n in range(strips - 1):
            pass_on(z * strips + n)

    def pass_plane(step):
        q, below = plane_of(step)

        @pl.when((q >= 0) & (q < planes))
        def _():
            def one(i, carry):
                f = q * GROUP + i
                wait_down(f)

                @pl.when((below == 1) & has_up)
                def _():
                    line_down(0, f, 2 + q).start()

                @pl.when((below == 0) & has_down)
                def _():
                    line_down(1, f, 2 + q).start()

                return carry

            lax.fori_loop(0, GROUP, one, 0)

    def sent(here, send, recv):
        remote(here, here, send, recv, (me, 1 - core)).wait_send()

    def drain_early():
        sent(tok.at[0:rows_own], sem_tok_send.at[0], sem_tok_recv.at[0, 0])
        sent(tok.at[0:part_rows], sem_diag_send.at[0], sem_diag_recv.at[0])
        sent(tok.at[0 : 3 * part_rows], sem_tok_pair_send.at[0], sem_tok_pair_recv.at[0])
        sent(edge.at[0 : 3 * EDGE], sem_edge_send.at[0], sem_edge_recv.at[0])
        sent(wu.at[0:3], sem_plane_send.at[0], sem_plane_recv.at[0, 0])
        sent(wd.at[0:3], sem_plane_send.at[1], sem_plane_recv.at[0, 0])
        whole = up_all.at[:, rows_of(0, GROUP), :]

        @pl.when(has_up)
        def _():
            edge_next.wait_send()

        for side in (0, 1):

            @pl.when(has_up if side == 0 else has_down)
            def _():
                sent(whole, sem_first_send.at[side], sem_first_recv.at[side, 0])

            onward = z + (1 - 2 * side)
            into_end = onward == (planes - 1 if side == 0 else 0)

            @pl.when(inner_plane & into_end)
            def _():
                sent(whole, sem_piece_send.at[0], sem_piece_recv.at[0])

            @pl.when(inner_plane)
            def _():
                for distance in range(1, planes - 1):
                    valid = (z >= distance) if side == 0 else (z < planes - distance)

                    @pl.when(valid & (jnp.logical_not(into_end) if distance == 1 else True))
                    def _():
                        sent(whole, sem_far_send.at[side, distance - 1], sem_far_recv.at[side, 0, 0])

    def down_step(n, before):
        step = n // strips
        q, below = plane_of(step)
        valid = (q >= 0) & (q < planes)
        c = q * strips + n % strips
        owed = before >= 0

        @pl.when((n == strips) & inner_plane)
        def _():
            pass_plane(1)
            pass_plane(2)

        @pl.when(n == 2 * strips)
        def _():
            drain_early()

        @pl.when((n == 2 * strips + 1) & inner_plane)
        def _():
            for later in range(3, 2 * planes - 1):
                pass_plane(later)

        @pl.when(valid & end_plane)
        def _():
            for i in range(GROUP // strips):
                wait_down(q * GROUP + n % strips * (GROUP // strips) + i)

        @pl.when(valid)
        def _():
            def one(i, inner):
                product(c, flip(3 - i))
                return inner

            lax.fori_loop(0, GROUP, one, 0)

            @pl.when(mine(c))
            def _():
                def one(i, inner):
                    send_out(c, 3 - i)
                    return inner

                lax.fori_loop(0, GROUP, one, 0)

        due = valid & owed & (mine(c) | (n % strips == strips - 1))

        @pl.when(due)
        def _():
            pass_on(before)

        return jnp.where(valid & mine(c), c, jnp.where(due, -1, before))

    first_owed = jnp.where(mine(z * strips), z * strips + strips - 1, -1)
    last = lax.fori_loop(strips, (2 * planes - 1) * strips, down_step, first_owed)

    def finish(c):
        i = c % per_core
        total = stage[c, p].astype(jnp.float32)
        landed_all = peer_in.at[i]
        remote(landed_all, landed_all, sem_peer_send.at[0], sem_peer_recv.at[i], chip(flip(1))).wait_recv()
        for mask in (1, 2):
            total = total + peer_in[i, mask - 1].astype(jnp.float32)
        cols = pl.ds(pl.multiple_of(i * strip, strip), strip)
        out[:, cols] = (total * osc[0:1, cols]).astype(jnp.bfloat16)

    @pl.when(last >= 0)
    def _():
        pass_on(last)

    def finish_one(i, carry):
        finish(core * per_core + i)
        return carry

    lax.fori_loop(0, per_core, finish_one, 0)

    sent(pair_in, sem_pair_send.at[0], sem_pair_recv.at[0, 0])
    sent(peer_in, sem_peer_send.at[0], sem_peer_recv.at[0])
    sent(relay_in, sem_relay_send.at[0], sem_relay_recv.at[0, 0])
    for side in (0, 1):

        @pl.when(has_up if side == 0 else has_down)
        def _():
            sent(down_all.at[0], sem_down_send.at[side], sem_down_recv.at[0])

    @pl.when(inner_plane)
    def _():
        def drain_down(q, carry):
            @pl.when(q != z)
            def _():
                sent(down_all.at[0], sem_down_send.at[2 + q], sem_down_recv.at[0])

            return carry

        lax.fori_loop(0, planes, drain_down, 0)


def grouped_body(count, tokens, norm_gain, gate_weight, value_weight, gate_scale, value_scale, gate_kernel, value_kernel, gate_bias, value_bias, down_weight, down_scale):
    planes = count // GROUP
    half = planes // 2
    rows, width = tokens.shape
    piece, local = gate_weight.shape
    out_piece = down_weight.shape[1]
    units = local // GROUP
    blocks = units // 128
    chunk = GROUP * out_piece
    strip = 2 * out_piece
    strips = chunk // strip
    per_core = half * strips
    dma = pltpu.SemaphoreType.DMA
    bf16, f32 = jnp.bfloat16, jnp.float32
    vmem = pl.BlockSpec(memory_space=pltpu.VMEM)
    hbm = pl.BlockSpec(memory_space=pl.ANY)
    return pl.pallas_call(
        functools.partial(fused_kernel, planes),
        out_shape=jax.ShapeDtypeStruct((rows, half * chunk), bf16),
        in_specs=[hbm] * 12,
        out_specs=vmem,
        scratch_shapes=[
            pltpu.VMEM((GROUP * rows, width), bf16),
            pltpu.VMEM((blocks, width, 256), bf16),
            pltpu.VMEM((planes, units, chunk), bf16),
            pltpu.VMEM((GROUP * rows, units), bf16),
            pltpu.VMEM((2 * per_core, GROUP, rows, strip), bf16),
            pltpu.VMEM((per_core, GROUP, rows, strip), bf16),
            pltpu.VMEM((per_core, 2, rows, strip), bf16),
            pltpu.VMEM((per_core, 2, rows // 2, strip), bf16),
            pltpu.VMEM((rows + 8, 256), f32),
            pltpu.VMEM(((GROUP + 1) * EDGE, width), bf16),
            pltpu.VMEM((blocks, GROUP * EDGE, 256), f32),
            pltpu.VMEM((8, 2 * units), f32),
            pltpu.VMEM((GROUP, blocks, piece, 256), bf16),
            pltpu.VMEM((GROUP, units, out_piece), bf16),
            pltpu.VMEM((rows, width), bf16),
            pltpu.VMEM((piece, local), f32),
            pltpu.VMEM((piece, local), f32),
            pltpu.VMEM((local, out_piece), f32),
            pltpu.VMEM((1, width), f32),
            pltpu.VMEM((local // 128, 128), f32),
            pltpu.VMEM((local // 128, 128), f32),
            pltpu.VMEM(gate_kernel.shape, f32),
            pltpu.VMEM(value_kernel.shape, f32),
            pltpu.VMEM((local // 128, 128), f32),
            pltpu.VMEM((local // 128, 128), f32),
            pltpu.VMEM((1, half * chunk), f32),
            dma((12,)),
            dma((2,)),
            dma((2,)),
            dma((2, GROUP)),
            dma((2,)),
            dma((2, GROUP)),
            dma((1,)),
            dma((GROUP,)),
            dma((2, max(1, planes - 2))),
            dma((2, max(1, planes - 2), blocks)),
            dma((2 + planes,)),
            dma((count,)),
            dma((2,)),
            dma((GROUP,)),
            dma((1,)),
            dma((2, 2)),
            dma((1,)),
            dma((1,)),
            dma((1,)),
            dma((3,)),
            dma((1,)),
            dma((per_core, GROUP)),
            dma((1,)),
            dma((per_core,)),
            dma((1,)),
            dma((per_core, 2)),
        ],
        compiler_params=pltpu.CompilerParams(
            collective_id=0, has_side_effects=True, vmem_limit_bytes=67043328
        ),
    )(
        tokens,
        gate_weight,
        value_weight,
        down_weight,
        norm_gain[None, :],
        gate_scale.reshape(-1, 128),
        value_scale.reshape(-1, 128),
        gate_kernel,
        value_kernel,
        gate_bias.reshape(-1, 128),
        value_bias.reshape(-1, 128),
        down_scale[None, :],
    )


def solution(mesh):
    count, tp = mesh.shape["fs"], mesh.shape["tp"]

    def whole(*arrays):
        local = arrays[2].shape[1]
        fits = tp == 2 and count % (2 * GROUP) == 0 and local % (GROUP * 128) == 0
        if fits:
            return grouped_body(count, *arrays)
        return body(*arrays)

    return jax.shard_map(
        whole,
        mesh=mesh,
        in_specs=(
            P("fs", None),
            P(),
            P("fs", "tp"),
            P("fs", "tp"),
            P("tp"),
            P("tp"),
            P(None, "tp"),
            P(None, "tp"),
            P("tp"),
            P("tp"),
            P("tp", "fs"),
            P("tp"),
        ),
        out_specs=P("fs", "tp"),
        check_vma=False,
    )
```

```python
import functools
import math

import jax
import jax.numpy as jnp
from jax import lax
from jax.experimental import pallas as pl
from jax.experimental.pallas import tpu as pltpu
from jax.sharding import PartitionSpec as P

epsilon = 1e-06


def from_behind(value, axis, steps):
    count = lax.axis_size(axis)
    leading, last = (max(0, -steps), min(count, count - steps))
    return lax.ppermute(value, axis, [(source, source + steps) for source in range(leading, last)])


def normalize(tokens, norm_gain):
    values = tokens.astype(jnp.float32)
    scaled = values * lax.rsqrt(jnp.mean(values * values, axis=1, keepdims=True) + epsilon)
    return (scaled * norm_gain[None, :]).astype(jnp.bfloat16)


def causal_mix(current, previous, kernel, tap_bias):
    row_count = current.shape[0]
    joined = jnp.concatenate([previous, current], axis=0).astype(jnp.float32)
    summed_taps = tap_bias[None, :] + kernel[2][None, :] * joined[2:]
    for back_by in (1, 2):
        summed_taps = (
            summed_taps
            + kernel[2 - back_by][None, :] * joined[2 - back_by : 2 - back_by + row_count]
        )
    return summed_taps


def body(
    tokens,
    norm_gain,
    gate_weight,
    value_weight,
    gate_scale,
    value_scale,
    gate_kernel,
    value_kernel,
    gate_bias,
    value_bias,
    down_weight,
    down_scale,
):
    normed = normalize(tokens, norm_gain)
    gate_low = gate_weight.astype(jnp.bfloat16)
    value_low = value_weight.astype(jnp.bfloat16)
    down_low = down_weight.astype(jnp.bfloat16)
    row_count = normed.shape[0]
    gate_full, value_full, down_full = (
        lax.all_gather(gate_low, "fs", axis=0, tiled=True),
        lax.all_gather(value_low, "fs", axis=0, tiled=True),
        lax.all_gather(down_low, "fs", axis=1, tiled=True),
    )
    gate_raw = jnp.dot(normed, gate_full, preferred_element_type=jnp.float32)
    value_raw = jnp.dot(normed, value_full, preferred_element_type=jnp.float32)
    gate_pre = (gate_raw * gate_scale[None, :]).astype(jnp.bfloat16)
    value_pre = (value_raw * value_scale[None, :]).astype(jnp.bfloat16)
    previous_gate, previous_value = from_behind(
        (gate_pre[row_count - 2 :], value_pre[row_count - 2 :]), "fs", 1
    )
    gate_conv = causal_mix(gate_pre, previous_gate, gate_kernel, gate_bias)
    value_conv = causal_mix(value_pre, previous_value, value_kernel, value_bias)
    hidden = (jax.nn.gelu(gate_conv, approximate=True) * value_conv).astype(jnp.bfloat16)
    partial_terms = jnp.dot(hidden, down_full, preferred_element_type=jnp.float32)
    summed = lax.psum_scatter(
        partial_terms.astype(jnp.bfloat16), "tp", scatter_dimension=1, tiled=True
    ).astype(jnp.float32)
    return (summed * down_scale[None, :]).astype(jnp.bfloat16)


MESH = pl.DeviceIdType.MESH
GROUP = 4
EDGE = 16


def fused_kernel(
    depth_planes,
    tok_hbm,
    gate_hbm,
    value_hbm,
    down_hbm,
    gain_hbm,
    gate_scale_hbm,
    value_scale_hbm,
    gate_kernel_hbm,
    value_kernel_hbm,
    gate_bias_hbm,
    value_bias_hbm,
    osc_hbm,
    out,
    tok,
    up_all,
    down_all,
    hidden,
    stage,
    pair_in,
    peer_in,
    relay_in,
    taps,
    edge,
    edge_pre,
    par,
    wu,
    wd,
    raw_gate,
    raw_value,
    raw_down,
    begun_sum,
    gain,
    gate_scale,
    value_scale,
    gate_kernel,
    value_kernel,
    gate_bias,
    value_bias,
    osc,
    sem_fetch,
    sem_own,
    sem_plane_send,
    sem_plane_recv,
    sem_first_send,
    sem_first_recv,
    sem_piece_send,
    sem_piece_recv,
    sem_far_send,
    sem_far_recv,
    sem_down_send,
    sem_down_recv,
    sem_edge_send,
    sem_edge_recv,
    sem_tok_send,
    sem_tok_recv,
    sem_diag_send,
    sem_diag_recv,
    sem_tok_pair_send,
    sem_tok_pair_recv,
    sem_pair_send,
    sem_pair_recv,
    sem_peer_send,
    sem_peer_recv,
    sem_relay_send,
    sem_relay_recv,
):
    planes = depth_planes
    half = planes // 2
    me = lax.axis_index("fs")
    core = lax.axis_index("tp")
    z, p = me // GROUP, me % GROUP
    rows_own = tok.shape[0] // GROUP
    part_rows = rows_own // 2
    blocks, piece = wu.shape[1], wu.shape[2]
    units = hidden.shape[1]
    out_piece = wd.shape[2]
    chunk = GROUP * out_piece
    has_up, has_down = z < planes - 1, z > 0
    inner_plane = has_up & has_down
    end_plane = jnp.logical_not(inner_plane)
    cut = min(2, blocks - 1)
    groups = ((0, cut), (cut, blocks))

    def flip(mask):
        px, py = p % 2, p // 2
        return (py + mask // 2) % 2 * 2 + (px + mask % 2) % 2

    def chip(target):
        return (z * GROUP + target, core)

    others = (1, 2, 3)

    own_rows = pl.ds(pl.multiple_of(p * rows_own, rows_own), rows_own)
    fetches = [
        pltpu.make_async_copy(src, dst, sem_fetch.at[i])
        for i, (src, dst) in enumerate(
            (
                (gate_hbm, raw_gate),
                (value_hbm, raw_value),
                (tok_hbm, tok.at[own_rows, :]),
                (down_hbm, raw_down),
                (gain_hbm, gain),
                (gate_scale_hbm, gate_scale),
                (value_scale_hbm, value_scale),
                (gate_kernel_hbm, gate_kernel),
                (value_kernel_hbm, value_kernel),
                (gate_bias_hbm, gate_bias),
                (value_bias_hbm, value_bias),
                (osc_hbm, osc),
            )
        )
    ]
    for fetch in fetches:
        fetch.start()

    barrier = pltpu.get_barrier_semaphore()
    for mask in others:
        pl.semaphore_signal(barrier, inc=1, device_id=chip(flip(mask)), device_id_type=MESH)
    pl.semaphore_signal(barrier, inc=1, device_id=(me, 1 - core), device_id_type=MESH)

    @pl.when(has_up)
    def _():
        pl.semaphore_signal(barrier, inc=1, device_id=(me + GROUP, core), device_id_type=MESH)

    @pl.when(has_down)
    def _():
        pl.semaphore_signal(barrier, inc=1, device_id=(me - GROUP, core), device_id_type=MESH)

    def remote(src, dst, send, recv, device):
        return pltpu.make_async_remote_copy(
            src_ref=src, dst_ref=dst, send_sem=send, recv_sem=recv, device_id=device, device_id_type=MESH
        )

    def rows_of(f, count=1):
        return pl.ds(pl.multiple_of(f * piece, piece), count * piece)

    def down_block(f):
        return down_all.at[f // GROUP, :, pl.ds(pl.multiple_of(f % GROUP * out_piece, out_piece), out_piece)]

    def line(side):
        return (me + (GROUP if side == 0 else -GROUP), core)

    def plane_up(g, mask):
        first, last = groups[g]
        return remote(
            wu.at[flip(mask), first:last],
            up_all.at[first:last, rows_of(me), :],
            sem_plane_send.at[0],
            sem_plane_recv.at[g, mask],
            chip(flip(mask)),
        )

    def plane_up_landed(g, mask):
        first, last = groups[g]
        here = up_all.at[first:last, rows_of(z * GROUP + flip(mask)), :]
        remote(here, here, sem_plane_send.at[0], sem_plane_recv.at[g, mask], chip(flip(mask))).wait_recv()

    def first_hop(side, g, mask):
        first, last = groups[g]
        there = up_all.at[first:last, rows_of(z * GROUP + flip(mask)), :]
        here = there if mask else wu.at[p, first:last]
        return remote(here, there, sem_first_send.at[side], sem_first_recv.at[side, mask], line(side))

    def first_landed(side, mask):
        here = up_all.at[:, rows_of((z + (2 * side - 1)) * GROUP + flip(mask)), :]
        remote(here, here, sem_first_send.at[side], sem_first_recv.at[side, mask], (me, 1 - core)).wait_recv()

    def piece_hop(side, mask):
        here = up_all.at[:, rows_of((z + (2 * side - 1)) * GROUP + flip(mask)), :]
        return remote(here, here, sem_piece_send.at[0], sem_piece_recv.at[mask], line(side))

    def piece_landed(side, mask):
        here = up_all.at[:, rows_of((z + 2 * (2 * side - 1)) * GROUP + flip(mask)), :]
        remote(here, here, sem_piece_send.at[0], sem_piece_recv.at[mask], (me, 1 - core)).wait_recv()

    def far_hop(side, distance, j):
        q = z + distance * (2 * side - 1)
        here = up_all.at[j, rows_of(q * GROUP, GROUP), :]
        return remote(
            here, here, sem_far_send.at[side, distance - 1], sem_far_recv.at[side, distance - 1, j], line(side)
        )

    def far_landed(side, distance, j):
        q = z + distance * (2 * side - 1)
        here = up_all.at[j, rows_of(q * GROUP, GROUP), :]
        remote(
            here, here, sem_far_send.at[side, distance - 2], sem_far_recv.at[side, distance - 2, j], (me, 1 - core)
        ).wait_recv()

    def plane_down(mask):
        return remote(
            wd.at[flip(mask)],
            down_block(me),
            sem_plane_send.at[1],
            sem_down_recv.at[me],
            chip(flip(mask)),
        )

    def line_down(side, f, slot, src=None):
        here = down_block(f)
        return remote(
            here if src is None else src, here, sem_down_send.at[slot], sem_down_recv.at[f], line(side)
        )

    def wait_down(f):
        here = down_block(f)
        remote(here, here, sem_down_send.at[0], sem_down_recv.at[f], (me, 1 - core)).wait_recv()

    def both_ways(copy_of):
        @pl.when(has_up)
        def _():
            copy_of(0).start()

        @pl.when(has_down)
        def _():
            copy_of(1).start()

    own_up = pltpu.make_async_copy(wu.at[p], up_all.at[:, rows_of(me), :], sem_own.at[0])
    own_down = pltpu.make_async_copy(wd.at[p], down_block(me), sem_own.at[1])

    def cast_block(j):
        for m in range(GROUP):
            first = m * units + j * 128
            wu[m, j, :, 0:128] = raw_gate[:, first : first + 128].astype(jnp.bfloat16)
            wu[m, j, :, 128:256] = raw_value[:, first : first + 128].astype(jnp.bfloat16)

    def normed(first, count):
        start = pl.multiple_of(p * rows_own + first, count)
        values = tok[pl.ds(start, count), :].astype(jnp.float32)
        scaled = values * lax.rsqrt(jnp.mean(values * values, axis=1, keepdims=True) + epsilon)
        return (scaled * gain[...]).astype(jnp.bfloat16)

    fetches[0].wait()
    fetches[1].wait()
    for g in range(2):
        for j in range(*groups[g]):
            cast_block(j)
        if g == 0:
            pl.semaphore_wait(barrier, 4 + has_up.astype(jnp.int32) + has_down.astype(jnp.int32))
        for mask in others:
            plane_up(g, mask).start()
        both_ways(lambda side: first_hop(side, g, 0))
    own_up.start()

    def edge_slot(slot):
        return edge.at[pl.ds(pl.multiple_of(slot * EDGE, EDGE), EDGE), :]

    def edge_copy(mask):
        here = edge_slot(p + 1)
        return remote(here, here, sem_edge_send.at[0], sem_edge_recv.at[mask], chip(flip(mask)))

    edge_next = remote(
        edge_slot(GROUP), edge_slot(0), sem_edge_send.at[1], sem_edge_recv.at[0], (me + GROUP, core)
    )

    @pl.when(jnp.logical_not(has_down))
    def _():
        edge[0:EDGE, :] = jnp.zeros_like(edge[0:EDGE, :])

    fetches[2].wait()
    fetches[4].wait()
    edge[pl.ds(pl.multiple_of((p + 1) * EDGE, EDGE), EDGE), :] = normed(rows_own - EDGE, EDGE)
    for mask in others:
        edge_copy(mask).start()
    norm_tile = 64

    def norm_step(i, carry):
        first = pl.multiple_of(i * norm_tile, norm_tile)
        tok[pl.ds(pl.multiple_of(p * rows_own + i * norm_tile, norm_tile), norm_tile), :] = normed(first, norm_tile)
        return carry

    lax.fori_loop(0, rows_own // norm_tile, norm_step, 0)

    parts = 2
    sub_rows = part_rows // parts
    diag_rows = sub_rows // 2

    def token_rows(owner, side, part):
        start = owner * rows_own + side * part_rows + part * sub_rows
        return tok.at[pl.ds(pl.multiple_of(start, sub_rows), sub_rows), :]

    def diag_part(owner, part, which):
        start = owner * rows_own + core * part_rows + part * sub_rows + which * diag_rows
        return tok.at[pl.ds(pl.multiple_of(start, diag_rows), diag_rows), :]

    def token_copy(mask, part):
        here = token_rows(p, core, part)
        return remote(here, here, sem_tok_send.at[0], sem_tok_recv.at[mask - 1, part], chip(flip(mask)))

    def token_relay(mask, part):
        here = diag_part(flip(mask), part, mask - 1)
        return remote(
            here,
            here,
            sem_diag_send.at[0],
            sem_diag_recv.at[0],
            chip(flip(3 - mask)),
        )

    def token_pair(mask, part):
        here = token_rows(flip(mask), core, part)
        return remote(
            here, here, sem_tok_pair_send.at[0], sem_tok_pair_recv.at[mask - 1], (me, 1 - core)
        )

    for part in range(parts):
        for mask in (1, 2):
            token_copy(mask, part).start()

    for i in (3, 5, 6, 7, 8, 9, 10, 11):
        fetches[i].wait()
    for m in range(GROUP):
        wd[m] = raw_down[m * units : (m + 1) * units, :].astype(jnp.bfloat16)
    own_down.start()
    for j in range(blocks):
        src = pl.ds(p * blocks + j, 1)
        cols = pl.ds(pl.multiple_of(p * units + j * 128, 128), 128)
        for side, (scale, kernel, tap_bias) in enumerate(
            ((gate_scale, gate_kernel, gate_bias), (value_scale, value_kernel, value_bias))
        ):
            dst = slice(j * 256 + side * 128, j * 256 + side * 128 + 128)
            par[1:4, dst] = kernel[0:3, cols] * scale[src, :]
            par[4:5, dst] = tap_bias[src, :]

    for g in range(2):
        for mask in others:
            plane_up_landed(g, mask)
            both_ways(lambda side: first_hop(side, g, mask))

    for mask in others:
        here = edge_slot(flip(mask) + 1)
        remote(here, here, sem_edge_send.at[0], sem_edge_recv.at[mask], (me, 1 - core)).wait_recv()

    @pl.when(has_up)
    def _():
        edge_next.start()

    low_half = (z < half).astype(jnp.int32)

    def plane_of(step):
        distance = (step + 1) // 2
        below = (step + low_half) % 2
        return z + distance * (1 - 2 * below), below

    def wide(j):
        return pl.ds(pl.multiple_of(j * 256, 256), 256)

    plane_rows = GROUP * piece
    near_part = pl.ds(pl.multiple_of(jnp.where(has_down, plane_rows, 0), plane_rows), (planes - 1) * plane_rows)
    far_part = pl.ds(pl.multiple_of(jnp.where(has_down, 0, (planes - 1) * plane_rows), plane_rows), plane_rows)

    def begin(owner, j, slot):
        rows = pl.ds(pl.multiple_of(owner * rows_own, rows_own), rows_own)
        begun_sum[slot] = jnp.dot(tok[rows, near_part], up_all[j, near_part, :], preferred_element_type=jnp.float32)

    def begin_own(j, carry):
        begin(p, j, j)
        return carry

    def unit(owner, j, slot=None):
        rows = pl.ds(pl.multiple_of(owner * rows_own, rows_own), rows_own)
        if slot is not None:
            rest = jnp.dot(tok[rows, far_part], up_all[j, far_part, :], preferred_element_type=jnp.float32)
            taps[8:, :] = begun_sum[slot] + rest
        else:
            taps[8:, :] = jnp.dot(tok[rows, :], up_all[j], preferred_element_type=jnp.float32)
        taps[0:8, :] = edge_pre[j, pl.ds(pl.multiple_of(owner * EDGE + EDGE - 8, 8), 8), :]
        conv = par[4:5, wide(j)] + par[3:4, wide(j)] * taps[8 : 8 + rows_own, :]
        conv = conv + par[2:3, wide(j)] * taps[7 : 7 + rows_own, :]
        conv = conv + par[1:2, wide(j)] * taps[6 : 6 + rows_own, :]
        g, v = conv[:, :128], conv[:, 128:]
        root = math.sqrt(2.0 / math.pi)
        bend = jnp.tanh(g * (root + (root * 0.044715) * (g * g)))
        hidden[rows, pl.ds(pl.multiple_of(j * 128, 128), 128)] = ((0.5 * (g * v)) * (1.0 + bend)).astype(jnp.bfloat16)

    def landed(mask, part):
        here = token_rows(flip(mask), core, part)
        remote(here, here, sem_tok_send.at[0], sem_tok_recv.at[mask - 1, part], (me, 1 - core)).wait_recv()

    def half_group(owner, side):
        return tok.at[pl.ds(pl.multiple_of(owner * rows_own + side * part_rows, part_rows), part_rows), :]

    def pair_landed(mask):
        there = half_group(flip(mask), 1 - core)
        remote(there, there, sem_tok_pair_send.at[0], sem_tok_pair_recv.at[mask - 1], (me, 1 - core)).wait_recv()

    def pass_tokens(part):
        for mask in (1, 2):
            landed(mask, part)
            token_relay(mask, part).start()
            token_pair(mask, part).start()

    def near(side):
        def pieces():
            for mask in range(GROUP):
                first_landed(side, mask)
                piece_hop(side, mask).start()

        def whole():
            for mask in range(GROUP):
                first_landed(side, mask)

        onward = z + (1 - 2 * side)
        into_end = onward == (planes - 1 if side == 0 else 0)

        @pl.when(inner_plane & into_end)
        def _():
            pieces()

        @pl.when(inner_plane & jnp.logical_not(into_end))
        def _():
            whole()

            def one(j, carry):
                far_hop(side, 1, j).start()
                return carry

            lax.fori_loop(0, blocks, one, 0)

        @pl.when(end_plane & (has_down if side == 0 else has_up))
        def _():
            whole()

    @pl.when(low_half == 1)
    def _():
        near(1)
        near(0)

    @pl.when(low_half == 0)
    def _():
        near(0)
        near(1)

    pass_tokens(0)

    def send_down():
        for mask in others:
            plane_down(mask).start()

    def pass_rest():
        pass_tokens(parts - 1)
        send_down()

    @pl.when(end_plane)
    def _():
        for mask in range(GROUP):
            for side in (0, 1):

                @pl.when((z >= 2) if side == 0 else (z < planes - 2))
                def _():
                    piece_landed(side, mask)

            if mask == GROUP - 2:
                pass_rest()

    @pl.when(has_down)
    def _():
        here = edge_slot(0)
        remote(here, here, sem_edge_send.at[1], sem_edge_recv.at[0], (me, 1 - core)).wait_recv()

    own_up.wait()
    own_down.wait()

    @pl.when(end_plane)
    def _():
        lax.fori_loop(0, blocks, begin_own, 0)


    def edge_block(j):
        ahead = jnp.dot(edge[0 : GROUP * EDGE, :], up_all[j], preferred_element_type=jnp.float32)
        edge_pre[j] = ahead

    def far_round(j, carry):
        @pl.when(inner_plane)
        def _():
            for distance in range(2, planes - 1):
                for side in (0, 1):

                    @pl.when((z >= distance) if side == 0 else (z < planes - distance))
                    def _():
                        far_landed(side, distance, j)
                        far_hop(side, distance, j).start()

            edge_block(j)
            unit(p, j)

            @pl.when(j == max(0, blocks - 2))
            def _():
                pass_rest()

        return carry

    lax.fori_loop(0, blocks, far_round, 0)

    def block_rows(owner):
        return pl.ds(pl.multiple_of(owner * rows_own, rows_own), rows_own)

    strip = 2 * out_piece
    strips = chunk // strip
    per_core = half * strips

    def pair_copy(c, owner):
        return remote(
            stage.at[c, owner],
            pair_in.at[c % per_core, owner],
            sem_pair_send.at[0],
            sem_pair_recv.at[c % per_core, owner],
            (me, 1 - core),
        )

    half_rows = rows_own // 2

    def half_of(which):
        return pl.ds(pl.multiple_of(which * half_rows, half_rows), half_rows)

    def peer_copy(c, mask, which):
        return remote(
            stage.at[c, flip(mask), half_of(which)],
            peer_in.at[c % per_core, mask - 1, half_of(which)],
            sem_peer_send.at[0],
            sem_peer_recv.at[c % per_core],
            chip(flip(mask)),
        )

    def relay_copy(c, mask):
        return remote(
            stage.at[c, flip(3), half_of(mask - 1)],
            relay_in.at[c % per_core, mask - 1],
            sem_relay_send.at[0],
            sem_relay_recv.at[c % per_core, mask - 1],
            chip(flip(mask)),
        )

    def combine(c, owner):
        pair_copy(c, owner).wait_recv()
        both = stage[c, owner].astype(jnp.float32) + pair_in[c % per_core, owner].astype(jnp.float32)
        stage[c, owner] = both.astype(jnp.bfloat16)

    def product(c, owner):
        first = pl.multiple_of(c % strips * strip, strip)
        value = jnp.dot(
            hidden[block_rows(owner), :], down_all[c // strips, :, pl.ds(first, strip)], preferred_element_type=jnp.float32
        )
        stage[c, owner] = value.astype(jnp.bfloat16)

        @pl.when(jnp.logical_not(mine(c)))
        def _():
            pair_copy(c, owner).start()

    def send_out(c, mask):
        combine(c, flip(mask))

        @pl.when(mask == 3)
        def _():
            for way in (1, 2):
                relay_copy(c, way).start()

        @pl.when((mask == 1) | (mask == 2))
        def _():
            peer_copy(c, mask, mask - 1).start()

    def pass_on(c):
        for mask in (1, 2):
            relay_copy(c, mask).wait_recv()
            owner = flip(3 - mask)
            rows = half_of(mask - 1)
            total = stage[c, owner, rows, :].astype(jnp.float32) + relay_in[c % per_core, mask - 1].astype(jnp.float32)
            stage[c, owner, rows, :] = total.astype(jnp.bfloat16)
            peer_copy(c, 3 - mask, mask - 1).start()

    def mine(c):
        return c // per_core == core

    def own_down_out():
        both_ways(lambda side: line_down(side, me, side, wd.at[p]))
        for mask in others:
            f = z * GROUP + flip(mask)
            wait_down(f)
            both_ways(lambda side: line_down(side, f, side))

    diag_round = jnp.where(inner_plane, blocks - 1, min(2, blocks - 1))

    def up_round(j, carry):
        @pl.when(j == diag_round)
        def _():
            here = half_group(flip(3), core)
            remote(here, here, sem_diag_send.at[0], sem_diag_recv.at[0], (me, 1 - core)).wait_recv()
            for part in range(parts):
                token_pair(3, part).start()

        @pl.when(end_plane & (j > 0) & (j < 3) & (blocks > 4))
        def _():
            for k in (blocks - 2, blocks - 1):
                begin(flip(j), k, 2 * j + k)

        @pl.when(end_plane)
        def _():
            for distance in range(3, planes):
                for side in (0, 1):

                    @pl.when((z >= distance) if side == 0 else (z < planes - distance))
                    def _():
                        far_landed(side, distance, j)

        @pl.when(end_plane)
        def _():
            edge_block(j)

        final = j == blocks - 1

        def group(i, inner):
            mask = jnp.where(final, 3 - i, i)
            ready = jnp.where(mask == 3, diag_round, 0)

            @pl.when((mask > 0) & (j == ready))
            def _():
                pair_landed(mask)

            first = jnp.where(j == ready, 0, j)
            last = jnp.where(j >= ready, j + 1, 0)

            begun = end_plane & ((mask == 0) | ((mask < 3) & (j >= blocks - 2) & (blocks > 4)))

            def one(k, deeper):
                unit(flip(mask), k)
                return deeper

            lax.fori_loop(first, jnp.where(mask == 0, first, jnp.where(begun, first, last)), one, inner)

            @pl.when(inner_plane & (mask == 3) & (j == diag_round))
            def _():
                own_down_out()

            @pl.when(begun)
            def _():
                unit(flip(mask), j, jnp.where(mask == 0, j, 2 * mask + j))


            @pl.when(final)
            def _():
                for n in range(strips):
                    product(z * strips + n, flip(mask))

                @pl.when(mine(z * strips))
                def _():
                    for n in range(strips):
                        send_out(z * strips + n, mask)

            return inner

        lax.fori_loop(0, GROUP, group, carry)

        @pl.when(end_plane & (j == diag_round))
        def _():
            own_down_out()

        return carry

    lax.fori_loop(0, blocks, up_round, 0)

    @pl.when(mine(z * strips))
    def _():
        for n in range(strips - 1):
            pass_on(z * strips + n)

    def pass_plane(step):
        q, below = plane_of(step)

        @pl.when((q >= 0) & (q < planes))
        def _():
            def one(i, carry):
                f = q * GROUP + i
                wait_down(f)

                @pl.when((below == 1) & has_up)
                def _():
                    line_down(0, f, 2 + q).start()

                @pl.when((below == 0) & has_down)
                def _():
                    line_down(1, f, 2 + q).start()

                return carry

            lax.fori_loop(0, GROUP, one, 0)

    def sent(here, send, recv):
        remote(here, here, send, recv, (me, 1 - core)).wait_send()

    def drain_early():
        sent(tok.at[0:rows_own], sem_tok_send.at[0], sem_tok_recv.at[0, 0])
        sent(tok.at[0:part_rows], sem_diag_send.at[0], sem_diag_recv.at[0])
        sent(tok.at[0 : 3 * part_rows], sem_tok_pair_send.at[0], sem_tok_pair_recv.at[0])
        sent(edge.at[0 : 3 * EDGE], sem_edge_send.at[0], sem_edge_recv.at[0])
        sent(wu.at[0:3], sem_plane_send.at[0], sem_plane_recv.at[0, 0])
        sent(wd.at[0:3], sem_plane_send.at[1], sem_plane_recv.at[0, 0])
        whole = up_all.at[:, rows_of(0, GROUP), :]

        @pl.when(has_up)
        def _():
            edge_next.wait_send()

        for side in (0, 1):

            @pl.when(has_up if side == 0 else has_down)
            def _():
                sent(whole, sem_first_send.at[side], sem_first_recv.at[side, 0])

            onward = z + (1 - 2 * side)
            into_end = onward == (planes - 1 if side == 0 else 0)

            @pl.when(inner_plane & into_end)
            def _():
                sent(whole, sem_piece_send.at[0], sem_piece_recv.at[0])

            @pl.when(inner_plane)
            def _():
                for distance in range(1, planes - 1):
                    valid = (z >= distance) if side == 0 else (z < planes - distance)

                    @pl.when(valid & (jnp.logical_not(into_end) if distance == 1 else True))
                    def _():
                        sent(whole, sem_far_send.at[side, distance - 1], sem_far_recv.at[side, 0, 0])

    def down_step(n, before):
        step = n // strips
        q, below = plane_of(step)
        valid = (q >= 0) & (q < planes)
        c = q * strips + n % strips
        owed = before >= 0

        @pl.when((n == strips) & inner_plane)
        def _():
            pass_plane(1)

        @pl.when((n == strips + 1) & inner_plane)
        def _():
            pass_plane(2)

        @pl.when(n == 2 * strips)
        def _():
            drain_early()

        @pl.when((n == 2 * strips + 1) & inner_plane)
        def _():
            for later in range(3, 2 * planes - 1):
                pass_plane(later)

        @pl.when(valid & end_plane)
        def _():
            for i in range(GROUP // strips):
                wait_down(q * GROUP + n % strips * (GROUP // strips) + i)

        @pl.when(valid)
        def _():
            def one(i, inner):
                product(c, flip(3 - i))
                return inner

            lax.fori_loop(0, GROUP, one, 0)

            @pl.when(mine(c))
            def _():
                def one(i, inner):
                    send_out(c, 3 - i)
                    return inner

                lax.fori_loop(0, GROUP, one, 0)

        due = valid & owed & (mine(c) | (n % strips == strips - 1))

        @pl.when(due)
        def _():
            pass_on(before)

        return jnp.where(valid & mine(c), c, jnp.where(due, -1, before))

    first_owed = jnp.where(mine(z * strips), z * strips + strips - 1, -1)
    last = lax.fori_loop(strips, (2 * planes - 1) * strips, down_step, first_owed)

    def finish(c):
        i = c % per_core
        total = stage[c, p].astype(jnp.float32)
        landed_all = peer_in.at[i]
        remote(landed_all, landed_all, sem_peer_send.at[0], sem_peer_recv.at[i], chip(flip(1))).wait_recv()
        for mask in (1, 2):
            total = total + peer_in[i, mask - 1].astype(jnp.float32)
        cols = pl.ds(pl.multiple_of(i * strip, strip), strip)
        out[:, cols] = (total * osc[0:1, cols]).astype(jnp.bfloat16)

    @pl.when(last >= 0)
    def _():
        pass_on(last)

    def finish_one(i, carry):
        finish(core * per_core + i)
        return carry

    lax.fori_loop(0, per_core, finish_one, 0)

    sent(pair_in, sem_pair_send.at[0], sem_pair_recv.at[0, 0])
    sent(peer_in, sem_peer_send.at[0], sem_peer_recv.at[0])
    sent(relay_in, sem_relay_send.at[0], sem_relay_recv.at[0, 0])
    for side in (0, 1):

        @pl.when(has_up if side == 0 else has_down)
        def _():
            sent(down_all.at[0], sem_down_send.at[side], sem_down_recv.at[0])

    @pl.when(inner_plane)
    def _():
        def drain_down(q, carry):
            @pl.when(q != z)
            def _():
                sent(down_all.at[0], sem_down_send.at[2 + q], sem_down_recv.at[0])

            return carry

        lax.fori_loop(0, planes, drain_down, 0)


def grouped_body(count, tokens, norm_gain, gate_weight, value_weight, gate_scale, value_scale, gate_kernel, value_kernel, gate_bias, value_bias, down_weight, down_scale):
    planes = count // GROUP
    half = planes // 2
    rows, width = tokens.shape
    piece, local = gate_weight.shape
    out_piece = down_weight.shape[1]
    units = local // GROUP
    blocks = units // 128
    chunk = GROUP * out_piece
    strip = 2 * out_piece
    strips = chunk // strip
    per_core = half * strips
    dma = pltpu.SemaphoreType.DMA
    bf16, f32 = jnp.bfloat16, jnp.float32
    vmem = pl.BlockSpec(memory_space=pltpu.VMEM)
    hbm = pl.BlockSpec(memory_space=pl.ANY)
    return pl.pallas_call(
        functools.partial(fused_kernel, planes),
        out_shape=pltpu.VMEM((rows, half * chunk), bf16),
        in_specs=[hbm] * 12,
        out_specs=vmem,
        scratch_shapes=[
            pltpu.VMEM((GROUP * rows, width), bf16),
            pltpu.VMEM((blocks, width, 256), bf16),
            pltpu.VMEM((planes, units, chunk), bf16),
            pltpu.VMEM((GROUP * rows, units), bf16),
            pltpu.VMEM((2 * per_core, GROUP, rows, strip), bf16),
            pltpu.VMEM((per_core, GROUP, rows, strip), bf16),
            pltpu.VMEM((per_core, 2, rows, strip), bf16),
            pltpu.VMEM((per_core, 2, rows // 2, strip), bf16),
            pltpu.VMEM((rows + 8, 256), f32),
            pltpu.VMEM(((GROUP + 1) * EDGE, width), bf16),
            pltpu.VMEM((blocks, GROUP * EDGE, 256), f32),
            pltpu.VMEM((8, 2 * units), f32),
            pltpu.VMEM((GROUP, blocks, piece, 256), bf16),
            pltpu.VMEM((GROUP, units, out_piece), bf16),
            pltpu.VMEM((piece, local), f32),
            pltpu.VMEM((piece, local), f32),
            pltpu.VMEM((local, out_piece), f32),
            pltpu.VMEM((blocks + 4, rows, 256), f32),
            pltpu.VMEM((1, width), f32),
            pltpu.VMEM((local // 128, 128), f32),
            pltpu.VMEM((local // 128, 128), f32),
            pltpu.VMEM(gate_kernel.shape, f32),
            pltpu.VMEM(value_kernel.shape, f32),
            pltpu.VMEM((local // 128, 128), f32),
            pltpu.VMEM((local // 128, 128), f32),
            pltpu.VMEM((1, half * chunk), f32),
            dma((12,)),
            dma((2,)),
            dma((2,)),
            dma((2, GROUP)),
            dma((2,)),
            dma((2, GROUP)),
            dma((1,)),
            dma((GROUP,)),
            dma((2, max(1, planes - 2))),
            dma((2, max(1, planes - 2), blocks)),
            dma((2 + planes,)),
            dma((count,)),
            dma((2,)),
            dma((GROUP,)),
            dma((1,)),
            dma((2, 2)),
            dma((1,)),
            dma((1,)),
            dma((1,)),
            dma((3,)),
            dma((1,)),
            dma((per_core, GROUP)),
            dma((1,)),
            dma((per_core,)),
            dma((1,)),
            dma((per_core, 2)),
        ],
        compiler_params=pltpu.CompilerParams(
            collective_id=0, has_side_effects=True, vmem_limit_bytes=65400000
        ),
    )(
        tokens,
        gate_weight,
        value_weight,
        down_weight,
        norm_gain[None, :],
        gate_scale.reshape(-1, 128),
        value_scale.reshape(-1, 128),
        gate_kernel,
        value_kernel,
        gate_bias.reshape(-1, 128),
        value_bias.reshape(-1, 128),
        down_scale[None, :],
    )


def solution(mesh):
    count, tp = mesh.shape["fs"], mesh.shape["tp"]

    def whole(*arrays):
        local = arrays[2].shape[1]
        fits = tp == 2 and count % (2 * GROUP) == 0 and local % (GROUP * 128) == 0
        if fits:
            return grouped_body(count, *arrays)
        return body(*arrays)

    return jax.shard_map(
        whole,
        mesh=mesh,
        in_specs=(
            P("fs", None),
            P(),
            P("fs", "tp"),
            P("fs", "tp"),
            P("tp"),
            P("tp"),
            P(None, "tp"),
            P(None, "tp"),
            P("tp"),
            P("tp"),
            P("tp", "fs"),
            P("tp"),
        ),
        out_specs=P("fs", "tp"),
        check_vma=False,
    )
```

```python
import functools
import math

import jax
import jax.numpy as jnp
from jax import lax
from jax.experimental import pallas as pl
from jax.experimental.pallas import tpu as pltpu
from jax.sharding import PartitionSpec as P

epsilon = 1e-06


def from_behind(value, axis, steps):
    count = lax.axis_size(axis)
    leading, last = (max(0, -steps), min(count, count - steps))
    return lax.ppermute(value, axis, [(source, source + steps) for source in range(leading, last)])


def normalize(tokens, norm_gain):
    values = tokens.astype(jnp.float32)
    scaled = values * lax.rsqrt(jnp.mean(values * values, axis=1, keepdims=True) + epsilon)
    return (scaled * norm_gain[None, :]).astype(jnp.bfloat16)


def causal_mix(current, previous, kernel, tap_bias):
    row_count = current.shape[0]
    joined = jnp.concatenate([previous, current], axis=0).astype(jnp.float32)
    summed_taps = tap_bias[None, :] + kernel[2][None, :] * joined[2:]
    for back_by in (1, 2):
        summed_taps = (
            summed_taps
            + kernel[2 - back_by][None, :] * joined[2 - back_by : 2 - back_by + row_count]
        )
    return summed_taps


def body(
    tokens,
    norm_gain,
    gate_weight,
    value_weight,
    gate_scale,
    value_scale,
    gate_kernel,
    value_kernel,
    gate_bias,
    value_bias,
    down_weight,
    down_scale,
):
    normed = normalize(tokens, norm_gain)
    gate_low = gate_weight.astype(jnp.bfloat16)
    value_low = value_weight.astype(jnp.bfloat16)
    down_low = down_weight.astype(jnp.bfloat16)
    row_count = normed.shape[0]
    gate_full, value_full, down_full = (
        lax.all_gather(gate_low, "fs", axis=0, tiled=True),
        lax.all_gather(value_low, "fs", axis=0, tiled=True),
        lax.all_gather(down_low, "fs", axis=1, tiled=True),
    )
    gate_raw = jnp.dot(normed, gate_full, preferred_element_type=jnp.float32)
    value_raw = jnp.dot(normed, value_full, preferred_element_type=jnp.float32)
    gate_pre = (gate_raw * gate_scale[None, :]).astype(jnp.bfloat16)
    value_pre = (value_raw * value_scale[None, :]).astype(jnp.bfloat16)
    previous_gate, previous_value = from_behind(
        (gate_pre[row_count - 2 :], value_pre[row_count - 2 :]), "fs", 1
    )
    gate_conv = causal_mix(gate_pre, previous_gate, gate_kernel, gate_bias)
    value_conv = causal_mix(value_pre, previous_value, value_kernel, value_bias)
    hidden = (jax.nn.gelu(gate_conv, approximate=True) * value_conv).astype(jnp.bfloat16)
    partial_terms = jnp.dot(hidden, down_full, preferred_element_type=jnp.float32)
    summed = lax.psum_scatter(
        partial_terms.astype(jnp.bfloat16), "tp", scatter_dimension=1, tiled=True
    ).astype(jnp.float32)
    return (summed * down_scale[None, :]).astype(jnp.bfloat16)


MESH = pl.DeviceIdType.MESH
GROUP = 4
EDGE = 16


def fused_kernel(
    depth_planes,
    tok_hbm,
    gate_hbm,
    value_hbm,
    down_hbm,
    gain_hbm,
    gate_scale_hbm,
    value_scale_hbm,
    gate_kernel_hbm,
    value_kernel_hbm,
    gate_bias_hbm,
    value_bias_hbm,
    osc_hbm,
    out,
    tok,
    up_all,
    down_all,
    hidden,
    stage,
    pair_in,
    peer_in,
    relay_in,
    guest_in,
    guest_sum,
    guest_out,
    guest_back,
    taps,
    edge,
    edge_pre,
    par,
    wu,
    wd,
    raw_gate,
    raw_value,
    raw_down,
    begun_sum,
    gain,
    gate_scale,
    value_scale,
    gate_kernel,
    value_kernel,
    gate_bias,
    value_bias,
    osc,
    sem_fetch,
    sem_own,
    sem_plane_send,
    sem_plane_recv,
    sem_first_send,
    sem_first_recv,
    sem_piece_send,
    sem_piece_recv,
    sem_far_send,
    sem_far_recv,
    sem_down_send,
    sem_down_recv,
    sem_edge_send,
    sem_edge_recv,
    sem_tok_send,
    sem_tok_recv,
    sem_diag_send,
    sem_diag_recv,
    sem_tok_pair_send,
    sem_tok_pair_recv,
    sem_pair_send,
    sem_pair_recv,
    sem_peer_send,
    sem_peer_recv,
    sem_relay_send,
    sem_relay_recv,
    sem_guest_send,
    sem_guest_recv,
    sem_swap_send,
    sem_swap_recv,
    sem_home_send,
    sem_home_recv,
):
    planes = depth_planes
    half = planes // 2
    me = lax.axis_index("fs")
    core = lax.axis_index("tp")
    z, p = me // GROUP, me % GROUP
    rows_own = tok.shape[0] // GROUP
    part_rows = rows_own // 2
    blocks, piece = wu.shape[1], wu.shape[2]
    units = hidden.shape[1]
    out_piece = wd.shape[2]
    chunk = GROUP * out_piece
    has_up, has_down = z < planes - 1, z > 0
    inner_plane = has_up & has_down
    end_plane = jnp.logical_not(inner_plane)
    cut = min(2, blocks - 1)
    groups = ((0, cut), (cut, blocks))

    def flip(mask):
        px, py = p % 2, p // 2
        return (py + mask // 2) % 2 * 2 + (px + mask % 2) % 2

    def chip(target):
        return (z * GROUP + target, core)

    others = (1, 2, 3)

    own_rows = pl.ds(pl.multiple_of(p * rows_own, rows_own), rows_own)
    fetches = [
        pltpu.make_async_copy(src, dst, sem_fetch.at[i])
        for i, (src, dst) in enumerate(
            (
                (gate_hbm, raw_gate),
                (value_hbm, raw_value),
                (tok_hbm, tok.at[own_rows, :]),
                (down_hbm, raw_down),
                (gain_hbm, gain),
                (gate_scale_hbm, gate_scale),
                (value_scale_hbm, value_scale),
                (gate_kernel_hbm, gate_kernel),
                (value_kernel_hbm, value_kernel),
                (gate_bias_hbm, gate_bias),
                (value_bias_hbm, value_bias),
                (osc_hbm, osc),
            )
        )
    ]
    for fetch in fetches:
        fetch.start()

    barrier = pltpu.get_barrier_semaphore()
    for mask in others:
        pl.semaphore_signal(barrier, inc=1, device_id=chip(flip(mask)), device_id_type=MESH)
    pl.semaphore_signal(barrier, inc=1, device_id=(me, 1 - core), device_id_type=MESH)

    @pl.when(has_up)
    def _():
        pl.semaphore_signal(barrier, inc=1, device_id=(me + GROUP, core), device_id_type=MESH)

    @pl.when(has_down)
    def _():
        pl.semaphore_signal(barrier, inc=1, device_id=(me - GROUP, core), device_id_type=MESH)

    def remote(src, dst, send, recv, device):
        return pltpu.make_async_remote_copy(
            src_ref=src, dst_ref=dst, send_sem=send, recv_sem=recv, device_id=device, device_id_type=MESH
        )

    def rows_of(f, count=1):
        return pl.ds(pl.multiple_of(f * piece, piece), count * piece)

    def down_block(f):
        return down_all.at[f // GROUP, :, pl.ds(pl.multiple_of(f % GROUP * out_piece, out_piece), out_piece)]

    def line(side):
        return (me + (GROUP if side == 0 else -GROUP), core)

    def plane_up(g, mask):
        first, last = groups[g]
        return remote(
            wu.at[flip(mask), first:last],
            up_all.at[first:last, rows_of(me), :],
            sem_plane_send.at[0],
            sem_plane_recv.at[g, mask],
            chip(flip(mask)),
        )

    def plane_up_landed(g, mask):
        first, last = groups[g]
        here = up_all.at[first:last, rows_of(z * GROUP + flip(mask)), :]
        remote(here, here, sem_plane_send.at[0], sem_plane_recv.at[g, mask], chip(flip(mask))).wait_recv()

    def first_hop(side, g, mask):
        first, last = groups[g]
        there = up_all.at[first:last, rows_of(z * GROUP + flip(mask)), :]
        here = there if mask else wu.at[p, first:last]
        return remote(here, there, sem_first_send.at[side], sem_first_recv.at[side, mask], line(side))

    def first_landed(side, mask):
        here = up_all.at[:, rows_of((z + (2 * side - 1)) * GROUP + flip(mask)), :]
        remote(here, here, sem_first_send.at[side], sem_first_recv.at[side, mask], (me, 1 - core)).wait_recv()

    def piece_hop(side, mask):
        here = up_all.at[:, rows_of((z + (2 * side - 1)) * GROUP + flip(mask)), :]
        return remote(here, here, sem_piece_send.at[0], sem_piece_recv.at[mask], line(side))

    def piece_landed(side, mask):
        here = up_all.at[:, rows_of((z + 2 * (2 * side - 1)) * GROUP + flip(mask)), :]
        remote(here, here, sem_piece_send.at[0], sem_piece_recv.at[mask], (me, 1 - core)).wait_recv()

    def far_hop(side, distance, j):
        q = z + distance * (2 * side - 1)
        here = up_all.at[j, rows_of(q * GROUP, GROUP), :]
        return remote(
            here, here, sem_far_send.at[side, distance - 1], sem_far_recv.at[side, distance - 1, j], line(side)
        )

    def far_landed(side, distance, j):
        q = z + distance * (2 * side - 1)
        here = up_all.at[j, rows_of(q * GROUP, GROUP), :]
        remote(
            here, here, sem_far_send.at[side, distance - 2], sem_far_recv.at[side, distance - 2, j], (me, 1 - core)
        ).wait_recv()

    def plane_down(mask):
        return remote(
            wd.at[flip(mask)],
            down_block(me),
            sem_plane_send.at[1],
            sem_down_recv.at[me],
            chip(flip(mask)),
        )

    def line_down(side, f, slot, src=None):
        here = down_block(f)
        return remote(
            here if src is None else src, here, sem_down_send.at[slot], sem_down_recv.at[f], line(side)
        )

    def wait_down(f):
        here = down_block(f)
        remote(here, here, sem_down_send.at[0], sem_down_recv.at[f], (me, 1 - core)).wait_recv()

    def both_ways(copy_of):
        @pl.when(has_up)
        def _():
            copy_of(0).start()

        @pl.when(has_down)
        def _():
            copy_of(1).start()

    own_up = pltpu.make_async_copy(wu.at[p], up_all.at[:, rows_of(me), :], sem_own.at[0])
    own_down = pltpu.make_async_copy(wd.at[p], down_block(me), sem_own.at[1])

    def cast_block(j):
        for m in range(GROUP):
            first = m * units + j * 128
            wu[m, j, :, 0:128] = raw_gate[:, first : first + 128].astype(jnp.bfloat16)
            wu[m, j, :, 128:256] = raw_value[:, first : first + 128].astype(jnp.bfloat16)

    def normed(first, count):
        start = pl.multiple_of(p * rows_own + first, count)
        values = tok[pl.ds(start, count), :].astype(jnp.float32)
        scaled = values * lax.rsqrt(jnp.mean(values * values, axis=1, keepdims=True) + epsilon)
        return (scaled * gain[...]).astype(jnp.bfloat16)

    fetches[0].wait()
    fetches[1].wait()
    for g in range(2):
        for j in range(*groups[g]):
            cast_block(j)
        if g == 0:
            pl.semaphore_wait(barrier, 4 + has_up.astype(jnp.int32) + has_down.astype(jnp.int32))
        for mask in others:
            plane_up(g, mask).start()
        both_ways(lambda side: first_hop(side, g, 0))
    own_up.start()

    def edge_slot(slot):
        return edge.at[pl.ds(pl.multiple_of(slot * EDGE, EDGE), EDGE), :]

    def edge_copy(mask):
        here = edge_slot(p + 1)
        return remote(here, here, sem_edge_send.at[0], sem_edge_recv.at[mask], chip(flip(mask)))

    edge_next = remote(
        edge_slot(GROUP), edge_slot(0), sem_edge_send.at[1], sem_edge_recv.at[0], (me + GROUP, core)
    )

    @pl.when(jnp.logical_not(has_down))
    def _():
        edge[0:EDGE, :] = jnp.zeros_like(edge[0:EDGE, :])

    fetches[2].wait()
    fetches[4].wait()
    edge[pl.ds(pl.multiple_of((p + 1) * EDGE, EDGE), EDGE), :] = normed(rows_own - EDGE, EDGE)
    for mask in others:
        edge_copy(mask).start()
    norm_tile = 64

    def norm_step(i, carry):
        first = pl.multiple_of(i * norm_tile, norm_tile)
        tok[pl.ds(pl.multiple_of(p * rows_own + i * norm_tile, norm_tile), norm_tile), :] = normed(first, norm_tile)
        return carry

    lax.fori_loop(0, rows_own // norm_tile, norm_step, 0)

    parts = 2
    sub_rows = part_rows // parts
    diag_rows = sub_rows // 2

    def token_rows(owner, side, part):
        start = owner * rows_own + side * part_rows + part * sub_rows
        return tok.at[pl.ds(pl.multiple_of(start, sub_rows), sub_rows), :]

    def diag_part(owner, part, which):
        start = owner * rows_own + core * part_rows + part * sub_rows + which * diag_rows
        return tok.at[pl.ds(pl.multiple_of(start, diag_rows), diag_rows), :]

    def token_copy(mask, part):
        here = token_rows(p, core, part)
        return remote(here, here, sem_tok_send.at[0], sem_tok_recv.at[mask - 1, part], chip(flip(mask)))

    def token_relay(mask, part):
        here = diag_part(flip(mask), part, mask - 1)
        return remote(
            here,
            here,
            sem_diag_send.at[0],
            sem_diag_recv.at[0],
            chip(flip(3 - mask)),
        )

    def token_pair(mask, part):
        here = token_rows(flip(mask), core, part)
        return remote(
            here, here, sem_tok_pair_send.at[0], sem_tok_pair_recv.at[mask - 1], (me, 1 - core)
        )

    for part in range(parts):
        for mask in (1, 2):
            token_copy(mask, part).start()

    for i in (3, 5, 6, 7, 8, 9, 10, 11):
        fetches[i].wait()
    for m in range(GROUP):
        wd[m] = raw_down[m * units : (m + 1) * units, :].astype(jnp.bfloat16)
    own_down.start()
    for j in range(blocks):
        src = pl.ds(p * blocks + j, 1)
        cols = pl.ds(pl.multiple_of(p * units + j * 128, 128), 128)
        for side, (scale, kernel, tap_bias) in enumerate(
            ((gate_scale, gate_kernel, gate_bias), (value_scale, value_kernel, value_bias))
        ):
            dst = slice(j * 256 + side * 128, j * 256 + side * 128 + 128)
            par[1:4, dst] = kernel[0:3, cols] * scale[src, :]
            par[4:5, dst] = tap_bias[src, :]

    for g in range(2):
        for mask in others:
            plane_up_landed(g, mask)
            both_ways(lambda side: first_hop(side, g, mask))

    for mask in others:
        here = edge_slot(flip(mask) + 1)
        remote(here, here, sem_edge_send.at[0], sem_edge_recv.at[mask], (me, 1 - core)).wait_recv()

    @pl.when(has_up)
    def _():
        edge_next.start()

    low_half = (z < half).astype(jnp.int32)

    def plane_of(step):
        distance = (step + 1) // 2
        below = (step + low_half) % 2
        return z + distance * (1 - 2 * below), below

    def wide(j):
        return pl.ds(pl.multiple_of(j * 256, 256), 256)

    plane_rows = GROUP * piece
    near_part = pl.ds(pl.multiple_of(jnp.where(has_down, plane_rows, 0), plane_rows), (planes - 1) * plane_rows)
    far_part = pl.ds(pl.multiple_of(jnp.where(has_down, 0, (planes - 1) * plane_rows), plane_rows), plane_rows)

    def begin(owner, j, slot):
        rows = pl.ds(pl.multiple_of(owner * rows_own, rows_own), rows_own)
        begun_sum[slot] = jnp.dot(tok[rows, near_part], up_all[j, near_part, :], preferred_element_type=jnp.float32)

    def begin_own(j, carry):
        begin(p, j, j)
        return carry

    def unit(owner, j, slot=None):
        rows = pl.ds(pl.multiple_of(owner * rows_own, rows_own), rows_own)
        if slot is not None:
            rest = jnp.dot(tok[rows, far_part], up_all[j, far_part, :], preferred_element_type=jnp.float32)
            taps[8:, :] = begun_sum[slot] + rest
        else:
            taps[8:, :] = jnp.dot(tok[rows, :], up_all[j], preferred_element_type=jnp.float32)
        taps[0:8, :] = edge_pre[j, pl.ds(pl.multiple_of(owner * EDGE + EDGE - 8, 8), 8), :]
        conv = par[4:5, wide(j)] + par[3:4, wide(j)] * taps[8 : 8 + rows_own, :]
        conv = conv + par[2:3, wide(j)] * taps[7 : 7 + rows_own, :]
        conv = conv + par[1:2, wide(j)] * taps[6 : 6 + rows_own, :]
        g, v = conv[:, :128], conv[:, 128:]
        root = math.sqrt(2.0 / math.pi)
        bend = jnp.tanh(g * (root + (root * 0.044715) * (g * g)))
        hidden[rows, pl.ds(pl.multiple_of(j * 128, 128), 128)] = ((0.5 * (g * v)) * (1.0 + bend)).astype(jnp.bfloat16)

    def landed(mask, part):
        here = token_rows(flip(mask), core, part)
        remote(here, here, sem_tok_send.at[0], sem_tok_recv.at[mask - 1, part], (me, 1 - core)).wait_recv()

    def half_group(owner, side):
        return tok.at[pl.ds(pl.multiple_of(owner * rows_own + side * part_rows, part_rows), part_rows), :]

    def pair_landed(mask):
        there = half_group(flip(mask), 1 - core)
        remote(there, there, sem_tok_pair_send.at[0], sem_tok_pair_recv.at[mask - 1], (me, 1 - core)).wait_recv()

    def pass_tokens(part):
        for mask in (1, 2):
            landed(mask, part)
            token_relay(mask, part).start()
            token_pair(mask, part).start()

    def near(side):
        def pieces():
            for mask in range(GROUP):
                first_landed(side, mask)
                piece_hop(side, mask).start()

        def whole():
            for mask in range(GROUP):
                first_landed(side, mask)

        onward = z + (1 - 2 * side)
        into_end = onward == (planes - 1 if side == 0 else 0)

        @pl.when(inner_plane & into_end)
        def _():
            pieces()

        @pl.when(inner_plane & jnp.logical_not(into_end))
        def _():
            whole()

            def one(j, carry):
                far_hop(side, 1, j).start()
                return carry

            lax.fori_loop(0, blocks, one, 0)

        @pl.when(end_plane & (has_down if side == 0 else has_up))
        def _():
            whole()

    @pl.when(low_half == 1)
    def _():
        near(1)
        near(0)

    @pl.when(low_half == 0)
    def _():
        near(0)
        near(1)

    pass_tokens(0)

    def send_down():
        for mask in others:
            plane_down(mask).start()

    def pass_rest():
        pass_tokens(parts - 1)
        send_down()

    @pl.when(end_plane)
    def _():
        for mask in range(GROUP):
            for side in (0, 1):

                @pl.when((z >= 2) if side == 0 else (z < planes - 2))
                def _():
                    piece_landed(side, mask)

            if mask == GROUP - 2:
                pass_rest()

    @pl.when(has_down)
    def _():
        here = edge_slot(0)
        remote(here, here, sem_edge_send.at[1], sem_edge_recv.at[0], (me, 1 - core)).wait_recv()

    own_up.wait()
    own_down.wait()

    @pl.when(end_plane)
    def _():
        lax.fori_loop(0, blocks, begin_own, 0)


    def edge_block(j):
        ahead = jnp.dot(edge[0 : GROUP * EDGE, :], up_all[j], preferred_element_type=jnp.float32)
        edge_pre[j] = ahead

    def far_round(j, carry):
        @pl.when(inner_plane)
        def _():
            for distance in range(2, planes - 1):
                for side in (0, 1):

                    @pl.when((z >= distance) if side == 0 else (z < planes - distance))
                    def _():
                        far_landed(side, distance, j)
                        far_hop(side, distance, j).start()

            edge_block(j)
            unit(p, j)

            @pl.when(j == max(0, blocks - 2))
            def _():
                pass_rest()

        return carry

    lax.fori_loop(0, blocks, far_round, 0)

    def block_rows(owner):
        return pl.ds(pl.multiple_of(owner * rows_own, rows_own), rows_own)

    strip = 2 * out_piece
    strips = chunk // strip
    per_core = half * strips

    def pair_copy(c, owner):
        return remote(
            stage.at[c, owner],
            pair_in.at[c % per_core, owner],
            sem_pair_send.at[0],
            sem_pair_recv.at[c % per_core, owner],
            (me, 1 - core),
        )

    slab = guest_in.shape[2]
    kept = rows_own - slab
    lends = end_plane & (z // half == core)
    hosts = inner_plane & (((z == 1) & (core == 0)) | ((z == planes - 2) & ((planes - 1) // half == core)))
    if planes < 4:
        lends = hosts = me < 0

    def sized(run):
        @pl.when(lends)
        def _():
            run(kept // 2)

        @pl.when(jnp.logical_not(lends))
        def _():
            run(rows_own // 2)

    def half_of(which, size):
        return pl.ds(pl.multiple_of(which * size, size), size)

    def peer_copy(c, mask, which, size):
        return remote(
            stage.at[c, flip(mask), half_of(which, size)],
            peer_in.at[c % per_core, mask - 1, half_of(which, size)],
            sem_peer_send.at[0],
            sem_peer_recv.at[c % per_core],
            chip(flip(mask)),
        )

    def relay_copy(c, mask, size):
        return remote(
            stage.at[c, flip(3), half_of(mask - 1, size)],
            relay_in.at[c % per_core, mask - 1, 0:size],
            sem_relay_send.at[0],
            sem_relay_recv.at[c % per_core, mask - 1],
            chip(flip(mask)),
        )

    def guest_copy(c):
        return remote(
            stage.at[c, :, kept:rows_own, :],
            guest_in.at[c % per_core],
            sem_guest_send.at[0],
            sem_guest_recv.at[c % per_core],
            (jnp.where(z == 0, me + GROUP, me - GROUP), core),
        )

    def guest_swap(k, mask):
        return remote(
            guest_in.at[k, flip(mask)],
            guest_sum.at[k, mask - 1],
            sem_swap_send.at[0],
            sem_swap_recv.at[k],
            chip(flip(mask)),
        )

    def guest_home(k):
        return remote(
            guest_out.at[k],
            guest_back.at[k],
            sem_home_send.at[0],
            sem_home_recv.at[k],
            (jnp.where(z == 1, me - GROUP, me + GROUP), core),
        )

    def landing(here, recv):
        remote(here, here, sem_guest_send.at[0], recv, chip(flip(1))).wait_recv()

    def swap_guests():
        for k in range(per_core):
            landing(guest_in.at[k], sem_guest_recv.at[k])
            for mask in others:
                guest_swap(k, mask).start()

    def return_guests():
        for k in range(per_core):
            landing(guest_sum.at[k], sem_swap_recv.at[k])
            total = guest_in[k, p].astype(jnp.float32)
            for mask in others:
                total = total + guest_sum[k, mask - 1].astype(jnp.float32)
            guest_out[k] = (total * osc[0:1, k * strip : (k + 1) * strip]).astype(jnp.bfloat16)
            guest_home(k).start()

    def combine(c, owner):
        pair_copy(c, owner).wait_recv()
        both = stage[c, owner].astype(jnp.float32) + pair_in[c % per_core, owner].astype(jnp.float32)
        stage[c, owner] = both.astype(jnp.bfloat16)

    def product(c, owner):
        first = pl.multiple_of(c % strips * strip, strip)
        value = jnp.dot(
            hidden[block_rows(owner), :], down_all[c // strips, :, pl.ds(first, strip)], preferred_element_type=jnp.float32
        )
        stage[c, owner] = value.astype(jnp.bfloat16)

        @pl.when(jnp.logical_not(mine(c)))
        def _():
            pair_copy(c, owner).start()

    def send_out(c, mask):
        combine(c, flip(mask))

        @pl.when(mask == 3)
        def _():
            def run(size):
                for way in (1, 2):
                    relay_copy(c, way, size).start()

            sized(run)

        @pl.when((mask == 1) | (mask == 2))
        def _():
            sized(lambda size: peer_copy(c, mask, mask - 1, size).start())

        @pl.when((mask == 0) & lends)
        def _():
            guest_copy(c).start()

    def pass_on(c):
        def run(size):
            for mask in (1, 2):
                relay_copy(c, mask, size).wait_recv()
                owner = flip(3 - mask)
                rows = half_of(mask - 1, size)
                added = relay_in[c % per_core, mask - 1, 0:size].astype(jnp.float32)
                stage[c, owner, rows, :] = (stage[c, owner, rows, :].astype(jnp.float32) + added).astype(jnp.bfloat16)
                peer_copy(c, 3 - mask, mask - 1, size).start()

        sized(run)

    def mine(c):
        return c // per_core == core

    def own_down_out():
        both_ways(lambda side: line_down(side, me, side, wd.at[p]))
        for mask in others:
            f = z * GROUP + flip(mask)
            wait_down(f)
            both_ways(lambda side: line_down(side, f, side))

    diag_round = jnp.where(inner_plane, blocks - 1, min(2, blocks - 1))

    down_unit = jnp.where(inner_plane, min(2, blocks - 1), 0)

    def up_round(j, carry):
        @pl.when(j == diag_round)
        def _():
            here = half_group(flip(3), core)
            remote(here, here, sem_diag_send.at[0], sem_diag_recv.at[0], (me, 1 - core)).wait_recv()
            for part in range(parts):
                token_pair(3, part).start()

        @pl.when(end_plane & (j > 0) & (j < 3) & (blocks > 4))
        def _():
            begin(flip(j), blocks - 1, blocks + j - 1)

        @pl.when(end_plane)
        def _():
            for distance in range(3, planes):
                for side in (0, 1):

                    @pl.when((z >= distance) if side == 0 else (z < planes - distance))
                    def _():
                        far_landed(side, distance, j)

        @pl.when(end_plane)
        def _():
            edge_block(j)

        final = j == blocks - 1

        def group(i, inner):
            mask = jnp.where(final, 3 - i, i)
            ready = jnp.where(mask == 3, diag_round, 0)

            @pl.when((mask > 0) & (j == ready))
            def _():
                pair_landed(mask)

            first = jnp.where(j == ready, 0, j)
            last = jnp.where(j >= ready, j + 1, 0)

            begun = end_plane & ((mask == 0) | ((mask < 3) & (j == blocks - 1) & (blocks > 4)))

            def one(k, deeper):
                unit(flip(mask), k)

                @pl.when((mask == 3) & (j == diag_round) & (k == down_unit))
                def _():
                    own_down_out()

                return deeper

            lax.fori_loop(first, jnp.where(mask == 0, first, jnp.where(begun, first, last)), one, inner)

            @pl.when(begun)
            def _():
                unit(flip(mask), j, jnp.where(mask == 0, j, mask + j))


            @pl.when(final)
            def _():
                for n in range(strips):
                    product(z * strips + n, flip(mask))

                @pl.when(mine(z * strips))
                def _():
                    for n in range(strips):
                        send_out(z * strips + n, mask)

            return inner

        lax.fori_loop(0, GROUP, group, carry)

        return carry

    lax.fori_loop(0, blocks, up_round, 0)

    @pl.when(mine(z * strips))
    def _():
        for n in range(strips - 1):
            pass_on(z * strips + n)

    def pass_plane(step):
        q, below = plane_of(step)

        @pl.when((q >= 0) & (q < planes))
        def _():
            def one(i, carry):
                f = q * GROUP + i
                wait_down(f)

                @pl.when((below == 1) & has_up)
                def _():
                    line_down(0, f, 2 + q).start()

                @pl.when((below == 0) & has_down)
                def _():
                    line_down(1, f, 2 + q).start()

                return carry

            lax.fori_loop(0, GROUP, one, 0)

    def sent(here, send, recv):
        remote(here, here, send, recv, (me, 1 - core)).wait_send()

    def drain_early():
        sent(tok.at[0:rows_own], sem_tok_send.at[0], sem_tok_recv.at[0, 0])
        sent(tok.at[0:part_rows], sem_diag_send.at[0], sem_diag_recv.at[0])
        sent(tok.at[0 : 3 * part_rows], sem_tok_pair_send.at[0], sem_tok_pair_recv.at[0])
        sent(edge.at[0 : 3 * EDGE], sem_edge_send.at[0], sem_edge_recv.at[0])
        sent(wu.at[0:3], sem_plane_send.at[0], sem_plane_recv.at[0, 0])
        sent(wd.at[0:3], sem_plane_send.at[1], sem_plane_recv.at[0, 0])
        whole = up_all.at[:, rows_of(0, GROUP), :]

        @pl.when(has_up)
        def _():
            edge_next.wait_send()

        for side in (0, 1):

            @pl.when(has_up if side == 0 else has_down)
            def _():
                sent(whole, sem_first_send.at[side], sem_first_recv.at[side, 0])

            onward = z + (1 - 2 * side)
            into_end = onward == (planes - 1 if side == 0 else 0)

            @pl.when(inner_plane & into_end)
            def _():
                sent(whole, sem_piece_send.at[0], sem_piece_recv.at[0])

            @pl.when(inner_plane)
            def _():
                for distance in range(1, planes - 1):
                    valid = (z >= distance) if side == 0 else (z < planes - distance)

                    @pl.when(valid & (jnp.logical_not(into_end) if distance == 1 else True))
                    def _():
                        sent(whole, sem_far_send.at[side, distance - 1], sem_far_recv.at[side, 0, 0])

    def down_step(n, before):
        step = n // strips
        q, below = plane_of(step)
        valid = (q >= 0) & (q < planes)
        c = q * strips + n % strips
        owed = before >= 0

        @pl.when((n == strips) & inner_plane)
        def _():
            pass_plane(1)

        @pl.when((n == strips + 1) & inner_plane)
        def _():
            pass_plane(2)

        @pl.when(n == 2 * strips)
        def _():
            drain_early()

        @pl.when((n == 2 * strips + 1) & inner_plane)
        def _():
            for later in range(3, 2 * planes - 1):
                pass_plane(later)

            @pl.when(hosts)
            def _():
                swap_guests()

        @pl.when(valid & end_plane)
        def _():
            for i in range(GROUP // strips):
                wait_down(q * GROUP + n % strips * (GROUP // strips) + i)

        @pl.when(valid)
        def _():
            def one(i, inner):
                product(c, flip(3 - i))
                return inner

            lax.fori_loop(0, GROUP, one, 0)

            @pl.when(mine(c))
            def _():
                def one(i, inner):
                    send_out(c, 3 - i)
                    return inner

                lax.fori_loop(0, GROUP, one, 0)

        due = valid & owed & (mine(c) | (n % strips == strips - 1))

        @pl.when(due)
        def _():
            pass_on(before)

        return jnp.where(valid & mine(c), c, jnp.where(due, -1, before))

    first_owed = jnp.where(mine(z * strips), z * strips + strips - 1, -1)
    last = lax.fori_loop(strips, (2 * planes - 1) * strips, down_step, first_owed)

    def finish(c):
        i = c % per_core
        cols = pl.ds(pl.multiple_of(i * strip, strip), strip)

        def run(size):
            rows = 2 * size
            landing(peer_in.at[i, :, 0:rows, :], sem_peer_recv.at[i])
            total = stage[c, p, 0:rows].astype(jnp.float32)
            for mask in (1, 2):
                total = total + peer_in[i, mask - 1, 0:rows].astype(jnp.float32)
            out[0:rows, cols] = (total * osc[0:1, cols]).astype(jnp.bfloat16)

        sized(run)

        @pl.when(lends)
        def _():
            landing(guest_back.at[i], sem_home_recv.at[i])
            out[kept:rows_own, cols] = guest_back[i]

    @pl.when(last >= 0)
    def _():
        pass_on(last)

    def finish_one(i, carry):
        finish(core * per_core + i)
        return carry

    @pl.when(hosts)
    def _():
        return_guests()

    lax.fori_loop(0, per_core, finish_one, 0)

    sent(pair_in, sem_pair_send.at[0], sem_pair_recv.at[0, 0])

    def drain_sums(size):
        sent(peer_in.at[:, :, 0 : 2 * size, :], sem_peer_send.at[0], sem_peer_recv.at[0])
        sent(relay_in.at[:, :, 0:size, :], sem_relay_send.at[0], sem_relay_recv.at[0, 0])

    sized(drain_sums)

    @pl.when(lends)
    def _():
        sent(guest_in, sem_guest_send.at[0], sem_guest_recv.at[0])

    @pl.when(hosts)
    def _():
        sent(guest_sum, sem_swap_send.at[0], sem_swap_recv.at[0])
        sent(guest_out, sem_home_send.at[0], sem_home_recv.at[0])

    for side in (0, 1):

        @pl.when(has_up if side == 0 else has_down)
        def _():
            sent(down_all.at[0], sem_down_send.at[side], sem_down_recv.at[0])

    @pl.when(inner_plane)
    def _():
        def drain_down(q, carry):
            @pl.when(q != z)
            def _():
                sent(down_all.at[0], sem_down_send.at[2 + q], sem_down_recv.at[0])

            return carry

        lax.fori_loop(0, planes, drain_down, 0)


def grouped_body(count, tokens, norm_gain, gate_weight, value_weight, gate_scale, value_scale, gate_kernel, value_kernel, gate_bias, value_bias, down_weight, down_scale):
    planes = count // GROUP
    half = planes // 2
    rows, width = tokens.shape
    piece, local = gate_weight.shape
    out_piece = down_weight.shape[1]
    units = local // GROUP
    blocks = units // 128
    chunk = GROUP * out_piece
    strip = 2 * out_piece
    strips = chunk // strip
    per_core = half * strips
    slab = max(1, rows // 8 // 32) * 32
    dma = pltpu.SemaphoreType.DMA
    bf16, f32 = jnp.bfloat16, jnp.float32
    vmem = pl.BlockSpec(memory_space=pltpu.VMEM)
    hbm = pl.BlockSpec(memory_space=pl.ANY)
    return pl.pallas_call(
        functools.partial(fused_kernel, planes),
        out_shape=pltpu.VMEM((rows, half * chunk), bf16),
        in_specs=[hbm] * 12,
        out_specs=vmem,
        scratch_shapes=[
            pltpu.VMEM((GROUP * rows, width), bf16),
            pltpu.VMEM((blocks, width, 256), bf16),
            pltpu.VMEM((planes, units, chunk), bf16),
            pltpu.VMEM((GROUP * rows, units), bf16),
            pltpu.VMEM((2 * per_core, GROUP, rows, strip), bf16),
            pltpu.VMEM((per_core, GROUP, rows, strip), bf16),
            pltpu.VMEM((per_core, 2, rows, strip), bf16),
            pltpu.VMEM((per_core, 2, rows // 2, strip), bf16),
            pltpu.VMEM((per_core, GROUP, slab, strip), bf16),
            pltpu.VMEM((per_core, 3, slab, strip), bf16),
            pltpu.VMEM((per_core, slab, strip), bf16),
            pltpu.VMEM((per_core, slab, strip), bf16),
            pltpu.VMEM((rows + 8, 256), f32),
            pltpu.VMEM(((GROUP + 1) * EDGE, width), bf16),
            pltpu.VMEM((blocks, GROUP * EDGE, 256), f32),
            pltpu.VMEM((8, 2 * units), f32),
            pltpu.VMEM((GROUP, blocks, piece, 256), bf16),
            pltpu.VMEM((GROUP, units, out_piece), bf16),
            pltpu.VMEM((piece, local), f32),
            pltpu.VMEM((piece, local), f32),
            pltpu.VMEM((local, out_piece), f32),
            pltpu.VMEM((blocks + 2, rows, 256), f32),
            pltpu.VMEM((1, width), f32),
            pltpu.VMEM((local // 128, 128), f32),
            pltpu.VMEM((local // 128, 128), f32),
            pltpu.VMEM(gate_kernel.shape, f32),
            pltpu.VMEM(value_kernel.shape, f32),
            pltpu.VMEM((local // 128, 128), f32),
            pltpu.VMEM((local // 128, 128), f32),
            pltpu.VMEM((1, half * chunk), f32),
            dma((12,)),
            dma((2,)),
            dma((2,)),
            dma((2, GROUP)),
            dma((2,)),
            dma((2, GROUP)),
            dma((1,)),
            dma((GROUP,)),
            dma((2, max(1, planes - 2))),
            dma((2, max(1, planes - 2), blocks)),
            dma((2 + planes,)),
            dma((count,)),
            dma((2,)),
            dma((GROUP,)),
            dma((1,)),
            dma((2, 2)),
            dma((1,)),
            dma((1,)),
            dma((1,)),
            dma((3,)),
            dma((1,)),
            dma((per_core, GROUP)),
            dma((1,)),
            dma((per_core,)),
            dma((1,)),
            dma((per_core, 2)),
            dma((1,)),
            dma((per_core,)),
            dma((1,)),
            dma((per_core,)),
            dma((1,)),
            dma((per_core,)),
        ],
        compiler_params=pltpu.CompilerParams(
            collective_id=0, has_side_effects=True, vmem_limit_bytes=65400000
        ),
    )(
        tokens,
        gate_weight,
        value_weight,
        down_weight,
        norm_gain[None, :],
        gate_scale.reshape(-1, 128),
        value_scale.reshape(-1, 128),
        gate_kernel,
        value_kernel,
        gate_bias.reshape(-1, 128),
        value_bias.reshape(-1, 128),
        down_scale[None, :],
    )


def solution(mesh):
    count, tp = mesh.shape["fs"], mesh.shape["tp"]

    def whole(*arrays):
        local = arrays[2].shape[1]
        fits = tp == 2 and count % (2 * GROUP) == 0 and local % (GROUP * 128) == 0
        if fits:
            return grouped_body(count, *arrays)
        return body(*arrays)

    return jax.shard_map(
        whole,
        mesh=mesh,
        in_specs=(
            P("fs", None),
            P(),
            P("fs", "tp"),
            P("fs", "tp"),
            P("tp"),
            P("tp"),
            P(None, "tp"),
            P(None, "tp"),
            P("tp"),
            P("tp"),
            P("tp", "fs"),
            P("tp"),
        ),
        out_specs=P("fs", "tp"),
        check_vma=False,
    )
```

```python
import functools
import math

import jax
import jax.numpy as jnp
from jax import lax
from jax.experimental import pallas as pl
from jax.experimental.pallas import tpu as pltpu
from jax.sharding import PartitionSpec as P

epsilon = 1e-06


def from_behind(value, axis, steps):
    count = lax.axis_size(axis)
    leading, last = (max(0, -steps), min(count, count - steps))
    return lax.ppermute(value, axis, [(source, source + steps) for source in range(leading, last)])


def normalize(tokens, norm_gain):
    values = tokens.astype(jnp.float32)
    scaled = values * lax.rsqrt(jnp.mean(values * values, axis=1, keepdims=True) + epsilon)
    return (scaled * norm_gain[None, :]).astype(jnp.bfloat16)


def causal_mix(current, previous, kernel, tap_bias):
    row_count = current.shape[0]
    joined = jnp.concatenate([previous, current], axis=0).astype(jnp.float32)
    summed_taps = tap_bias[None, :] + kernel[2][None, :] * joined[2:]
    for back_by in (1, 2):
        summed_taps = (
            summed_taps
            + kernel[2 - back_by][None, :] * joined[2 - back_by : 2 - back_by + row_count]
        )
    return summed_taps


def body(
    tokens,
    norm_gain,
    gate_weight,
    value_weight,
    gate_scale,
    value_scale,
    gate_kernel,
    value_kernel,
    gate_bias,
    value_bias,
    down_weight,
    down_scale,
):
    normed = normalize(tokens, norm_gain)
    gate_low = gate_weight.astype(jnp.bfloat16)
    value_low = value_weight.astype(jnp.bfloat16)
    down_low = down_weight.astype(jnp.bfloat16)
    row_count = normed.shape[0]
    gate_full, value_full, down_full = (
        lax.all_gather(gate_low, "fs", axis=0, tiled=True),
        lax.all_gather(value_low, "fs", axis=0, tiled=True),
        lax.all_gather(down_low, "fs", axis=1, tiled=True),
    )
    gate_raw = jnp.dot(normed, gate_full, preferred_element_type=jnp.float32)
    value_raw = jnp.dot(normed, value_full, preferred_element_type=jnp.float32)
    gate_pre = (gate_raw * gate_scale[None, :]).astype(jnp.bfloat16)
    value_pre = (value_raw * value_scale[None, :]).astype(jnp.bfloat16)
    previous_gate, previous_value = from_behind(
        (gate_pre[row_count - 2 :], value_pre[row_count - 2 :]), "fs", 1
    )
    gate_conv = causal_mix(gate_pre, previous_gate, gate_kernel, gate_bias)
    value_conv = causal_mix(value_pre, previous_value, value_kernel, value_bias)
    hidden = (jax.nn.gelu(gate_conv, approximate=True) * value_conv).astype(jnp.bfloat16)
    partial_terms = jnp.dot(hidden, down_full, preferred_element_type=jnp.float32)
    summed = lax.psum_scatter(
        partial_terms.astype(jnp.bfloat16), "tp", scatter_dimension=1, tiled=True
    ).astype(jnp.float32)
    return (summed * down_scale[None, :]).astype(jnp.bfloat16)


MESH = pl.DeviceIdType.MESH
GROUP = 4
EDGE = 16


def fused_kernel(
    depth_planes,
    tok_hbm,
    gate_hbm,
    value_hbm,
    down_hbm,
    gain_hbm,
    gate_scale_hbm,
    value_scale_hbm,
    gate_kernel_hbm,
    value_kernel_hbm,
    gate_bias_hbm,
    value_bias_hbm,
    osc_hbm,
    out,
    tok,
    up_all,
    down_all,
    hidden,
    stage,
    pair_in,
    peer_in,
    relay_in,
    guest_in,
    guest_sum,
    guest_out,
    guest_back,
    taps,
    edge,
    edge_pre,
    par,
    wu,
    wd,
    raw_gate,
    raw_value,
    raw_down,
    begun_sum,
    gain,
    gate_scale,
    value_scale,
    gate_kernel,
    value_kernel,
    gate_bias,
    value_bias,
    osc,
    sem_fetch,
    sem_own,
    sem_plane_send,
    sem_plane_recv,
    sem_first_send,
    sem_first_recv,
    sem_piece_send,
    sem_piece_recv,
    sem_far_send,
    sem_far_recv,
    sem_down_send,
    sem_down_recv,
    sem_edge_send,
    sem_edge_recv,
    sem_tok_send,
    sem_tok_recv,
    sem_diag_send,
    sem_diag_recv,
    sem_tok_pair_send,
    sem_tok_pair_recv,
    sem_pair_send,
    sem_pair_recv,
    sem_peer_send,
    sem_peer_recv,
    sem_relay_send,
    sem_relay_recv,
    sem_guest_send,
    sem_guest_recv,
    sem_swap_send,
    sem_swap_recv,
    sem_home_send,
    sem_home_recv,
):
    planes = depth_planes
    half = planes // 2
    me = lax.axis_index("fs")
    core = lax.axis_index("tp")
    z, p = me // GROUP, me % GROUP
    rows_own = tok.shape[0] // GROUP
    part_rows = rows_own // 2
    blocks, piece = wu.shape[1], wu.shape[2]
    units = hidden.shape[1]
    out_piece = wd.shape[2]
    chunk = GROUP * out_piece
    has_up, has_down = z < planes - 1, z > 0
    inner_plane = has_up & has_down
    end_plane = jnp.logical_not(inner_plane)
    cut = min(2, blocks - 1)
    groups = ((0, cut), (cut, blocks))

    def flip(mask):
        px, py = p % 2, p // 2
        return (py + mask // 2) % 2 * 2 + (px + mask % 2) % 2

    def chip(target):
        return (z * GROUP + target, core)

    others = (1, 2, 3)

    own_rows = pl.ds(pl.multiple_of(p * rows_own, rows_own), rows_own)
    fetches = [
        pltpu.make_async_copy(src, dst, sem_fetch.at[i])
        for i, (src, dst) in enumerate(
            (
                (gate_hbm, raw_gate),
                (value_hbm, raw_value),
                (tok_hbm, tok.at[own_rows, :]),
                (down_hbm, raw_down),
                (gain_hbm, gain),
                (gate_scale_hbm, gate_scale),
                (value_scale_hbm, value_scale),
                (gate_kernel_hbm, gate_kernel),
                (value_kernel_hbm, value_kernel),
                (gate_bias_hbm, gate_bias),
                (value_bias_hbm, value_bias),
                (osc_hbm, osc),
            )
        )
    ]
    for fetch in fetches:
        fetch.start()

    barrier = pltpu.get_barrier_semaphore()
    for mask in others:
        pl.semaphore_signal(barrier, inc=1, device_id=chip(flip(mask)), device_id_type=MESH)
    pl.semaphore_signal(barrier, inc=1, device_id=(me, 1 - core), device_id_type=MESH)

    @pl.when(has_up)
    def _():
        pl.semaphore_signal(barrier, inc=1, device_id=(me + GROUP, core), device_id_type=MESH)

    @pl.when(has_down)
    def _():
        pl.semaphore_signal(barrier, inc=1, device_id=(me - GROUP, core), device_id_type=MESH)

    def remote(src, dst, send, recv, device):
        return pltpu.make_async_remote_copy(
            src_ref=src, dst_ref=dst, send_sem=send, recv_sem=recv, device_id=device, device_id_type=MESH
        )

    def rows_of(f, count=1):
        return pl.ds(pl.multiple_of(f * piece, piece), count * piece)

    def down_block(f):
        return down_all.at[f // GROUP, :, pl.ds(pl.multiple_of(f % GROUP * out_piece, out_piece), out_piece)]

    def line(side):
        return (me + (GROUP if side == 0 else -GROUP), core)

    def plane_up(g, mask):
        first, last = groups[g]
        return remote(
            wu.at[flip(mask), first:last],
            up_all.at[first:last, rows_of(me), :],
            sem_plane_send.at[0],
            sem_plane_recv.at[g, mask],
            chip(flip(mask)),
        )

    def plane_up_landed(g, mask):
        first, last = groups[g]
        here = up_all.at[first:last, rows_of(z * GROUP + flip(mask)), :]
        remote(here, here, sem_plane_send.at[0], sem_plane_recv.at[g, mask], chip(flip(mask))).wait_recv()

    def first_hop(side, g, mask):
        first, last = groups[g]
        there = up_all.at[first:last, rows_of(z * GROUP + flip(mask)), :]
        here = there if mask else wu.at[p, first:last]
        return remote(here, there, sem_first_send.at[side], sem_first_recv.at[side, mask], line(side))

    def first_landed(side, mask):
        here = up_all.at[:, rows_of((z + (2 * side - 1)) * GROUP + flip(mask)), :]
        remote(here, here, sem_first_send.at[side], sem_first_recv.at[side, mask], (me, 1 - core)).wait_recv()

    def piece_hop(side, mask):
        here = up_all.at[:, rows_of((z + (2 * side - 1)) * GROUP + flip(mask)), :]
        return remote(here, here, sem_piece_send.at[0], sem_piece_recv.at[mask], line(side))

    def piece_landed(side, mask):
        here = up_all.at[:, rows_of((z + 2 * (2 * side - 1)) * GROUP + flip(mask)), :]
        remote(here, here, sem_piece_send.at[0], sem_piece_recv.at[mask], (me, 1 - core)).wait_recv()

    def far_hop(side, distance, j):
        q = z + distance * (2 * side - 1)
        here = up_all.at[j, rows_of(q * GROUP, GROUP), :]
        return remote(
            here, here, sem_far_send.at[side, distance - 1], sem_far_recv.at[side, distance - 1, j], line(side)
        )

    def far_landed(side, distance, j):
        q = z + distance * (2 * side - 1)
        here = up_all.at[j, rows_of(q * GROUP, GROUP), :]
        remote(
            here, here, sem_far_send.at[side, distance - 2], sem_far_recv.at[side, distance - 2, j], (me, 1 - core)
        ).wait_recv()

    def plane_down(mask):
        return remote(
            wd.at[flip(mask)],
            down_block(me),
            sem_plane_send.at[1],
            sem_down_recv.at[me],
            chip(flip(mask)),
        )

    def line_down(side, f, slot, src=None):
        here = down_block(f)
        return remote(
            here if src is None else src, here, sem_down_send.at[slot], sem_down_recv.at[f], line(side)
        )

    def wait_down(f):
        here = down_block(f)
        remote(here, here, sem_down_send.at[0], sem_down_recv.at[f], (me, 1 - core)).wait_recv()

    def both_ways(copy_of):
        @pl.when(has_up)
        def _():
            copy_of(0).start()

        @pl.when(has_down)
        def _():
            copy_of(1).start()

    own_up = pltpu.make_async_copy(wu.at[p], up_all.at[:, rows_of(me), :], sem_own.at[0])
    own_down = pltpu.make_async_copy(wd.at[p], down_block(me), sem_own.at[1])

    def cast_block(j):
        for m in range(GROUP):
            first = m * units + j * 128
            wu[m, j, :, 0:128] = raw_gate[:, first : first + 128].astype(jnp.bfloat16)
            wu[m, j, :, 128:256] = raw_value[:, first : first + 128].astype(jnp.bfloat16)

    def normed(first, count):
        start = pl.multiple_of(p * rows_own + first, count)
        values = tok[pl.ds(start, count), :].astype(jnp.float32)
        scaled = values * lax.rsqrt(jnp.mean(values * values, axis=1, keepdims=True) + epsilon)
        return (scaled * gain[...]).astype(jnp.bfloat16)

    fetches[0].wait()
    fetches[1].wait()
    for g in range(2):
        for j in range(*groups[g]):
            cast_block(j)
        if g == 0:
            pl.semaphore_wait(barrier, 4 + has_up.astype(jnp.int32) + has_down.astype(jnp.int32))
        for mask in others:
            plane_up(g, mask).start()
        both_ways(lambda side: first_hop(side, g, 0))
    own_up.start()

    def edge_slot(slot):
        return edge.at[pl.ds(pl.multiple_of(slot * EDGE, EDGE), EDGE), :]

    def edge_copy(mask):
        here = edge_slot(p + 1)
        return remote(here, here, sem_edge_send.at[0], sem_edge_recv.at[mask], chip(flip(mask)))

    edge_next = remote(
        edge_slot(GROUP), edge_slot(0), sem_edge_send.at[1], sem_edge_recv.at[0], (me + GROUP, core)
    )

    @pl.when(jnp.logical_not(has_down))
    def _():
        edge[0:EDGE, :] = jnp.zeros_like(edge[0:EDGE, :])

    fetches[2].wait()
    fetches[4].wait()
    edge[pl.ds(pl.multiple_of((p + 1) * EDGE, EDGE), EDGE), :] = normed(rows_own - EDGE, EDGE)
    for mask in others:
        edge_copy(mask).start()
    norm_tile = 64

    def norm_step(i, carry):
        first = pl.multiple_of(i * norm_tile, norm_tile)
        tok[pl.ds(pl.multiple_of(p * rows_own + i * norm_tile, norm_tile), norm_tile), :] = normed(first, norm_tile)
        return carry

    lax.fori_loop(0, rows_own // norm_tile, norm_step, 0)

    parts = 2
    sub_rows = part_rows // parts
    diag_rows = sub_rows // 2

    def token_rows(owner, side, part):
        start = owner * rows_own + side * part_rows + part * sub_rows
        return tok.at[pl.ds(pl.multiple_of(start, sub_rows), sub_rows), :]

    def diag_part(owner, part, which):
        start = owner * rows_own + core * part_rows + part * sub_rows + which * diag_rows
        return tok.at[pl.ds(pl.multiple_of(start, diag_rows), diag_rows), :]

    def token_copy(mask, part):
        here = token_rows(p, core, part)
        return remote(here, here, sem_tok_send.at[0], sem_tok_recv.at[mask - 1, part], chip(flip(mask)))

    def token_relay(mask, part):
        here = diag_part(flip(mask), part, mask - 1)
        return remote(
            here,
            here,
            sem_diag_send.at[0],
            sem_diag_recv.at[0],
            chip(flip(3 - mask)),
        )

    def token_pair(mask, part):
        here = token_rows(flip(mask), core, part)
        return remote(
            here, here, sem_tok_pair_send.at[0], sem_tok_pair_recv.at[mask - 1], (me, 1 - core)
        )

    for part in range(parts):
        for mask in (1, 2):
            token_copy(mask, part).start()

    for i in (3, 5, 6, 7, 8, 9, 10, 11):
        fetches[i].wait()
    for m in range(GROUP):
        wd[m] = raw_down[m * units : (m + 1) * units, :].astype(jnp.bfloat16)
    own_down.start()
    for j in range(blocks):
        src = pl.ds(p * blocks + j, 1)
        cols = pl.ds(pl.multiple_of(p * units + j * 128, 128), 128)
        for side, (scale, kernel, tap_bias) in enumerate(
            ((gate_scale, gate_kernel, gate_bias), (value_scale, value_kernel, value_bias))
        ):
            dst = slice(j * 256 + side * 128, j * 256 + side * 128 + 128)
            par[1:4, dst] = kernel[0:3, cols] * scale[src, :]
            par[4:5, dst] = tap_bias[src, :]

    for g in range(2):
        for mask in others:
            plane_up_landed(g, mask)
            both_ways(lambda side: first_hop(side, g, mask))

    for mask in others:
        here = edge_slot(flip(mask) + 1)
        remote(here, here, sem_edge_send.at[0], sem_edge_recv.at[mask], (me, 1 - core)).wait_recv()

    @pl.when(has_up)
    def _():
        edge_next.start()

    low_half = (z < half).astype(jnp.int32)

    def plane_of(step):
        distance = (step + 1) // 2
        below = (step + low_half) % 2
        return z + distance * (1 - 2 * below), below

    def wide(j):
        return pl.ds(pl.multiple_of(j * 256, 256), 256)

    plane_rows = GROUP * piece
    near_part = pl.ds(pl.multiple_of(jnp.where(has_down, plane_rows, 0), plane_rows), (planes - 1) * plane_rows)
    far_part = pl.ds(pl.multiple_of(jnp.where(has_down, 0, (planes - 1) * plane_rows), plane_rows), plane_rows)

    def begin(owner, j, slot):
        rows = pl.ds(pl.multiple_of(owner * rows_own, rows_own), rows_own)
        begun_sum[slot] = jnp.dot(tok[rows, near_part], up_all[j, near_part, :], preferred_element_type=jnp.float32)

    def begin_own(j, carry):
        begin(p, j, j)
        return carry

    def unit(owner, j, slot=None):
        rows = pl.ds(pl.multiple_of(owner * rows_own, rows_own), rows_own)
        if slot is not None:
            rest = jnp.dot(tok[rows, far_part], up_all[j, far_part, :], preferred_element_type=jnp.float32)
            taps[8:, :] = begun_sum[slot] + rest
        else:
            taps[8:, :] = jnp.dot(tok[rows, :], up_all[j], preferred_element_type=jnp.float32)
        taps[0:8, :] = edge_pre[j, pl.ds(pl.multiple_of(owner * EDGE + EDGE - 8, 8), 8), :]
        conv = par[4:5, wide(j)] + par[3:4, wide(j)] * taps[8 : 8 + rows_own, :]
        conv = conv + par[2:3, wide(j)] * taps[7 : 7 + rows_own, :]
        conv = conv + par[1:2, wide(j)] * taps[6 : 6 + rows_own, :]
        g, v = conv[:, :128], conv[:, 128:]
        root = math.sqrt(2.0 / math.pi)
        bend = jnp.tanh(g * (root + (root * 0.044715) * (g * g)))
        hidden[rows, pl.ds(pl.multiple_of(j * 128, 128), 128)] = ((0.5 * (g * v)) * (1.0 + bend)).astype(jnp.bfloat16)

    def landed(mask, part):
        here = token_rows(flip(mask), core, part)
        remote(here, here, sem_tok_send.at[0], sem_tok_recv.at[mask - 1, part], (me, 1 - core)).wait_recv()

    def half_group(owner, side):
        return tok.at[pl.ds(pl.multiple_of(owner * rows_own + side * part_rows, part_rows), part_rows), :]

    def pair_landed(mask):
        there = half_group(flip(mask), 1 - core)
        remote(there, there, sem_tok_pair_send.at[0], sem_tok_pair_recv.at[mask - 1], (me, 1 - core)).wait_recv()

    def pass_tokens(part):
        for mask in (1, 2):
            landed(mask, part)
            token_relay(mask, part).start()
            token_pair(mask, part).start()

    def near(side):
        def pieces():
            for mask in range(GROUP):
                first_landed(side, mask)
                piece_hop(side, mask).start()

        def whole():
            for mask in range(GROUP):
                first_landed(side, mask)

        onward = z + (1 - 2 * side)
        into_end = onward == (planes - 1 if side == 0 else 0)

        @pl.when(inner_plane & into_end)
        def _():
            pieces()

        @pl.when(inner_plane & jnp.logical_not(into_end))
        def _():
            whole()

            def one(j, carry):
                far_hop(side, 1, j).start()
                return carry

            lax.fori_loop(0, blocks, one, 0)

        @pl.when(end_plane & (has_down if side == 0 else has_up))
        def _():
            whole()

    @pl.when(low_half == 1)
    def _():
        near(1)
        near(0)

    @pl.when(low_half == 0)
    def _():
        near(0)
        near(1)

    pass_tokens(0)

    def send_down():
        for mask in others:
            plane_down(mask).start()

    def pass_rest():
        pass_tokens(parts - 1)
        send_down()

    @pl.when(end_plane)
    def _():
        for mask in range(GROUP):
            for side in (0, 1):

                @pl.when((z >= 2) if side == 0 else (z < planes - 2))
                def _():
                    piece_landed(side, mask)

            if mask == GROUP - 2:
                pass_rest()

    @pl.when(has_down)
    def _():
        here = edge_slot(0)
        remote(here, here, sem_edge_send.at[1], sem_edge_recv.at[0], (me, 1 - core)).wait_recv()

    own_up.wait()
    own_down.wait()

    @pl.when(end_plane)
    def _():
        lax.fori_loop(0, blocks, begin_own, 0)


    def edge_block(j):
        ahead = jnp.dot(edge[0 : GROUP * EDGE, :], up_all[j], preferred_element_type=jnp.float32)
        edge_pre[j] = ahead

    def far_round(j, carry):
        @pl.when(inner_plane)
        def _():
            for distance in range(2, planes - 1):
                for side in (0, 1):

                    @pl.when((z >= distance) if side == 0 else (z < planes - distance))
                    def _():
                        far_landed(side, distance, j)
                        far_hop(side, distance, j).start()

            edge_block(j)
            unit(p, j)

            @pl.when(j == max(0, blocks - 2))
            def _():
                pass_rest()

        return carry

    lax.fori_loop(0, blocks, far_round, 0)

    def block_rows(owner):
        return pl.ds(pl.multiple_of(owner * rows_own, rows_own), rows_own)

    strip = 2 * out_piece
    strips = chunk // strip
    per_core = half * strips

    def pair_copy(c, owner):
        return remote(
            stage.at[c, owner],
            pair_in.at[c % per_core, owner],
            sem_pair_send.at[0],
            sem_pair_recv.at[c % per_core, owner],
            (me, 1 - core),
        )

    slab = guest_in.shape[2]
    kept = rows_own - slab
    lends = end_plane & (z // half == core)
    hosts = inner_plane & (((z == 1) & (core == 0)) | ((z == planes - 2) & ((planes - 1) // half == core)))
    if planes < 4:
        lends = hosts = me < 0

    def sized(run):
        @pl.when(lends)
        def _():
            run(kept // 2)

        @pl.when(jnp.logical_not(lends))
        def _():
            run(rows_own // 2)

    def half_of(which, size):
        return pl.ds(pl.multiple_of(which * size, size), size)

    def peer_copy(c, mask, which, size):
        return remote(
            stage.at[c, flip(mask), half_of(which, size)],
            peer_in.at[c % per_core, mask - 1, half_of(which, size)],
            sem_peer_send.at[0],
            sem_peer_recv.at[c % per_core],
            chip(flip(mask)),
        )

    def relay_copy(c, mask, size):
        return remote(
            stage.at[c, flip(3), half_of(mask - 1, size)],
            relay_in.at[c % per_core, mask - 1, 0:size],
            sem_relay_send.at[0],
            sem_relay_recv.at[c % per_core, mask - 1],
            chip(flip(mask)),
        )

    def guest_copy(c):
        return remote(
            stage.at[c, :, kept:rows_own, :],
            guest_in.at[c % per_core],
            sem_guest_send.at[0],
            sem_guest_recv.at[c % per_core],
            (jnp.where(z == 0, me + GROUP, me - GROUP), core),
        )

    def guest_swap(k, mask):
        return remote(
            guest_in.at[k, flip(mask)],
            guest_sum.at[k, mask - 1],
            sem_swap_send.at[0],
            sem_swap_recv.at[k],
            chip(flip(mask)),
        )

    def guest_home(k):
        return remote(
            guest_out.at[k],
            guest_back.at[k],
            sem_home_send.at[0],
            sem_home_recv.at[k],
            (jnp.where(z == 1, me - GROUP, me + GROUP), core),
        )

    def landing(here, recv):
        remote(here, here, sem_guest_send.at[0], recv, chip(flip(1))).wait_recv()

    def swap_guests():
        for k in range(per_core):
            landing(guest_in.at[k], sem_guest_recv.at[k])
            for mask in others:
                guest_swap(k, mask).start()

    def return_guests():
        for k in range(per_core):
            landing(guest_sum.at[k], sem_swap_recv.at[k])
            total = guest_in[k, p].astype(jnp.float32)
            for mask in others:
                total = total + guest_sum[k, mask - 1].astype(jnp.float32)
            guest_out[k] = (total * osc[0:1, k * strip : (k + 1) * strip]).astype(jnp.bfloat16)
            guest_home(k).start()

    def combine(c, owner):
        pair_copy(c, owner).wait_recv()
        both = stage[c, owner].astype(jnp.float32) + pair_in[c % per_core, owner].astype(jnp.float32)
        stage[c, owner] = both.astype(jnp.bfloat16)

    def product(c, owner):
        first = pl.multiple_of(c % strips * strip, strip)
        value = jnp.dot(
            hidden[block_rows(owner), :], down_all[c // strips, :, pl.ds(first, strip)], preferred_element_type=jnp.float32
        )
        stage[c, owner] = value.astype(jnp.bfloat16)

        @pl.when(jnp.logical_not(mine(c)))
        def _():
            pair_copy(c, owner).start()

    def send_out(c, mask):
        combine(c, flip(mask))

        @pl.when(mask == 3)
        def _():
            def run(size):
                for way in (1, 2):
                    relay_copy(c, way, size).start()

            sized(run)

        @pl.when((mask == 1) | (mask == 2))
        def _():
            sized(lambda size: peer_copy(c, mask, mask - 1, size).start())

        @pl.when((mask == 0) & lends)
        def _():
            guest_copy(c).start()

    def pass_on(c):
        def run(size):
            for mask in (1, 2):
                relay_copy(c, mask, size).wait_recv()
                owner = flip(3 - mask)
                rows = half_of(mask - 1, size)
                added = relay_in[c % per_core, mask - 1, 0:size].astype(jnp.float32)
                stage[c, owner, rows, :] = (stage[c, owner, rows, :].astype(jnp.float32) + added).astype(jnp.bfloat16)
                peer_copy(c, 3 - mask, mask - 1, size).start()

        sized(run)

    def mine(c):
        return c // per_core == core

    def own_down_out():
        both_ways(lambda side: line_down(side, me, side, wd.at[p]))
        for mask in others:
            f = z * GROUP + flip(mask)
            wait_down(f)
            both_ways(lambda side: line_down(side, f, side))

    diag_round = jnp.where(inner_plane, blocks - 1, min(2, blocks - 1))

    down_unit = jnp.where(inner_plane, min(2, blocks - 1), 0)

    def up_round(j, carry):
        @pl.when(j == diag_round)
        def _():
            here = half_group(flip(3), core)
            remote(here, here, sem_diag_send.at[0], sem_diag_recv.at[0], (me, 1 - core)).wait_recv()
            for part in range(parts):
                token_pair(3, part).start()

        @pl.when(end_plane & (j > 0) & (j < 3) & (blocks > 4))
        def _():
            begin(flip(j), blocks - 1, blocks + j - 1)

        @pl.when(end_plane)
        def _():
            for distance in range(3, planes):
                for side in (0, 1):

                    @pl.when((z >= distance) if side == 0 else (z < planes - distance))
                    def _():
                        far_landed(side, distance, j)

        @pl.when(end_plane)
        def _():
            edge_block(j)

        final = j == blocks - 1

        def group(i, inner):
            mask = jnp.where(final, 3 - i, i)
            ready = jnp.where(mask == 3, diag_round, 0)

            @pl.when((mask > 0) & (j == ready))
            def _():
                pair_landed(mask)

            first = jnp.where(j == ready, 0, j)
            last = jnp.where(j >= ready, j + 1, 0)

            begun = end_plane & ((mask == 0) | ((mask < 3) & (j == blocks - 1) & (blocks > 4)))

            def one(k, deeper):
                unit(flip(mask), k)

                @pl.when((mask == 3) & (j == diag_round) & (k == down_unit))
                def _():
                    own_down_out()

                return deeper

            lax.fori_loop(first, jnp.where(mask == 0, first, jnp.where(begun, first, last)), one, inner)

            @pl.when(begun)
            def _():
                unit(flip(mask), j, jnp.where(mask == 0, j, mask + j))


            @pl.when(final)
            def _():
                for n in range(strips):
                    product(z * strips + n, flip(mask))

                @pl.when(mine(z * strips))
                def _():
                    for n in range(strips):
                        send_out(z * strips + n, mask)

            return inner

        lax.fori_loop(0, GROUP, group, carry)

        return carry

    lax.fori_loop(0, blocks, up_round, 0)

    @pl.when(mine(z * strips))
    def _():
        for n in range(strips - 1):
            pass_on(z * strips + n)

    def pass_plane(step):
        q, below = plane_of(step)

        @pl.when((q >= 0) & (q < planes))
        def _():
            def one(i, carry):
                f = q * GROUP + i
                wait_down(f)

                @pl.when((below == 1) & has_up)
                def _():
                    line_down(0, f, 2 + q).start()

                @pl.when((below == 0) & has_down)
                def _():
                    line_down(1, f, 2 + q).start()

                return carry

            lax.fori_loop(0, GROUP, one, 0)

    def sent(here, send, recv):
        remote(here, here, send, recv, (me, 1 - core)).wait_send()

    def drain_early():
        sent(tok.at[0:rows_own], sem_tok_send.at[0], sem_tok_recv.at[0, 0])
        sent(tok.at[0:part_rows], sem_diag_send.at[0], sem_diag_recv.at[0])
        sent(tok.at[0 : 3 * part_rows], sem_tok_pair_send.at[0], sem_tok_pair_recv.at[0])
        sent(edge.at[0 : 3 * EDGE], sem_edge_send.at[0], sem_edge_recv.at[0])
        sent(wu.at[0:3], sem_plane_send.at[0], sem_plane_recv.at[0, 0])
        sent(wd.at[0:3], sem_plane_send.at[1], sem_plane_recv.at[0, 0])
        whole = up_all.at[:, rows_of(0, GROUP), :]

        @pl.when(has_up)
        def _():
            edge_next.wait_send()

        for side in (0, 1):

            @pl.when(has_up if side == 0 else has_down)
            def _():
                sent(whole, sem_first_send.at[side], sem_first_recv.at[side, 0])

            onward = z + (1 - 2 * side)
            into_end = onward == (planes - 1 if side == 0 else 0)

            @pl.when(inner_plane & into_end)
            def _():
                sent(whole, sem_piece_send.at[0], sem_piece_recv.at[0])

            @pl.when(inner_plane)
            def _():
                for distance in range(1, planes - 1):
                    valid = (z >= distance) if side == 0 else (z < planes - distance)

                    @pl.when(valid & (jnp.logical_not(into_end) if distance == 1 else True))
                    def _():
                        sent(whole, sem_far_send.at[side, distance - 1], sem_far_recv.at[side, 0, 0])

    def down_step(n, before):
        step = n // strips
        q, below = plane_of(step)
        valid = (q >= 0) & (q < planes)
        c = q * strips + n % strips
        owed = before >= 0

        @pl.when((n == strips) & inner_plane)
        def _():
            pass_plane(1)

        @pl.when((n == strips + 1) & inner_plane)
        def _():
            pass_plane(2)

        @pl.when(n == 2 * strips)
        def _():
            drain_early()

        @pl.when((n == 2 * strips + 1) & inner_plane)
        def _():
            for later in range(3, 2 * planes - 1):
                pass_plane(later)

            @pl.when(hosts)
            def _():
                swap_guests()

        @pl.when(valid & end_plane)
        def _():
            for i in range(GROUP // strips):
                wait_down(q * GROUP + n % strips * (GROUP // strips) + i)

        @pl.when(valid)
        def _():
            def one(i, inner):
                product(c, flip(3 - i))
                return inner

            lax.fori_loop(0, GROUP, one, 0)

            @pl.when(mine(c))
            def _():
                def one(i, inner):
                    send_out(c, 3 - i)
                    return inner

                lax.fori_loop(0, GROUP, one, 0)

        due = valid & owed & (mine(c) | (n % strips == strips - 1))

        @pl.when(due)
        def _():
            pass_on(before)

        return jnp.where(valid & mine(c), c, jnp.where(due, -1, before))

    first_owed = jnp.where(mine(z * strips), z * strips + strips - 1, -1)
    last = lax.fori_loop(strips, (2 * planes - 1) * strips, down_step, first_owed)

    def finish(c):
        i = c % per_core
        cols = pl.ds(pl.multiple_of(i * strip, strip), strip)

        def run(size):
            rows = 2 * size
            landing(peer_in.at[i, :, 0:rows, :], sem_peer_recv.at[i])
            total = stage[c, p, 0:rows].astype(jnp.float32)
            for mask in (1, 2):
                total = total + peer_in[i, mask - 1, 0:rows].astype(jnp.float32)
            out[0:rows, cols] = (total * osc[0:1, cols]).astype(jnp.bfloat16)

        sized(run)

        @pl.when(lends)
        def _():
            landing(guest_back.at[i], sem_home_recv.at[i])
            out[kept:rows_own, cols] = guest_back[i]

    @pl.when(last >= 0)
    def _():
        pass_on(last)

    def finish_one(i, carry):
        finish(core * per_core + i)
        return carry

    @pl.when(hosts)
    def _():
        return_guests()

    lax.fori_loop(0, per_core, finish_one, 0)

    sent(pair_in, sem_pair_send.at[0], sem_pair_recv.at[0, 0])

    def drain_sums(size):
        sent(peer_in.at[:, :, 0 : 2 * size, :], sem_peer_send.at[0], sem_peer_recv.at[0])
        sent(relay_in.at[:, :, 0:size, :], sem_relay_send.at[0], sem_relay_recv.at[0, 0])

    sized(drain_sums)

    @pl.when(lends)
    def _():
        sent(guest_in, sem_guest_send.at[0], sem_guest_recv.at[0])

    @pl.when(hosts)
    def _():
        sent(guest_sum, sem_swap_send.at[0], sem_swap_recv.at[0])
        sent(guest_out, sem_home_send.at[0], sem_home_recv.at[0])

    for side in (0, 1):

        @pl.when(has_up if side == 0 else has_down)
        def _():
            sent(down_all.at[0], sem_down_send.at[side], sem_down_recv.at[0])

    @pl.when(inner_plane)
    def _():
        def drain_down(q, carry):
            @pl.when(q != z)
            def _():
                sent(down_all.at[0], sem_down_send.at[2 + q], sem_down_recv.at[0])

            return carry

        lax.fori_loop(0, planes, drain_down, 0)


def grouped_body(count, tokens, norm_gain, gate_weight, value_weight, gate_scale, value_scale, gate_kernel, value_kernel, gate_bias, value_bias, down_weight, down_scale):
    planes = count // GROUP
    half = planes // 2
    rows, width = tokens.shape
    piece, local = gate_weight.shape
    out_piece = down_weight.shape[1]
    units = local // GROUP
    blocks = units // 128
    chunk = GROUP * out_piece
    strip = 2 * out_piece
    strips = chunk // strip
    per_core = half * strips
    slab = max(1, rows // 6 // 32) * 32
    dma = pltpu.SemaphoreType.DMA
    bf16, f32 = jnp.bfloat16, jnp.float32
    vmem = pl.BlockSpec(memory_space=pltpu.VMEM)
    hbm = pl.BlockSpec(memory_space=pl.ANY)
    return pl.pallas_call(
        functools.partial(fused_kernel, planes),
        out_shape=pltpu.VMEM((rows, half * chunk), bf16),
        in_specs=[hbm] * 12,
        out_specs=vmem,
        scratch_shapes=[
            pltpu.VMEM((GROUP * rows, width), bf16),
            pltpu.VMEM((blocks, width, 256), bf16),
            pltpu.VMEM((planes, units, chunk), bf16),
            pltpu.VMEM((GROUP * rows, units), bf16),
            pltpu.VMEM((2 * per_core, GROUP, rows, strip), bf16),
            pltpu.VMEM((per_core, GROUP, rows, strip), bf16),
            pltpu.VMEM((per_core, 2, rows, strip), bf16),
            pltpu.VMEM((per_core, 2, rows // 2, strip), bf16),
            pltpu.VMEM((per_core, GROUP, slab, strip), bf16),
            pltpu.VMEM((per_core, 3, slab, strip), bf16),
            pltpu.VMEM((per_core, slab, strip), bf16),
            pltpu.VMEM((per_core, slab, strip), bf16),
            pltpu.VMEM((rows + 8, 256), f32),
            pltpu.VMEM(((GROUP + 1) * EDGE, width), bf16),
            pltpu.VMEM((blocks, GROUP * EDGE, 256), f32),
            pltpu.VMEM((8, 2 * units), f32),
            pltpu.VMEM((GROUP, blocks, piece, 256), bf16),
            pltpu.VMEM((GROUP, units, out_piece), bf16),
            pltpu.VMEM((piece, local), f32),
            pltpu.VMEM((piece, local), f32),
            pltpu.VMEM((local, out_piece), f32),
            pltpu.VMEM((blocks + 2, rows, 256), f32),
            pltpu.VMEM((1, width), f32),
            pltpu.VMEM((local // 128, 128), f32),
            pltpu.VMEM((local // 128, 128), f32),
            pltpu.VMEM(gate_kernel.shape, f32),
            pltpu.VMEM(value_kernel.shape, f32),
            pltpu.VMEM((local // 128, 128), f32),
            pltpu.VMEM((local // 128, 128), f32),
            pltpu.VMEM((1, half * chunk), f32),
            dma((12,)),
            dma((2,)),
            dma((2,)),
            dma((2, GROUP)),
            dma((2,)),
            dma((2, GROUP)),
            dma((1,)),
            dma((GROUP,)),
            dma((2, max(1, planes - 2))),
            dma((2, max(1, planes - 2), blocks)),
            dma((2 + planes,)),
            dma((count,)),
            dma((2,)),
            dma((GROUP,)),
            dma((1,)),
            dma((2, 2)),
            dma((1,)),
            dma((1,)),
            dma((1,)),
            dma((3,)),
            dma((1,)),
            dma((per_core, GROUP)),
            dma((1,)),
            dma((per_core,)),
            dma((1,)),
            dma((per_core, 2)),
            dma((1,)),
            dma((per_core,)),
            dma((1,)),
            dma((per_core,)),
            dma((1,)),
            dma((per_core,)),
        ],
        compiler_params=pltpu.CompilerParams(
            collective_id=0, has_side_effects=True, vmem_limit_bytes=65400000
        ),
    )(
        tokens,
        gate_weight,
        value_weight,
        down_weight,
        norm_gain[None, :],
        gate_scale.reshape(-1, 128),
        value_scale.reshape(-1, 128),
        gate_kernel,
        value_kernel,
        gate_bias.reshape(-1, 128),
        value_bias.reshape(-1, 128),
        down_scale[None, :],
    )


def solution(mesh):
    count, tp = mesh.shape["fs"], mesh.shape["tp"]

    def whole(*arrays):
        local = arrays[2].shape[1]
        fits = tp == 2 and count % (2 * GROUP) == 0 and local % (GROUP * 128) == 0
        if fits:
            return grouped_body(count, *arrays)
        return body(*arrays)

    return jax.shard_map(
        whole,
        mesh=mesh,
        in_specs=(
            P("fs", None),
            P(),
            P("fs", "tp"),
            P("fs", "tp"),
            P("tp"),
            P("tp"),
            P(None, "tp"),
            P(None, "tp"),
            P("tp"),
            P("tp"),
            P("tp", "fs"),
            P("tp"),
        ),
        out_specs=P("fs", "tp"),
        check_vma=False,
    )
```
